128 devices in a mesh: sp: 64 (over z, y, x), tp: 2 (over core).
Axes of the slice: x: 4, y: 4, z: 4, core: 2. Of those that a mesh axis runs over, the one named last changes fastest.
Arguments:
- glu_value: bfloat16 [16384, 1024], P('sp', 'tp'), may hold values from -12 to 12
- glu_gate: bfloat16 [16384, 1024], P('sp', 'tp'), may hold values from -8 to 8
- conv_kernel: bfloat16 [31, 1024], P(None, 'tp'), may hold values from -1 to 1
- conv_bias: float32 [1024], P('tp'), may hold values from -1.5 to 1.5
- group_gain: float32 [1024], P('tp'), may hold values from 0.1 to 1.9
- group_shift: float32 [1024], P('tp'), may hold values from -2.5 to 2.5
- out_weight: bfloat16 [1024, 2048], replicated, may hold values from -0.1875 to 0.1875
- residual: bfloat16 [16384, 2048], P(('sp', 'tp')), may hold values from -12 to 12
- ffn_gain: float32 [2048], replicated, may hold values from 0.1 to 1.9
- expert_pick: int32 [16384, 2], P(('sp', 'tp')), may hold values from 0 to 127, as said below
- pair_logits: float32 [16384, 2], P(('sp', 'tp')), may hold values from -1.2 to 1.2
- group_prob: float32 [16384], P(('sp', 'tp')), may hold values from 0.5 to 1
- gate_weight: bfloat16 [128, 2048, 512], P(('sp', 'tp')), may hold values from -0.125 to 0.125
- up_weight: bfloat16 [128, 2048, 512], P(('sp', 'tp')), may hold values from -0.125 to 0.125
- down_weight: bfloat16 [128, 512, 2048], P(('sp', 'tp')), may hold values from -0.75 to 0.75
Outputs:
- result: bfloat16 [16384, 2048], P(('sp', 'tp'))
The draws below stay inside these ranges and needn't reach their ends.
Inputs may be any that keep to these rules, and one draw needn't show every extreme that they name: `expert_pick`: both picks of a token are different experts of the same group of 32 consecutive experts. Among the 128 tokens of one device (aligned blocks of rows) no expert is picked more than 4 times, and in every such block some expert is picked exactly 4 times.
All inputs are finite; a program needn't handle non-finite values.
Results may differ from the reference program's by a relative error of at most 0.014.
Values may be sent and summed in bfloat16 or wider, within the bound.
No kernel may reach another device: no remote copies, remote signals or barrier semaphores. Data moves between devices by JAX's collectives and lax.ppermute only.
A program may use at most 64 MiB of HBM per device.

```python
import math
import jax
import jax.numpy as jnp
from jax import lax

D = 2048
CONV = 1024
CONV_GROUPS = 8
KERNEL = 31
FFE = 512
GROUPS = 4
TOK_DEV = 128
TOKENS = 16384
EXPERTS = 128
CAP = 4
N_SP = 64
N_TP = 2


def scaled_normal(key, row_total, columns, lowest, highest):
    subkeys = jax.random.split(key, 3)
    normal_part = jax.random.normal(subkeys[0], (row_total, columns), jnp.float32)
    row_scale = jnp.exp(jax.random.uniform(subkeys[1], (row_total, 1), jnp.float32, jnp.log(lowest), jnp.log(highest)))
    column_scale = jnp.exp(jax.random.uniform(subkeys[2], (1, columns), jnp.float32, jnp.log(lowest), jnp.log(highest)))
    return normal_part * row_scale * column_scale


def draw_residual(key, part):
    scaled = scaled_normal(key, TOKENS, D, 0.2, 2.0)
    return jnp.clip(scaled, -12.0, 12.0).astype(jnp.bfloat16)


def draw_glu_value(key, part):
    scaled = scaled_normal(key, TOKENS, CONV, 0.3, 3.0)
    return jnp.clip(scaled, -12.0, 12.0).astype(jnp.bfloat16)


def draw_expert_pick(key, part):
    per_group = EXPERTS // GROUPS
    pairs = per_group * CAP // 2
    universe = GROUPS * pairs
    blocks = TOKENS // TOK_DEV
    subkeys = jax.random.split(key, 3)
    full_group = jax.random.randint(subkeys[0], (), 0, GROUPS)

    def label_order(label_key):
        return jax.random.permutation(label_key, per_group)
    labels = jax.vmap(label_order)(jax.random.split(subkeys[1], GROUPS)).astype(jnp.int32)
    slot_index = jnp.arange(universe, dtype=jnp.int32)
    slot_group = slot_index // pairs
    slot_pair = slot_index % pairs
    forced = (slot_group == full_group) & (slot_pair < CAP)

    def one_block(block_key):
        inner = jax.random.split(block_key, 3)
        scores = jax.random.randint(inner[0], (universe,), 0, 1 << 18) * universe + slot_index
        scores = jnp.where(forced, slot_pair - CAP, scores)
        chosen = jnp.argsort(scores, stable=True)[:TOK_DEV]
        chosen = chosen[jax.random.permutation(inner[1], TOK_DEV)]
        group_of = slot_group[chosen]
        low_label = slot_pair[chosen] // CAP
        high_label = low_label + per_group // 2
        first_expert = group_of * per_group + labels[group_of, low_label]
        second_expert = group_of * per_group + labels[group_of, high_label]
        flipped = jax.random.randint(inner[2], (TOK_DEV,), 0, 2)
        left_pick = jnp.where(flipped == 1, second_expert, first_expert)
        right_pick = jnp.where(flipped == 1, first_expert, second_expert)
        return jnp.stack([left_pick, right_pick], axis=1)
    picked = jax.vmap(one_block)(jax.random.split(subkeys[2], blocks))
    return picked.reshape(TOKENS, 2).astype(jnp.int32)


def block_scale(key, shape, cuts, low, top_value):
    gain = 1.0
    for position, parts in cuts:
        draws = jax.random.uniform(jax.random.fold_in(jax.random.fold_in(key, 6), position), (parts,), jnp.float32, low / len(cuts), top_value / len(cuts))
        gain = gain * jnp.repeat(jnp.exp(draws), shape[position] // parts).reshape((-1,) + (1,) * (len(shape) - 1 - position))
    return gain


def scatter_about(rng, shape, spread, limit, pieces=(), kind=jnp.bfloat16):
    level = block_scale(rng, shape, pieces, -0.22, 0.18) if pieces else 1.0
    values = jax.random.normal(rng, shape, jnp.float32) * spread * level
    return jnp.minimum(jnp.maximum(values, -limit), limit).astype(kind)


def setup_inputs(seed: int = 0) -> dict:
    key_of = jax.random.split(jax.random.key(seed), 16)
    glu_value = draw_glu_value(jax.random.fold_in(key_of[15], 71), 0)
    glu_gate = scatter_about(key_of[1], (TOKENS, CONV), 1.5, 8.0, ((0, 64), (1, 2)))
    conv_kernel = scatter_about(key_of[2], (KERNEL, CONV), KERNEL ** -0.5, 1.0, ((1, 2),))
    conv_bias = scatter_about(key_of[3], (CONV,), 0.3, 1.5, ((0, 2),), jnp.float32)
    group_gain = jnp.clip(1.0 + 0.18 * jax.random.normal(key_of[4], (CONV,), jnp.float32), 0.1, 1.9)
    group_shift = scatter_about(key_of[5], (CONV,), 0.5, 2.5, ((0, 2),), jnp.float32)
    out_weight = scatter_about(key_of[6], (CONV, D), CONV ** -0.5, 0.1875)
    residual = draw_residual(jax.random.fold_in(key_of[15], 71), 0)
    ffn_gain = jnp.clip(1.0 + 0.18 * jax.random.normal(key_of[8], (D,), jnp.float32), 0.1, 1.9)
    expert_pick = draw_expert_pick(jax.random.fold_in(key_of[15], 71), 0)
    pair_logits = scatter_about(key_of[10], (TOKENS, 2), 0.3, 1.2, ((0, 128),), jnp.float32)
    group_prob = jnp.clip(jnp.exp(math.log(1.0) - 0.6931472 * jax.random.uniform(key_of[11], (TOKENS,), jnp.float32) ** block_scale(key_of[11], (TOKENS,), ((0, 128),), -0.2, 0.2)), 0.5, 1.0)
    gate_weight = scatter_about(key_of[12], (EXPERTS, D, FFE), D ** -0.5, 0.125, ((0, 128),))
    up_weight = scatter_about(key_of[13], (EXPERTS, D, FFE), D ** -0.5, 0.125, ((0, 128),))
    down_weight = scatter_about(key_of[14], (EXPERTS, FFE, D), (FFE // 8) ** -0.5, 0.75, ((0, 128),))
    return dict(glu_value=glu_value, glu_gate=glu_gate, conv_kernel=conv_kernel, conv_bias=conv_bias, group_gain=group_gain, group_shift=group_shift, out_weight=out_weight, residual=residual, ffn_gain=ffn_gain, expert_pick=expert_pick, pair_logits=pair_logits, group_prob=group_prob, gate_weight=gate_weight, up_weight=up_weight, down_weight=down_weight)


EPS = 1e-06

def conv_module(glu_value, glu_gate, conv_kernel, conv_bias, group_gain, group_shift):
    glued_rows = (glu_value.astype(jnp.float32) * jax.nn.sigmoid(glu_gate.astype(jnp.float32))).astype(jnp.bfloat16)
    reach_rows = conv_kernel.shape[0] - 1
    length = glued_rows.shape[0]
    padded = jnp.pad(glued_rows, ((reach_rows, 0), (0, 0))).astype(jnp.float32)
    kernel = conv_kernel.astype(jnp.float32)
    summed = jnp.zeros(glued_rows.shape, jnp.float32) + conv_bias.astype(jnp.float32)
    for offset in range(reach_rows + 1):
        summed = summed + kernel[offset] * padded[offset:offset + length]
    grouped = summed.reshape(length, CONV_GROUPS, -1)
    centre = lax.optimization_barrier(jnp.mean(grouped, axis=-1, keepdims=True))
    variance = lax.optimization_barrier(jnp.mean(jnp.square(grouped - centre), axis=-1, keepdims=True))
    leveled = ((grouped - centre) * lax.rsqrt(variance + EPS)).reshape(length, -1)
    return jax.nn.silu(leveled * group_gain + group_shift).astype(jnp.bfloat16)

def experts_apply(normed, expert_pick, gate_weight, up_weight, down_weight):
    picks = expert_pick.shape[1]
    slot_experts = expert_pick.reshape(-1)
    slot_total = slot_experts.shape[0]
    most_rows = N_SP * N_TP * CAP
    onehot = (slot_experts[:, None] == jnp.arange(EXPERTS, dtype=jnp.int32)[None, :]).astype(jnp.int32)
    before = (jnp.cumsum(onehot, axis=0) - onehot).astype(jnp.int32)
    slot_rank = lax.optimization_barrier(jnp.sum(before * onehot, axis=1)).astype(jnp.int32)
    slot_place = (slot_experts * most_rows + slot_rank).astype(jnp.int32)
    source_flat = jnp.full((EXPERTS * most_rows,), slot_total, jnp.int32)
    source_flat = source_flat.at[slot_place].set(jnp.arange(slot_total, dtype=jnp.int32))
    source_table = source_flat.reshape(EXPERTS, most_rows)
    padded_rows = jnp.concatenate([normed, jnp.zeros((1, normed.shape[1]), normed.dtype)], axis=0)

    def apply_expert(inputs):
        source_index, gate_part, up_part, down_part = inputs
        picked = padded_rows[source_index // picks]
        gate_out = jnp.dot(picked, gate_part, preferred_element_type=jnp.float32)
        up_out = jnp.dot(picked, up_part, preferred_element_type=jnp.float32)
        active = (jax.nn.silu(gate_out) * up_out).astype(jnp.bfloat16)
        return jnp.dot(active, down_part, preferred_element_type=jnp.float32).astype(jnp.bfloat16)
    answers = lax.map(apply_expert, (source_table, gate_weight, up_weight, down_weight))
    flat_answers = answers.reshape(EXPERTS * most_rows, -1)
    return flat_answers[slot_place].reshape(-1, picks, normed.shape[1])

def reference(glu_value, glu_gate, conv_kernel, conv_bias, group_gain, group_shift, out_weight, residual, ffn_gain, expert_pick, pair_logits, group_prob, gate_weight, up_weight, down_weight):
    mixed_rows = conv_module(glu_value, glu_gate, conv_kernel, conv_bias, group_gain, group_shift)
    projected = jnp.dot(mixed_rows, out_weight, preferred_element_type=jnp.float32)
    hidden = (residual.astype(jnp.float32) + projected).astype(jnp.bfloat16)
    hidden_full = hidden.astype(jnp.float32)
    scale_rows = lax.rsqrt(lax.optimization_barrier(jnp.mean(hidden_full * hidden_full, axis=-1, keepdims=True)) + EPS)
    normed = (hidden_full * scale_rows * ffn_gain).astype(jnp.bfloat16)
    answer = experts_apply(normed, expert_pick, gate_weight, up_weight, down_weight)
    first_share = group_prob * jax.nn.sigmoid(pair_logits[:, 0] - pair_logits[:, 1])
    second_share = group_prob * jax.nn.sigmoid(pair_logits[:, 1] - pair_logits[:, 0])
    combined = hidden_full + first_share[:, None] * answer[:, 0].astype(jnp.float32)
    combined = combined + second_share[:, None] * answer[:, 1].astype(jnp.float32)
    return combined.astype(jnp.bfloat16)
```

```python
import functools
import jax
import jax.numpy as jnp
from jax import lax
from jax.experimental import pallas as pl
from jax.experimental.pallas import tpu as pltpu
from jax.sharding import PartitionSpec as P

EPS = 1e-06
F32 = jnp.float32
BF16 = jnp.bfloat16
HALO = 32
PARTS = 4
LANE = 128
MIB = 1024 * 1024


def iota(shape, axis):
    return lax.broadcasted_iota(jnp.int32, shape, axis)


def onehot(cond):
    return jnp.where(cond, 1.0, 0.0).astype(BF16)


def call(body, out_shape, scratch=(), limit=16, smem=(), n_in=0, flops=0, moved=0, name=None):
    spec = [
        pl.BlockSpec(memory_space=pltpu.SMEM if i in smem else pltpu.VMEM) for i in range(n_in)
    ]
    multi = isinstance(out_shape, (tuple, list))
    outs = [pl.BlockSpec(memory_space=pltpu.VMEM) for _ in out_shape] if multi else pl.BlockSpec(
        memory_space=pltpu.VMEM
    )
    return pl.pallas_call(
        body,
        out_shape=out_shape,
        in_specs=spec,
        out_specs=outs,
        scratch_shapes=list(scratch),
        compiler_params=pltpu.CompilerParams(vmem_limit_bytes=limit * MIB),
        cost_estimate=pl.CostEstimate(flops=flops, bytes_accessed=moved, transcendentals=0),
        name=name,
    )


def route_body(pick, logits, prob, place, cols):
    e_iota = iota((LANE, LANE), 0)
    n_iota = iota((LANE, LANE), 1)
    picks = [pick[k : k + 1, :] for k in range(2)]
    hits = [(e_iota == p).astype(F32) for p in picks]
    both = (hits[0] + hits[1]).astype(BF16)
    before = jnp.dot(both, onehot(e_iota < n_iota), preferred_element_type=F32)
    spots = []
    for k in range(2):
        rank = jnp.sum(before * hits[k], axis=0, keepdims=True)
        spots.append(4 * picks[k] + rank.astype(jnp.int32))
        place[k : k + 1, :] = spots[k]
    first = prob[...] * jax.nn.sigmoid(logits[0:1, :] - logits[1:2, :])
    second = prob[...] * jax.nn.sigmoid(logits[1:2, :] - logits[0:1, :])
    rows = [spots[0].astype(F32), spots[1].astype(F32), first, second]
    table = jnp.zeros((LANE, LANE), F32)
    for i, row in enumerate(rows):
        table = jnp.where(e_iota == i, row, table)
    cols[...] = table.T


def conv_body(me, value, gate, halo, kernel, bias, gain, shift, mine, theirs, ext, taps, mixed):
    n_taps, width = kernel.shape
    length = value.shape[0]
    blocks = width // LANE
    for b in range(blocks):
        lanes = slice(b * LANE, (b + 1) * LANE)
        ext[b, 0:HALO, :] = halo[:, lanes].astype(F32)
        taps[b, 0:n_taps, :] = kernel[:, lanes].astype(F32)
        glued = value[:, lanes].astype(F32) * jax.nn.sigmoid(gate[:, lanes].astype(F32))
        ext[b, HALO : HALO + length, :] = glued.astype(BF16).astype(F32)
    first = HALO - (n_taps - 1)
    chunk = 32

    def block(b, carry):
        lanes = pl.ds(pl.multiple_of(b * LANE, LANE), LANE)
        g, s, c0 = gain[:, lanes], shift[:, lanes], bias[:, lanes]
        for r in range(0, length, chunk):
            acc = jnp.broadcast_to(c0, (chunk, LANE))
            for j in range(n_taps):
                at = r + first + j
                acc = acc + taps[b, j : j + 1, :] * ext[b, at : at + chunk, :]
            centre = jnp.mean(acc, axis=-1, keepdims=True)
            away = acc - centre
            variance = jnp.mean(away * away, axis=-1, keepdims=True)
            v = away * lax.rsqrt(variance + EPS) * g + s
            mixed[r : r + chunk, lanes] = (v / (1.0 + jnp.exp(-v))).astype(BF16)
        return carry

    lax.fori_loop(0, blocks, block, 0)
    half = length // 2
    mine[...] = mixed[pl.ds(pl.multiple_of(me[0] * half, half), half), :]
    theirs[...] = mixed[pl.ds(pl.multiple_of((1 - me[0]) * half, half), half), :]


def slots(stacked, place, out, part):
    tokens = place.shape[1]
    quarter = iota((LANE, tokens), 0) // 2 % PARTS
    for b in range(out.shape[0] // LANE):
        row = iota((LANE, tokens), 0) + b * LANE
        code = row // (2 * PARTS) * 4 + 2 * part + row % 2
        hit = jnp.logical_or(code == place[0:1, :], code == place[1:2, :])
        lhs = jnp.concatenate(
            [onehot(jnp.logical_and(hit, quarter == q)) for q in range(PARTS)], axis=1
        )
        out[b * LANE : (b + 1) * LANE, :] = jnp.dot(
            lhs, stacked[...], preferred_element_type=F32
        ).astype(BF16)


def project_body(me, mine, other, weight, residual, gain, place, hidden, stacked, out):
    half = mine.shape[1]
    width = residual.shape[1]
    tokens = mine.shape[0]
    step = width // PARTS
    here = pl.ds(pl.multiple_of(me[0] * half, half), half)
    there = pl.ds(pl.multiple_of((1 - me[0]) * half, half), half)
    total = jnp.zeros((tokens, 1), F32)
    for q in range(PARTS):
        lanes = slice(q * step, (q + 1) * step)
        acc = jnp.dot(mine[...], weight[here, lanes], preferred_element_type=F32)
        acc = acc + jnp.dot(other[...], weight[there, lanes], preferred_element_type=F32)
        full = (acc + residual[:, lanes].astype(F32)).astype(BF16)
        hidden[:, lanes] = full
        wide = full.astype(F32)
        total = total + jnp.sum(wide * wide, axis=-1, keepdims=True)
    scale = lax.rsqrt(total / width + EPS)
    for q in range(PARTS):
        lanes = slice(q * step, (q + 1) * step)
        stacked[q * tokens : (q + 1) * tokens, :] = (
            hidden[:, lanes].astype(F32) * scale * gain[:, lanes]
        ).astype(BF16)
    slots(stacked, place, out, 0)


def second_body(stacked, place, out):
    slots(stacked, place, out, 1)


def perm(back):
    i, j = iota((LANE, LANE), 0), iota((LANE, LANE), 1)
    if back:
        i, j = j, i
    rows = LANE // PARTS
    return onehot(j == (i % rows) // 2 * (2 * PARTS) + i // rows * 2 + i % 2)


def unpack(message, flat):
    p = perm(False)
    rows = LANE // PARTS
    step = message.shape[1]
    for b in range(message.shape[0] // LANE):
        y = jnp.dot(p, message[b * LANE : (b + 1) * LANE, :], preferred_element_type=F32).astype(BF16)
        for q in range(PARTS):
            flat[b * rows : (b + 1) * rows, q * step : (q + 1) * step] = y[q * rows : (q + 1) * rows]


def expert_body(message, gate, up, down, out, flat, answer):
    unpack(message, flat)
    x = flat[...]
    g = jnp.dot(x, gate[...], preferred_element_type=F32)
    u = jnp.dot(x, up[...], preferred_element_type=F32)
    active = (g / (1.0 + jnp.exp(-g)) * u).astype(BF16)
    answer[...] = jnp.dot(active, down[...], preferred_element_type=F32).astype(BF16)
    p = perm(True)
    rows = LANE // PARTS
    step = out.shape[1]
    for b in range(out.shape[0] // LANE):
        z = jnp.concatenate(
            [answer[b * rows : (b + 1) * rows, q * step : (q + 1) * step] for q in range(PARTS)], axis=0
        )
        out[b * LANE : (b + 1) * LANE, :] = jnp.dot(p, z, preferred_element_type=F32).astype(BF16)


def combine_body(part, message, cols, base, out, flat):
    unpack(message, flat)
    rows = flat.shape[0]
    tokens, width = out.shape
    step = width // PARTS
    slot = iota((tokens, rows), 1)
    code = (slot // 2 * 4 + 2 * part + slot % 2).astype(F32)
    picked = [onehot(cols[:, k : k + 1] == code) for k in range(2)]
    for q in range(PARTS):
        lanes = slice(q * step, (q + 1) * step)
        acc = base[:, lanes].astype(F32)
        for k in range(2):
            acc = acc + cols[:, 2 + k : 3 + k] * jnp.dot(
                picked[k], flat[:, lanes], preferred_element_type=F32
            )
        out[:, lanes] = acc.astype(out.dtype)


def local(
    glu_value,
    glu_gate,
    conv_kernel,
    conv_bias,
    group_gain,
    group_shift,
    out_weight,
    residual,
    ffn_gain,
    expert_pick,
    pair_logits,
    group_prob,
    gate_weight,
    up_weight,
    down_weight,
):
    shape = jax.ShapeDtypeStruct
    length, width = glu_value.shape
    tokens, model = residual.shape
    experts = lax.axis_size("sp") * lax.axis_size("tp")
    peers = lax.axis_size("sp")
    me = lax.axis_index("tp").astype(jnp.int32).reshape(1)

    tail = (
        glu_value[length - HALO :].astype(F32) * jax.nn.sigmoid(glu_gate[length - HALO :].astype(F32))
    ).astype(BF16)
    halo = lax.ppermute(tail, "sp", [(i, i + 1) for i in range(peers - 1)])

    place, cols = call(
        route_body,
        (shape((2, tokens), jnp.int32), shape((tokens, LANE), F32)),
        n_in=3,
        limit=4,
        flops=4_000_000,
        name="route",
    )(expert_pick.T, pair_logits.T, group_prob.reshape(1, tokens))

    mine, theirs = call(
        conv_body,
        (shape((length // 2, width), BF16), shape((length // 2, width), BF16)),
        scratch=(
            pltpu.VMEM((width // LANE, HALO + length, LANE), F32),
            pltpu.VMEM((width // LANE, 32, LANE), F32),
            pltpu.VMEM((length, width), BF16),
        ),
        smem=(0,),
        n_in=8,
        limit=8,
        flops=8_000_000,
        name="conv",
    )(
        me,
        glu_value,
        glu_gate,
        halo,
        conv_kernel,
        conv_bias.reshape(1, width),
        group_gain.reshape(1, width),
        group_shift.reshape(1, width),
    )
    other = lax.ppermute(theirs, "tp", [(0, 1), (1, 0)])

    step = model // PARTS
    rows = experts * 2 * PARTS
    message = shape((rows, step), BF16)
    hidden, stacked, send0 = call(
        project_body,
        (shape((tokens, model), BF16), shape((PARTS * tokens, step), BF16), message),
        smem=(0,),
        n_in=7,
        limit=16,
        flops=1_000_000_000,
        name="project",
    )(me, mine, other, out_weight, residual, ffn_gain.reshape(1, model), place)
    send1 = call(second_body, message, n_in=2, limit=8, flops=500_000_000, name="second")(stacked, place)

    def exchange(x):
        x = x.reshape(experts, 2 * PARTS, step)
        return lax.all_to_all(x, ("sp", "tp"), 0, 0, tiled=True).reshape(rows, step)

    expert = call(
        expert_body,
        message,
        scratch=(pltpu.VMEM((2 * experts, model), BF16), pltpu.VMEM((2 * experts, model), BF16)),
        n_in=4,
        limit=20,
        flops=2_000_000_000,
        name="expert",
    )

    def combine(part, dtype):
        return call(
            functools.partial(combine_body, part),
            shape((tokens, model), dtype),
            scratch=(pltpu.VMEM((2 * experts, model), BF16),),
            n_in=3,
            limit=12,
            flops=1_000_000_000,
            name=f"combine{part}",
        )

    with jax.named_scope("out0"):
        got0 = exchange(send0)
    with jax.named_scope("out1"):
        got1 = exchange(send1)
    done0 = expert(got0, gate_weight[0], up_weight[0], down_weight[0])
    with jax.named_scope("back0"):
        back0 = exchange(done0)
    done1 = expert(got1, gate_weight[0], up_weight[0], down_weight[0])
    with jax.named_scope("back1"):
        back1 = exchange(done1)
    acc = combine(0, F32)(back0, cols, hidden)
    return combine(1, BF16)(back1, cols, acc)


def solution(mesh):
    in_specs = (
        P("sp", "tp"),
        P("sp", "tp"),
        P(None, "tp"),
        P("tp"),
        P("tp"),
        P("tp"),
        P(),
        P(("sp", "tp"), None),
        P(),
        P(("sp", "tp"), None),
        P(("sp", "tp"), None),
        P(("sp", "tp")),
        P(("sp", "tp"), None, None),
        P(("sp", "tp"), None, None),
        P(("sp", "tp"), None, None),
    )
    out_specs = P(("sp", "tp"), None)
    return jax.shard_map(local, mesh=mesh, in_specs=in_specs, out_specs=out_specs, check_vma=False)
```

```python
import functools
import jax
import jax.numpy as jnp
from jax import lax
from jax.experimental import pallas as pl
from jax.experimental.pallas import tpu as pltpu
from jax.sharding import PartitionSpec as P

EPS = 1e-06
F32 = jnp.float32
BF16 = jnp.bfloat16
HALO = 32
PARTS = 2
RANKS = 4
LANE = 128
MIB = 1024 * 1024


def iota(shape, axis):
    return lax.broadcasted_iota(jnp.int32, shape, axis)


def onehot(cond):
    return jnp.where(cond, 1.0, 0.0).astype(BF16)


def call(body, out_shape, scratch=(), limit=16, smem=(), hbm=(), n_in=0, out_hbm=(), flops=0, name=None):
    kind = {**dict.fromkeys(smem, pltpu.SMEM), **dict.fromkeys(hbm, pltpu.HBM)}
    n_out = len(out_shape)
    run = pl.pallas_call(
        body,
        out_shape=out_shape,
        in_specs=[pl.BlockSpec(memory_space=kind.get(i, pltpu.VMEM)) for i in range(n_in)],
        out_specs=[
            pl.BlockSpec(memory_space=pltpu.HBM if i in out_hbm else pltpu.VMEM) for i in range(n_out)
        ],
        scratch_shapes=list(scratch),
        compiler_params=pltpu.CompilerParams(vmem_limit_bytes=limit * MIB),
        cost_estimate=pl.CostEstimate(flops=flops, bytes_accessed=0, transcendentals=0),
        name=name,
    )
    return lambda *args: run(
        *(pltpu.with_memory_space_constraint(a, pltpu.HBM) if i in hbm else a for i, a in enumerate(args))
    )


def fetch(sources, targets, sems):
    copies = [
        pltpu.make_async_copy(source, target, sems.at[i])
        for i, (source, target) in enumerate(zip(sources, targets, strict=True))
    ]
    for copy in copies:
        copy.start()
    return copies


def route_body(pick_in, logits_in, prob_in, place, cols, pick, logits, prob, sems):
    for copy in fetch((pick_in, logits_in, prob_in), (pick, logits, prob), sems):
        copy.wait()
    e_iota = iota((LANE, LANE), 0)
    n_iota = iota((LANE, LANE), 1)
    picks = [pick[k : k + 1, :] for k in range(2)]
    hits = [(e_iota == p).astype(F32) for p in picks]
    both = (hits[0] + hits[1]).astype(BF16)
    before = jnp.dot(both, onehot(e_iota < n_iota), preferred_element_type=F32)
    spots = []
    for k in range(2):
        rank = jnp.sum(before * hits[k], axis=0, keepdims=True)
        spots.append(4 * picks[k] + rank.astype(jnp.int32))
        place[k : k + 1, :] = spots[k]
    first = prob[...] * jax.nn.sigmoid(logits[0:1, :] - logits[1:2, :])
    second = prob[...] * jax.nn.sigmoid(logits[1:2, :] - logits[0:1, :])
    rows = [spots[0].astype(F32), spots[1].astype(F32), first, second]
    table = jnp.zeros((LANE, LANE), F32)
    for i, row in enumerate(rows):
        table = jnp.where(e_iota == i, row, table)
    cols[...] = table.T


def taps_and_norm(ext, taps, vecs, b, start, rows, n_taps):
    lanes = pl.ds(pl.multiple_of(b * LANE, LANE), LANE)
    acc = jnp.broadcast_to(vecs[0:1, lanes], (rows, LANE))
    for j in range(n_taps):
        at = start + HALO - (n_taps - 1) + j
        acc = acc + taps[b, j : j + 1, :] * ext[b, at : at + rows, :]
    centre = jnp.mean(acc, axis=-1, keepdims=True)
    away = acc - centre
    variance = jnp.mean(away * away, axis=-1, keepdims=True)
    v = away * lax.rsqrt(variance + EPS) * vecs[1:2, lanes] + vecs[2:3, lanes]
    return (v / (1.0 + jnp.exp(-v))).astype(BF16)


def conv_body(
    value_in, gate_in, kernel_in, bias_in, gain_in, shift_in, weight_in,
    rest, front, taps, vecs, weight,
    value, gate, kernel, ext, sems,
):
    n_taps, width = kernel.shape
    length = value.shape[0]
    blocks = width // LANE
    *small, large = fetch(
        (kernel_in, bias_in, gain_in, shift_in, value_in, gate_in, weight_in),
        (kernel, vecs.at[0:1], vecs.at[1:2], vecs.at[2:3], value, gate, weight),
        sems,
    )
    for copy in small:
        copy.wait()
    for b in range(blocks):
        lanes = slice(b * LANE, (b + 1) * LANE)
        taps[b, 0:n_taps, :] = kernel[:, lanes].astype(F32)
        glued = value[:, lanes].astype(F32) * jax.nn.sigmoid(gate[:, lanes].astype(F32))
        ext[b, HALO : HALO + length, :] = glued.astype(BF16).astype(F32)
        front[b, :, :] = ext[b, HALO : 2 * HALO, :]

    def block(b, carry):
        lanes = pl.ds(pl.multiple_of(b * LANE, LANE), LANE)
        for r in range(HALO, length, HALO):
            rest[r : r + HALO, lanes] = taps_and_norm(ext, taps, vecs, b, r, HALO, n_taps)
        return carry

    lax.fori_loop(0, blocks, block, 0)
    large.wait()


def head_body(me, rest, front, taps, vecs, halo, mine, theirs, ext, mixed):
    n_taps = 31
    blocks, _, _ = front.shape
    half = mine.shape[0]
    for b in range(blocks):
        lanes = slice(b * LANE, (b + 1) * LANE)
        ext[b, 0:HALO, :] = halo[:, lanes].astype(F32)
        ext[b, HALO : 2 * HALO, :] = front[b, :, :]
    for b in range(blocks):
        lanes = slice(b * LANE, (b + 1) * LANE)
        mixed[:, lanes] = taps_and_norm(ext, taps, vecs, b, 0, HALO, n_taps)

    @pl.when(me[0] == 0)
    def _():
        mine[0:HALO, :] = mixed[...]
        mine[HALO:half, :] = rest[HALO:half, :]
        theirs[...] = rest[half : 2 * half, :]

    @pl.when(me[0] != 0)
    def _():
        theirs[0:HALO, :] = mixed[...]
        theirs[HALO:half, :] = rest[HALO:half, :]
        mine[...] = rest[half : 2 * half, :]


def slots(stacked, place, out):
    tokens = place.shape[1]
    part = iota((LANE, tokens), 0) // RANKS % PARTS
    for b in range(out.shape[0] // LANE):
        row = iota((LANE, tokens), 0) + b * LANE
        code = row // (RANKS * PARTS) * RANKS + row % RANKS
        hit = jnp.logical_or(code == place[0:1, :], code == place[1:2, :])
        lhs = jnp.concatenate(
            [onehot(jnp.logical_and(hit, part == q)) for q in range(PARTS)], axis=1
        )
        out[b * LANE : (b + 1) * LANE, :] = jnp.dot(
            lhs, stacked[...], preferred_element_type=F32
        ).astype(BF16)


def project_body(me, mine, other, weight, residual, gain, place, hidden, out, stacked):
    half = mine.shape[1]
    width = residual.shape[1]
    tokens = mine.shape[0]
    step = width // PARTS
    here = pl.ds(pl.multiple_of(me[0] * half, half), half)
    there = pl.ds(pl.multiple_of((1 - me[0]) * half, half), half)
    total = jnp.zeros((tokens, 1), F32)
    for q in range(PARTS):
        lanes = slice(q * step, (q + 1) * step)
        acc = jnp.dot(mine[...], weight[here, lanes], preferred_element_type=F32)
        acc = acc + jnp.dot(other[...], weight[there, lanes], preferred_element_type=F32)
        full = (acc + residual[:, lanes].astype(F32)).astype(BF16)
        hidden[:, lanes] = full
        wide = full.astype(F32)
        total = total + jnp.sum(wide * wide, axis=-1, keepdims=True)
    scale = lax.rsqrt(total / width + EPS)
    for q in range(PARTS):
        lanes = slice(q * step, (q + 1) * step)
        stacked[q * tokens : (q + 1) * tokens, :] = (
            hidden[:, lanes].astype(F32) * scale * gain[:, lanes]
        ).astype(BF16)
    slots(stacked, place, out)


def perm(back):
    i, j = iota((LANE, LANE), 0), iota((LANE, LANE), 1)
    if back:
        i, j = j, i
    rows = LANE // PARTS
    return onehot(j == (i % rows) // RANKS * (RANKS * PARTS) + i // rows * RANKS + i % RANKS)


def unpack(message, flat):
    p = perm(False)
    rows = LANE // PARTS
    step = message.shape[1]
    for b in range(message.shape[0] // LANE):
        y = jnp.dot(p, message[b * LANE : (b + 1) * LANE, :], preferred_element_type=F32).astype(BF16)
        for q in range(PARTS):
            flat[b * rows : (b + 1) * rows, q * step : (q + 1) * step] = y[q * rows : (q + 1) * rows]


def expert_body(message, gate, up, down, out, flat, answer):
    unpack(message, flat)
    x = flat[...]
    g = jnp.dot(x, gate[...], preferred_element_type=F32)
    u = jnp.dot(x, up[...], preferred_element_type=F32)
    active = (g / (1.0 + jnp.exp(-g)) * u).astype(BF16)
    answer[...] = jnp.dot(active, down[...], preferred_element_type=F32).astype(BF16)
    p = perm(True)
    rows = LANE // PARTS
    step = out.shape[1]
    for b in range(out.shape[0] // LANE):
        z = jnp.concatenate(
            [answer[b * rows : (b + 1) * rows, q * step : (q + 1) * step] for q in range(PARTS)], axis=0
        )
        out[b * LANE : (b + 1) * LANE, :] = jnp.dot(p, z, preferred_element_type=F32).astype(BF16)


def combine_body(message, cols, base, out, flat):
    unpack(message, flat)
    rows = flat.shape[0]
    tokens, width = out.shape
    step = width // 4
    code = iota((tokens, rows), 1).astype(F32)
    picked = [onehot(cols[:, k : k + 1] == code) for k in range(2)]
    for q in range(4):
        lanes = slice(q * step, (q + 1) * step)
        acc = base[:, lanes].astype(F32)
        for k in range(2):
            acc = acc + cols[:, 2 + k : 3 + k] * jnp.dot(
                picked[k], flat[:, lanes], preferred_element_type=F32
            )
        out[:, lanes] = acc.astype(out.dtype)


def local(
    glu_value,
    glu_gate,
    conv_kernel,
    conv_bias,
    group_gain,
    group_shift,
    out_weight,
    residual,
    ffn_gain,
    expert_pick,
    pair_logits,
    group_prob,
    gate_weight,
    up_weight,
    down_weight,
):
    shape = jax.ShapeDtypeStruct
    length, width = glu_value.shape
    tokens, model = residual.shape
    experts = lax.axis_size("sp") * lax.axis_size("tp")
    peers = lax.axis_size("sp")
    me = lax.axis_index("tp").astype(jnp.int32).reshape(1)

    tail = (
        glu_value[length - HALO :].astype(F32) * jax.nn.sigmoid(glu_gate[length - HALO :].astype(F32))
    ).astype(BF16)
    halo = lax.ppermute(tail, "sp", [(i, i + 1) for i in range(peers - 1)])

    n_taps = conv_kernel.shape[0]
    blocks = width // LANE
    rest, front, taps, vecs, weight = call(
        conv_body,
        (
            shape((length, width), BF16),
            shape((blocks, HALO, LANE), F32),
            shape((blocks, 32, LANE), F32),
            shape((8, width), F32),
            shape(out_weight.shape, BF16),
        ),
        scratch=(
            pltpu.VMEM((length, width), BF16),
            pltpu.VMEM((length, width), BF16),
            pltpu.VMEM((n_taps, width), BF16),
            pltpu.VMEM((blocks, HALO + length, LANE), F32),
            pltpu.SemaphoreType.DMA((7,)),
        ),
        hbm=range(7),
        n_in=7,
        limit=8,
        flops=3_000_000_000,
        name="conv",
    )(
        glu_value,
        glu_gate,
        conv_kernel,
        conv_bias.reshape(1, width),
        group_gain.reshape(1, width),
        group_shift.reshape(1, width),
        out_weight,
    )
    mine, theirs = call(
        head_body,
        (shape((length // 2, width), BF16), shape((length // 2, width), BF16)),
        scratch=(pltpu.VMEM((blocks, 2 * HALO, LANE), F32), pltpu.VMEM((HALO, width), BF16)),
        smem=(0,),
        n_in=6,
        limit=4,
        flops=500_000_000,
        name="head",
    )(me, rest, front, taps, vecs, halo)
    place, cols = call(
        route_body,
        (shape((2, tokens), jnp.int32), shape((tokens, LANE), F32)),
        scratch=(
            pltpu.VMEM((2, tokens), jnp.int32),
            pltpu.VMEM((2, tokens), F32),
            pltpu.VMEM((1, tokens), F32),
            pltpu.SemaphoreType.DMA((3,)),
        ),
        hbm=range(3),
        n_in=3,
        limit=4,
        flops=500_000_000,
        name="route",
    )(expert_pick.T, pair_logits.T, group_prob.reshape(1, tokens))
    other = lax.ppermute(theirs, "tp", [(0, 1), (1, 0)])

    step = model // PARTS
    rows = experts * RANKS * PARTS
    message = shape((rows, step), BF16)
    flat = pltpu.VMEM((RANKS * experts, model), BF16)
    hidden, send = call(
        project_body,
        (shape((tokens, model), BF16), message),
        scratch=(pltpu.VMEM((PARTS * tokens, step), BF16),),
        smem=(0,),
        n_in=7,
        limit=16,
        flops=1_000_000_000,
        name="project",
    )(me, mine, other, weight, residual, ffn_gain.reshape(1, model), place)

    def exchange(x):
        x = x.reshape(experts, RANKS * PARTS, step)
        return lax.all_to_all(x, ("sp", "tp"), 0, 0, tiled=True).reshape(rows, step)

    got = exchange(send)
    (done,) = call(
        expert_body,
        (message,),
        scratch=(flat, flat),
        n_in=4,
        limit=24,
        flops=4_000_000_000,
        name="expert",
    )(got, gate_weight[0], up_weight[0], down_weight[0])
    back = exchange(done)
    (result,) = call(
        combine_body,
        (shape((tokens, model), BF16),),
        scratch=(flat,),
        n_in=3,
        limit=12,
        flops=1_000_000_000,
        name="combine",
    )(back, cols, hidden)
    return result


def solution(mesh):
    in_specs = (
        P("sp", "tp"),
        P("sp", "tp"),
        P(None, "tp"),
        P("tp"),
        P("tp"),
        P("tp"),
        P(),
        P(("sp", "tp"), None),
        P(),
        P(("sp", "tp"), None),
        P(("sp", "tp"), None),
        P(("sp", "tp")),
        P(("sp", "tp"), None, None),
        P(("sp", "tp"), None, None),
        P(("sp", "tp"), None, None),
    )
    out_specs = P(("sp", "tp"), None)
    return jax.shard_map(local, mesh=mesh, in_specs=in_specs, out_specs=out_specs, check_vma=False)
```

```python
import functools
import jax
import jax.numpy as jnp
from jax import lax
from jax.experimental import pallas as pl
from jax.experimental.pallas import tpu as pltpu
from jax.sharding import PartitionSpec as P

EPS = 1e-06
F32 = jnp.float32
BF16 = jnp.bfloat16
HALO = 32
PARTS = 2
RANKS = 4
LANE = 128
MIB = 1024 * 1024


def iota(shape, axis):
    return lax.broadcasted_iota(jnp.int32, shape, axis)


def onehot(cond):
    return jnp.where(cond, 1.0, 0.0).astype(BF16)


def call(body, out_shape, scratch=(), limit=16, smem=(), hbm=(), n_in=0, out_hbm=(), flops=0, name=None):
    kind = {**dict.fromkeys(smem, pltpu.SMEM), **dict.fromkeys(hbm, pltpu.HBM)}
    n_out = len(out_shape)
    run = pl.pallas_call(
        body,
        out_shape=out_shape,
        in_specs=[pl.BlockSpec(memory_space=kind.get(i, pltpu.VMEM)) for i in range(n_in)],
        out_specs=[
            pl.BlockSpec(memory_space=pltpu.HBM if i in out_hbm else pltpu.VMEM) for i in range(n_out)
        ],
        scratch_shapes=list(scratch),
        compiler_params=pltpu.CompilerParams(vmem_limit_bytes=limit * MIB),
        cost_estimate=pl.CostEstimate(flops=flops, bytes_accessed=0, transcendentals=0),
        name=name,
    )
    return lambda *args: run(
        *(pltpu.with_memory_space_constraint(a, pltpu.HBM) if i in hbm else a for i, a in enumerate(args))
    )


def fetch(sources, targets, sems):
    copies = [
        pltpu.make_async_copy(source, target, sems.at[i])
        for i, (source, target) in enumerate(zip(sources, targets, strict=True))
    ]
    for copy in copies:
        copy.start()
    return copies


def route_body(pick_in, logits_in, prob_in, place, cols, pick, logits, prob, sems):
    for copy in fetch((pick_in, logits_in, prob_in), (pick, logits, prob), sems):
        copy.wait()
    e_iota = iota((LANE, LANE), 0)
    n_iota = iota((LANE, LANE), 1)
    picks = [pick[k : k + 1, :] for k in range(2)]
    hits = [(e_iota == p).astype(F32) for p in picks]
    both = (hits[0] + hits[1]).astype(BF16)
    before = jnp.dot(both, onehot(e_iota < n_iota), preferred_element_type=F32)
    spots = []
    for k in range(2):
        rank = jnp.sum(before * hits[k], axis=0, keepdims=True)
        spots.append(4 * picks[k] + rank.astype(jnp.int32))
        place[k : k + 1, :] = spots[k]
    first = prob[...] * jax.nn.sigmoid(logits[0:1, :] - logits[1:2, :])
    second = prob[...] * jax.nn.sigmoid(logits[1:2, :] - logits[0:1, :])
    rows = [spots[0].astype(F32), spots[1].astype(F32), first, second]
    table = jnp.zeros((LANE, LANE), F32)
    for i, row in enumerate(rows):
        table = jnp.where(e_iota == i, row, table)
    cols[...] = table.T


def taps_and_norm(ext, taps, vecs, b, start, rows, n_taps):
    lanes = pl.ds(pl.multiple_of(b * LANE, LANE), LANE)
    acc = jnp.broadcast_to(vecs[0:1, lanes], (rows, LANE))
    for j in range(n_taps):
        at = start + HALO - (n_taps - 1) + j
        acc = acc + taps[b, j : j + 1, :] * ext[b, at : at + rows, :]
    centre = jnp.mean(acc, axis=-1, keepdims=True)
    away = acc - centre
    variance = jnp.mean(away * away, axis=-1, keepdims=True)
    v = away * lax.rsqrt(variance + EPS) * vecs[1:2, lanes] + vecs[2:3, lanes]
    return (v / (1.0 + jnp.exp(-v))).astype(BF16)


def conv_body(
    _, value_in, gate_in, kernel_in, bias_in, gain_in, shift_in, weight_in,
    rest, front, taps, vecs, weight,
    value, gate, kernel, ext, sems,
):
    n_taps, width = kernel.shape
    length = value.shape[0]
    blocks = width // LANE
    *small, large = fetch(
        (kernel_in, bias_in, gain_in, shift_in, value_in, gate_in, weight_in),
        (kernel, vecs.at[0:1], vecs.at[1:2], vecs.at[2:3], value, gate, weight),
        sems,
    )
    for copy in small:
        copy.wait()
    for b in range(blocks):
        lanes = slice(b * LANE, (b + 1) * LANE)
        taps[b, 0:n_taps, :] = kernel[:, lanes].astype(F32)
        glued = value[:, lanes].astype(F32) * jax.nn.sigmoid(gate[:, lanes].astype(F32))
        ext[b, HALO : HALO + length, :] = glued.astype(BF16).astype(F32)
        front[b, :, :] = ext[b, HALO : 2 * HALO, :]

    def block(b, carry):
        lanes = pl.ds(pl.multiple_of(b * LANE, LANE), LANE)
        for r in range(HALO, length, HALO):
            rest[r : r + HALO, lanes] = taps_and_norm(ext, taps, vecs, b, r, HALO, n_taps)
        return carry

    lax.fori_loop(0, blocks, block, 0)
    large.wait()


def head_body(me, rest, front, taps, vecs, halo, mine, theirs, ext, mixed):
    n_taps = 31
    blocks, _, _ = front.shape
    half = mine.shape[0]
    for b in range(blocks):
        lanes = slice(b * LANE, (b + 1) * LANE)
        ext[b, 0:HALO, :] = jnp.where(me[1] > 0, halo[:, lanes].astype(F32), 0.0)
        ext[b, HALO : 2 * HALO, :] = front[b, :, :]
    for b in range(blocks):
        lanes = slice(b * LANE, (b + 1) * LANE)
        mixed[:, lanes] = taps_and_norm(ext, taps, vecs, b, 0, HALO, n_taps)

    @pl.when(me[0] == 0)
    def _():
        mine[0:HALO, :] = mixed[...]
        mine[HALO:half, :] = rest[HALO:half, :]
        theirs[...] = rest[half : 2 * half, :]

    @pl.when(me[0] != 0)
    def _():
        theirs[0:HALO, :] = mixed[...]
        theirs[HALO:half, :] = rest[HALO:half, :]
        mine[...] = rest[half : 2 * half, :]


def slots(stacked, place, out):
    tokens = place.shape[1]
    part = iota((LANE, tokens), 0) // RANKS % PARTS
    for b in range(out.shape[0] // LANE):
        row = iota((LANE, tokens), 0) + b * LANE
        code = row // (RANKS * PARTS) * RANKS + row % RANKS
        hit = jnp.logical_or(code == place[0:1, :], code == place[1:2, :])
        lhs = jnp.concatenate(
            [onehot(jnp.logical_and(hit, part == q)) for q in range(PARTS)], axis=1
        )
        out[b * LANE : (b + 1) * LANE, :] = jnp.dot(
            lhs, stacked[...], preferred_element_type=F32
        ).astype(BF16)


def project_body(me, mine, other, weight, residual, gain, place, hidden, out, stacked):
    half = mine.shape[1]
    width = residual.shape[1]
    tokens = mine.shape[0]
    step = width // PARTS
    here = pl.ds(pl.multiple_of(me[0] * half, half), half)
    there = pl.ds(pl.multiple_of((1 - me[0]) * half, half), half)
    total = jnp.zeros((tokens, 1), F32)
    for q in range(PARTS):
        lanes = slice(q * step, (q + 1) * step)
        acc = jnp.dot(mine[...], weight[here, lanes], preferred_element_type=F32)
        acc = acc + jnp.dot(other[...], weight[there, lanes], preferred_element_type=F32)
        full = (acc + residual[:, lanes].astype(F32)).astype(BF16)
        hidden[:, lanes] = full
        wide = full.astype(F32)
        total = total + jnp.sum(wide * wide, axis=-1, keepdims=True)
    scale = lax.rsqrt(total / width + EPS)
    for q in range(PARTS):
        lanes = slice(q * step, (q + 1) * step)
        stacked[q * tokens : (q + 1) * tokens, :] = (
            hidden[:, lanes].astype(F32) * scale * gain[:, lanes]
        ).astype(BF16)
    slots(stacked, place, out)


def perm(back):
    i, j = iota((LANE, LANE), 0), iota((LANE, LANE), 1)
    if back:
        i, j = j, i
    rows = LANE // PARTS
    return onehot(j == (i % rows) // RANKS * (RANKS * PARTS) + i // rows * RANKS + i % RANKS)


def unpack(message, flat):
    p = perm(False)
    rows = LANE // PARTS
    step = message.shape[1]
    for b in range(message.shape[0] // LANE):
        y = jnp.dot(p, message[b * LANE : (b + 1) * LANE, :], preferred_element_type=F32).astype(BF16)
        for q in range(PARTS):
            flat[b * rows : (b + 1) * rows, q * step : (q + 1) * step] = y[q * rows : (q + 1) * rows]


def expert_body(message, gate, up, down, out, flat, answer):
    unpack(message, flat)
    x = flat[...]
    g = jnp.dot(x, gate[...], preferred_element_type=F32)
    u = jnp.dot(x, up[...], preferred_element_type=F32)
    active = (g / (1.0 + jnp.exp(-g)) * u).astype(BF16)
    answer[...] = jnp.dot(active, down[...], preferred_element_type=F32).astype(BF16)
    p = perm(True)
    rows = LANE // PARTS
    step = out.shape[1]
    for b in range(out.shape[0] // LANE):
        z = jnp.concatenate(
            [answer[b * rows : (b + 1) * rows, q * step : (q + 1) * step] for q in range(PARTS)], axis=0
        )
        out[b * LANE : (b + 1) * LANE, :] = jnp.dot(p, z, preferred_element_type=F32).astype(BF16)


def combine_body(message, cols, base, out, flat):
    unpack(message, flat)
    rows = flat.shape[0]
    tokens, width = out.shape
    step = width // 4
    code = iota((tokens, rows), 1).astype(F32)
    picked = [onehot(cols[:, k : k + 1] == code) for k in range(2)]
    for q in range(4):
        lanes = slice(q * step, (q + 1) * step)
        acc = base[:, lanes].astype(F32)
        for k in range(2):
            acc = acc + cols[:, 2 + k : 3 + k] * jnp.dot(
                picked[k], flat[:, lanes], preferred_element_type=F32
            )
        out[:, lanes] = acc.astype(out.dtype)


def local(
    glu_value,
    glu_gate,
    conv_kernel,
    conv_bias,
    group_gain,
    group_shift,
    out_weight,
    residual,
    ffn_gain,
    expert_pick,
    pair_logits,
    group_prob,
    gate_weight,
    up_weight,
    down_weight,
):
    shape = jax.ShapeDtypeStruct
    length, width = glu_value.shape
    tokens, model = residual.shape
    experts = lax.axis_size("sp") * lax.axis_size("tp")
    peers = lax.axis_size("sp")
    me = jnp.stack([lax.axis_index("tp"), lax.axis_index("sp")]).astype(jnp.int32)

    tail = (
        glu_value[length - HALO :].astype(F32) * jax.nn.sigmoid(glu_gate[length - HALO :].astype(F32))
    ).astype(BF16)
    halo = lax.ppermute(tail, "sp", [(i, (i + 1) % peers) for i in range(peers)])

    n_taps = conv_kernel.shape[0]
    blocks = width // LANE
    rest, front, taps, vecs, weight = call(
        conv_body,
        (
            shape((length, width), BF16),
            shape((blocks, HALO, LANE), F32),
            shape((blocks, 32, LANE), F32),
            shape((8, width), F32),
            shape(out_weight.shape, BF16),
        ),
        scratch=(
            pltpu.VMEM((length, width), BF16),
            pltpu.VMEM((length, width), BF16),
            pltpu.VMEM((n_taps, width), BF16),
            pltpu.VMEM((blocks, HALO + length, LANE), F32),
            pltpu.SemaphoreType.DMA((7,)),
        ),
        smem=(0,),
        hbm=range(1, 8),
        n_in=8,
        limit=8,
        flops=3_000_000_000,
        name="conv",
    )(
        me,
        glu_value,
        glu_gate,
        conv_kernel,
        conv_bias.reshape(1, width),
        group_gain.reshape(1, width),
        group_shift.reshape(1, width),
        out_weight,
    )
    mine, theirs = call(
        head_body,
        (shape((length // 2, width), BF16), shape((length // 2, width), BF16)),
        scratch=(pltpu.VMEM((blocks, 2 * HALO, LANE), F32), pltpu.VMEM((HALO, width), BF16)),
        smem=(0,),
        n_in=6,
        limit=4,
        flops=500_000_000,
        name="head",
    )(me, rest, front, taps, vecs, halo)
    place, cols = call(
        route_body,
        (shape((2, tokens), jnp.int32), shape((tokens, LANE), F32)),
        scratch=(
            pltpu.VMEM((2, tokens), jnp.int32),
            pltpu.VMEM((2, tokens), F32),
            pltpu.VMEM((1, tokens), F32),
            pltpu.SemaphoreType.DMA((3,)),
        ),
        hbm=range(3),
        n_in=3,
        limit=4,
        flops=500_000_000,
        name="route",
    )(expert_pick.T, pair_logits.T, group_prob.reshape(1, tokens))
    other = lax.ppermute(theirs, "tp", [(0, 1), (1, 0)])

    step = model // PARTS
    rows = experts * RANKS * PARTS
    message = shape((rows, step), BF16)
    flat = pltpu.VMEM((RANKS * experts, model), BF16)
    hidden, send = call(
        project_body,
        (shape((tokens, model), BF16), message),
        scratch=(pltpu.VMEM((PARTS * tokens, step), BF16),),
        smem=(0,),
        n_in=7,
        limit=16,
        flops=1_000_000_000,
        name="project",
    )(me, mine, other, weight, residual, ffn_gain.reshape(1, model), place)

    def exchange(x):
        x = x.reshape(experts, RANKS * PARTS, step)
        return lax.all_to_all(x, ("sp", "tp"), 0, 0, tiled=True).reshape(rows, step)

    got = exchange(send)
    (done,) = call(
        expert_body,
        (message,),
        scratch=(flat, flat),
        n_in=4,
        limit=24,
        flops=4_000_000_000,
        name="expert",
    )(got, gate_weight[0], up_weight[0], down_weight[0])
    back = exchange(done)
    (result,) = call(
        combine_body,
        (shape((tokens, model), BF16),),
        scratch=(flat,),
        n_in=3,
        limit=12,
        flops=1_000_000_000,
        name="combine",
    )(back, cols, hidden)
    return result


def solution(mesh):
    in_specs = (
        P("sp", "tp"),
        P("sp", "tp"),
        P(None, "tp"),
        P("tp"),
        P("tp"),
        P("tp"),
        P(),
        P(("sp", "tp"), None),
        P(),
        P(("sp", "tp"), None),
        P(("sp", "tp"), None),
        P(("sp", "tp")),
        P(("sp", "tp"), None, None),
        P(("sp", "tp"), None, None),
        P(("sp", "tp"), None, None),
    )
    out_specs = P(("sp", "tp"), None)
    return jax.shard_map(local, mesh=mesh, in_specs=in_specs, out_specs=out_specs, check_vma=False)
```

```python
import functools
import jax
import jax.numpy as jnp
from jax import lax
from jax.experimental import pallas as pl
from jax.experimental.pallas import tpu as pltpu
from jax.sharding import PartitionSpec as P

EPS = 1e-06
F32 = jnp.float32
BF16 = jnp.bfloat16
HALO = 32
PARTS = 2
RANKS = 4
LANE = 128
MIB = 1024 * 1024


def iota(shape, axis):
    return lax.broadcasted_iota(jnp.int32, shape, axis)


def onehot(cond):
    return jnp.where(cond, 1.0, 0.0).astype(BF16)


def call(body, out_shape, scratch=(), limit=16, smem=(), hbm=(), n_in=0, out_hbm=(), flops=0, name=None):
    kind = {**dict.fromkeys(smem, pltpu.SMEM), **dict.fromkeys(hbm, pltpu.HBM)}
    n_out = len(out_shape)
    run = pl.pallas_call(
        body,
        out_shape=out_shape,
        in_specs=[pl.BlockSpec(memory_space=kind.get(i, pltpu.VMEM)) for i in range(n_in)],
        out_specs=[
            pl.BlockSpec(memory_space=pltpu.HBM if i in out_hbm else pltpu.VMEM) for i in range(n_out)
        ],
        scratch_shapes=list(scratch),
        compiler_params=pltpu.CompilerParams(vmem_limit_bytes=limit * MIB),
        cost_estimate=pl.CostEstimate(flops=flops, bytes_accessed=0, transcendentals=0),
        name=name,
    )
    return lambda *args: run(
        *(pltpu.with_memory_space_constraint(a, pltpu.HBM) if i in hbm else a for i, a in enumerate(args))
    )


def fetch(sources, targets, sems):
    copies = [
        pltpu.make_async_copy(source, target, sems.at[i])
        for i, (source, target) in enumerate(zip(sources, targets, strict=True))
    ]
    for copy in copies:
        copy.start()
    return copies


def route_body(pick_in, logits_in, prob_in, place, cols, pick, logits, prob, sems):
    for copy in fetch((pick_in, logits_in, prob_in), (pick, logits, prob), sems):
        copy.wait()
    e_iota = iota((LANE, LANE), 0)
    n_iota = iota((LANE, LANE), 1)
    picks = [pick[k : k + 1, :] for k in range(2)]
    hits = [(e_iota == p).astype(F32) for p in picks]
    both = (hits[0] + hits[1]).astype(BF16)
    before = jnp.dot(both, onehot(e_iota < n_iota), preferred_element_type=F32)
    spots = []
    for k in range(2):
        rank = jnp.sum(before * hits[k], axis=0, keepdims=True)
        spots.append(4 * picks[k] + rank.astype(jnp.int32))
        place[k : k + 1, :] = spots[k]
    first = prob[...] * jax.nn.sigmoid(logits[0:1, :] - logits[1:2, :])
    second = prob[...] * jax.nn.sigmoid(logits[1:2, :] - logits[0:1, :])
    rows = [spots[0].astype(F32), spots[1].astype(F32), first, second]
    table = jnp.zeros((LANE, LANE), F32)
    for i, row in enumerate(rows):
        table = jnp.where(e_iota == i, row, table)
    cols[...] = table.T


def taps_and_norm(ext, taps, vecs, b, start, rows, n_taps):
    lanes = pl.ds(pl.multiple_of(b * LANE, LANE), LANE)
    acc = jnp.broadcast_to(vecs[0:1, lanes], (rows, LANE))
    for j in range(n_taps):
        at = start + HALO - (n_taps - 1) + j
        acc = acc + taps[b, j : j + 1, :] * ext[b, at : at + rows, :]
    centre = jnp.mean(acc, axis=-1, keepdims=True)
    away = acc - centre
    variance = jnp.mean(away * away, axis=-1, keepdims=True)
    v = away * lax.rsqrt(variance + EPS) * vecs[1:2, lanes] + vecs[2:3, lanes]
    return (v / (1.0 + jnp.exp(-v))).astype(BF16)


def conv_body(
    _, value_in, gate_in, kernel_in, bias_in, gain_in, shift_in, weight_in,
    rest, front, taps, vecs, weight,
    value, gate, kernel, ext, sems,
):
    n_taps, width = kernel.shape
    length = value.shape[0]
    blocks = width // LANE
    small = fetch(
        (value_in, gate_in, kernel_in, bias_in, gain_in, shift_in),
        (value, gate, kernel, vecs.at[0:1], vecs.at[1:2], vecs.at[2:3]),
        sems,
    )
    for copy in small:
        copy.wait()
    large = pltpu.make_async_copy(weight_in, weight, sems.at[len(small)])
    large.start()
    for b in range(blocks):
        lanes = slice(b * LANE, (b + 1) * LANE)
        taps[b, 0:n_taps, :] = kernel[:, lanes].astype(F32)
        glued = value[:, lanes].astype(F32) * jax.nn.sigmoid(gate[:, lanes].astype(F32))
        ext[b, HALO : HALO + length, :] = glued.astype(BF16).astype(F32)
        front[b, :, :] = ext[b, HALO : 2 * HALO, :]

    def block(b, carry):
        lanes = pl.ds(pl.multiple_of(b * LANE, LANE), LANE)
        for r in range(HALO, length, HALO):
            rest[r : r + HALO, lanes] = taps_and_norm(ext, taps, vecs, b, r, HALO, n_taps)
        return carry

    lax.fori_loop(0, blocks, block, 0)
    large.wait()


def head_body(cores, me, rest, front, taps, vecs, halo, mine, theirs, ext, mixed):
    n_taps = 31
    blocks, _, _ = front.shape
    half = mine.shape[0]
    for b in range(blocks):
        lanes = slice(b * LANE, (b + 1) * LANE)
        ext[b, 0:HALO, :] = jnp.where(me[0] >= cores, halo[:, lanes].astype(F32), 0.0)
        ext[b, HALO : 2 * HALO, :] = front[b, :, :]
    for b in range(blocks):
        lanes = slice(b * LANE, (b + 1) * LANE)
        mixed[:, lanes] = taps_and_norm(ext, taps, vecs, b, 0, HALO, n_taps)

    core = lax.rem(me[0], cores)

    @pl.when(core == 0)
    def _():
        mine[0:HALO, :] = mixed[...]
        mine[HALO:half, :] = rest[HALO:half, :]
        theirs[...] = rest[half : 2 * half, :]

    @pl.when(core != 0)
    def _():
        theirs[0:HALO, :] = mixed[...]
        theirs[HALO:half, :] = rest[HALO:half, :]
        mine[...] = rest[half : 2 * half, :]


def slots(stacked, place, out):
    tokens = place.shape[1]
    part = iota((LANE, tokens), 0) // RANKS % PARTS
    for b in range(out.shape[0] // LANE):
        row = iota((LANE, tokens), 0) + b * LANE
        code = row // (RANKS * PARTS) * RANKS + row % RANKS
        hit = jnp.logical_or(code == place[0:1, :], code == place[1:2, :])
        lhs = jnp.concatenate(
            [onehot(jnp.logical_and(hit, part == q)) for q in range(PARTS)], axis=1
        )
        out[b * LANE : (b + 1) * LANE, :] = jnp.dot(
            lhs, stacked[...], preferred_element_type=F32
        ).astype(BF16)


def project_body(cores, me, mine, other, weight, residual, gain, place, hidden, out, stacked):
    half = mine.shape[1]
    width = residual.shape[1]
    tokens = mine.shape[0]
    step = width // PARTS
    core = lax.rem(me[0], cores)
    here = pl.ds(pl.multiple_of(core * half, half), half)
    there = pl.ds(pl.multiple_of((1 - core) * half, half), half)
    total = jnp.zeros((tokens, 1), F32)
    for q in range(PARTS):
        lanes = slice(q * step, (q + 1) * step)
        acc = jnp.dot(mine[...], weight[here, lanes], preferred_element_type=F32)
        acc = acc + jnp.dot(other[...], weight[there, lanes], preferred_element_type=F32)
        full = (acc + residual[:, lanes].astype(F32)).astype(BF16)
        hidden[:, lanes] = full
        wide = full.astype(F32)
        total = total + jnp.sum(wide * wide, axis=-1, keepdims=True)
    scale = lax.rsqrt(total / width + EPS)
    for q in range(PARTS):
        lanes = slice(q * step, (q + 1) * step)
        stacked[q * tokens : (q + 1) * tokens, :] = (
            hidden[:, lanes].astype(F32) * scale * gain[:, lanes]
        ).astype(BF16)
    slots(stacked, place, out)


def perm(back):
    i, j = iota((LANE, LANE), 0), iota((LANE, LANE), 1)
    if back:
        i, j = j, i
    rows = LANE // PARTS
    return onehot(j == (i % rows) // RANKS * (RANKS * PARTS) + i // rows * RANKS + i % RANKS)


def unpack(message, flat):
    p = perm(False)
    rows = LANE // PARTS
    step = message.shape[1]
    for b in range(message.shape[0] // LANE):
        y = jnp.dot(p, message[b * LANE : (b + 1) * LANE, :], preferred_element_type=F32).astype(BF16)
        for q in range(PARTS):
            flat[b * rows : (b + 1) * rows, q * step : (q + 1) * step] = y[q * rows : (q + 1) * rows]


def expert_body(message, gate, up, down, out, flat, answer):
    unpack(message, flat)
    x = flat[...]
    g = jnp.dot(x, gate[...], preferred_element_type=F32)
    u = jnp.dot(x, up[...], preferred_element_type=F32)
    active = (g / (1.0 + jnp.exp(-g)) * u).astype(BF16)
    answer[...] = jnp.dot(active, down[...], preferred_element_type=F32).astype(BF16)
    p = perm(True)
    rows = LANE // PARTS
    step = out.shape[1]
    for b in range(out.shape[0] // LANE):
        z = jnp.concatenate(
            [answer[b * rows : (b + 1) * rows, q * step : (q + 1) * step] for q in range(PARTS)], axis=0
        )
        out[b * LANE : (b + 1) * LANE, :] = jnp.dot(p, z, preferred_element_type=F32).astype(BF16)


def combine_body(message, cols, base, out_hbm, out, sems):
    tokens, width = out.shape
    rows, step = message.shape
    slot = iota((tokens, rows), 1)
    code = (slot // (RANKS * PARTS) * RANKS + slot % RANKS).astype(F32)
    share = jnp.where(cols[:, 0:1] == code, cols[:, 2:3], 0.0)
    share = jnp.where(cols[:, 1:2] == code, cols[:, 3:4], share)
    part = slot // RANKS % PARTS
    picked = jnp.concatenate(
        [jnp.where(part == q, share, 0.0).astype(BF16) for q in range(PARTS)], axis=0
    )
    pieces = 4
    size = step // pieces
    copies = []
    for p in range(pieces):
        got = jnp.dot(picked, message[:, p * size : (p + 1) * size], preferred_element_type=F32)
        for q in range(PARTS):
            lanes = slice(q * step + p * size, q * step + (p + 1) * size)
            out[:, lanes] = (base[:, lanes].astype(F32) + got[q * tokens : (q + 1) * tokens]).astype(BF16)
            copy = pltpu.make_async_copy(
                out.at[:, lanes], out_hbm.at[:, lanes], sems.at[p * PARTS + q]
            )
            copy.start()
            copies.append(copy)
    for copy in copies:
        copy.wait()


def local(
    glu_value,
    glu_gate,
    conv_kernel,
    conv_bias,
    group_gain,
    group_shift,
    out_weight,
    residual,
    ffn_gain,
    expert_pick,
    pair_logits,
    group_prob,
    gate_weight,
    up_weight,
    down_weight,
):
    shape = jax.ShapeDtypeStruct
    length, width = glu_value.shape
    tokens, model = residual.shape
    experts = lax.axis_size("sp") * lax.axis_size("tp")
    peers = lax.axis_size("sp")
    me = lax.axis_index(("sp", "tp")).astype(jnp.int32).reshape(1)

    tail = (
        glu_value[length - HALO :].astype(F32) * jax.nn.sigmoid(glu_gate[length - HALO :].astype(F32))
    ).astype(BF16)
    halo = lax.ppermute(tail, "sp", [(i, (i + 1) % peers) for i in range(peers)])

    n_taps = conv_kernel.shape[0]
    blocks = width // LANE
    rest, front, taps, vecs, weight = call(
        conv_body,
        (
            shape((length, width), BF16),
            shape((blocks, HALO, LANE), F32),
            shape((blocks, 32, LANE), F32),
            shape((8, width), F32),
            shape(out_weight.shape, BF16),
        ),
        scratch=(
            pltpu.VMEM((length, width), BF16),
            pltpu.VMEM((length, width), BF16),
            pltpu.VMEM((n_taps, width), BF16),
            pltpu.VMEM((blocks, HALO + length, LANE), F32),
            pltpu.SemaphoreType.DMA((7,)),
        ),
        smem=(0,),
        hbm=range(1, 8),
        n_in=8,
        limit=8,
        flops=3_000_000_000,
        name="conv",
    )(
        me,
        glu_value,
        glu_gate,
        conv_kernel,
        conv_bias.reshape(1, width),
        group_gain.reshape(1, width),
        group_shift.reshape(1, width),
        out_weight,
    )
    mine, theirs = call(
        functools.partial(head_body, lax.axis_size("tp")),
        (shape((length // 2, width), BF16), shape((length // 2, width), BF16)),
        scratch=(pltpu.VMEM((blocks, 2 * HALO, LANE), F32), pltpu.VMEM((HALO, width), BF16)),
        smem=(0,),
        n_in=6,
        limit=4,
        flops=500_000_000,
        name="head",
    )(me, rest, front, taps, vecs, halo)
    place, cols = call(
        route_body,
        (shape((2, tokens), jnp.int32), shape((tokens, LANE), F32)),
        scratch=(
            pltpu.VMEM((2, tokens), jnp.int32),
            pltpu.VMEM((2, tokens), F32),
            pltpu.VMEM((1, tokens), F32),
            pltpu.SemaphoreType.DMA((3,)),
        ),
        hbm=range(3),
        n_in=3,
        limit=4,
        flops=500_000_000,
        name="route",
    )(expert_pick.T, pair_logits.T, group_prob.reshape(1, tokens))
    other = lax.ppermute(theirs, "tp", [(0, 1), (1, 0)])

    step = model // PARTS
    rows = experts * RANKS * PARTS
    message = shape((rows, step), BF16)
    flat = pltpu.VMEM((RANKS * experts, model), BF16)
    hidden, send = call(
        functools.partial(project_body, lax.axis_size("tp")),
        (shape((tokens, model), BF16), message),
        scratch=(pltpu.VMEM((PARTS * tokens, step), BF16),),
        smem=(0,),
        n_in=7,
        limit=16,
        flops=1_000_000_000,
        name="project",
    )(me, mine, other, weight, residual, ffn_gain.reshape(1, model), place)

    def exchange(x):
        x = x.reshape(experts, RANKS * PARTS, step)
        return lax.all_to_all(x, ("sp", "tp"), 0, 0, tiled=True).reshape(rows, step)

    got = exchange(send)
    (done,) = call(
        expert_body,
        (message,),
        scratch=(flat, flat),
        n_in=4,
        limit=24,
        flops=4_000_000_000,
        name="expert",
    )(got, gate_weight[0], up_weight[0], down_weight[0])
    back = exchange(done)
    (result,) = call(
        combine_body,
        (shape((tokens, model), BF16),),
        scratch=(pltpu.VMEM((tokens, model), BF16), pltpu.SemaphoreType.DMA((8,))),
        n_in=3,
        out_hbm=(0,),
        limit=12,
        flops=1_000_000_000,
        name="combine",
    )(back, cols, hidden)
    return result


def solution(mesh):
    in_specs = (
        P("sp", "tp"),
        P("sp", "tp"),
        P(None, "tp"),
        P("tp"),
        P("tp"),
        P("tp"),
        P(),
        P(("sp", "tp"), None),
        P(),
        P(("sp", "tp"), None),
        P(("sp", "tp"), None),
        P(("sp", "tp")),
        P(("sp", "tp"), None, None),
        P(("sp", "tp"), None, None),
        P(("sp", "tp"), None, None),
    )
    out_specs = P(("sp", "tp"), None)
    return jax.shard_map(local, mesh=mesh, in_specs=in_specs, out_specs=out_specs, check_vma=False)
```

```python
import functools
import jax
import jax.numpy as jnp
from jax import lax
from jax.experimental import pallas as pl
from jax.experimental.pallas import tpu as pltpu
from jax.sharding import PartitionSpec as P

EPS = 1e-06
F32 = jnp.float32
BF16 = jnp.bfloat16
HALO = 32
PARTS = 2
RANKS = 4
LANE = 128
MIB = 1024 * 1024


def iota(shape, axis):
    return lax.broadcasted_iota(jnp.int32, shape, axis)


def onehot(cond):
    return jnp.where(cond, 1.0, 0.0).astype(BF16)


def call(body, out_shape, scratch=(), limit=16, smem=(), hbm=(), n_in=0, out_hbm=(), flops=0, name=None):
    kind = {**dict.fromkeys(smem, pltpu.SMEM), **dict.fromkeys(hbm, pltpu.HBM)}
    n_out = len(out_shape)
    run = pl.pallas_call(
        body,
        out_shape=out_shape,
        in_specs=[pl.BlockSpec(memory_space=kind.get(i, pltpu.VMEM)) for i in range(n_in)],
        out_specs=[
            pl.BlockSpec(memory_space=pltpu.HBM if i in out_hbm else pltpu.VMEM) for i in range(n_out)
        ],
        scratch_shapes=list(scratch),
        compiler_params=pltpu.CompilerParams(vmem_limit_bytes=limit * MIB),
        cost_estimate=pl.CostEstimate(flops=flops, bytes_accessed=0, transcendentals=0),
        name=name,
    )
    return lambda *args: run(
        *(pltpu.with_memory_space_constraint(a, pltpu.HBM) if i in hbm else a for i, a in enumerate(args))
    )


def fetch(sources, targets, sems):
    copies = [
        pltpu.make_async_copy(source, target, sems.at[i])
        for i, (source, target) in enumerate(zip(sources, targets, strict=True))
    ]
    for copy in copies:
        copy.start()
    return copies


def route(pick, logits, prob, cols, spread):
    e_iota = iota((LANE, LANE), 0)
    n_iota = iota((LANE, LANE), 1)
    picks = [pick[k : k + 1, :] for k in range(2)]
    hits = [(e_iota == p).astype(F32) for p in picks]
    both = (hits[0] + hits[1]).astype(BF16)
    before = jnp.dot(both, onehot(e_iota < n_iota), preferred_element_type=F32)
    places = []
    for k in range(2):
        rank = jnp.sum(before * hits[k], axis=0, keepdims=True)
        places.append(RANKS * picks[k] + rank.astype(jnp.int32))
    first = prob[...] * jax.nn.sigmoid(logits[0:1, :] - logits[1:2, :])
    second = prob[...] * jax.nn.sigmoid(logits[1:2, :] - logits[0:1, :])
    rows = [places[0].astype(F32), places[1].astype(F32), first, second]
    table = jnp.zeros((LANE, LANE), F32)
    for i, row in enumerate(rows):
        table = jnp.where(e_iota == i, row, table)
    cols[...] = table.T
    part = e_iota // RANKS % PARTS
    for b in range(spread.shape[0] // LANE):
        row = e_iota + b * LANE
        code = row // (RANKS * PARTS) * RANKS + row % RANKS
        hit = jnp.logical_or(code == places[0], code == places[1])
        for q in range(PARTS):
            spread[b * LANE : (b + 1) * LANE, q * LANE : (q + 1) * LANE] = onehot(
                jnp.logical_and(hit, part == q)
            )


def select(cols, picked):
    tokens, rows = cols.shape[0], picked.shape[1]
    slot = iota((tokens, rows), 1)
    code = (slot // (RANKS * PARTS) * RANKS + slot % RANKS).astype(F32)
    share = jnp.where(cols[:, 0:1] == code, cols[:, 2:3], 0.0)
    share = jnp.where(cols[:, 1:2] == code, cols[:, 3:4], share)
    part = slot // RANKS % PARTS
    for q in range(PARTS):
        picked[q * tokens : (q + 1) * tokens, :] = jnp.where(part == q, share, 0.0).astype(BF16)


def load_body(
    value_in, gate_in, kernel_in, bias_in, gain_in, shift_in, pick_in, logits_in, prob_in,
    value, gate, tail, kernel, vecs, pick, logits, prob,
    sems,
):
    length = value.shape[0]
    cut = length - HALO
    last = fetch(
        (value_in.at[cut:length, :], gate_in.at[cut:length, :]),
        (value.at[cut:length, :], gate.at[cut:length, :]),
        sems,
    )
    rest = fetch(
        (
            value_in.at[0:cut, :], gate_in.at[0:cut, :],
            kernel_in, bias_in, gain_in, shift_in, pick_in, logits_in, prob_in,
        ),
        (
            value.at[0:cut, :], gate.at[0:cut, :],
            kernel, vecs.at[0:1], vecs.at[1:2], vecs.at[2:3], pick, logits, prob,
        ),
        sems.at[2:11],
    )
    for copy in last:
        copy.wait()
    glued = value[cut:length, :].astype(F32) * jax.nn.sigmoid(gate[cut:length, :].astype(F32))
    tail[...] = glued.astype(BF16)
    for copy in rest:
        copy.wait()


def taps_and_norm(ext, taps, vecs, b, start, rows, n_taps):
    lanes = pl.ds(pl.multiple_of(b * LANE, LANE), LANE)
    acc = jnp.broadcast_to(vecs[0:1, lanes], (rows, LANE))
    for j in range(n_taps):
        at = start + HALO - (n_taps - 1) + j
        acc = acc + taps[b, j : j + 1, :] * ext[b, at : at + rows, :]
    centre = jnp.mean(acc, axis=-1, keepdims=True)
    away = acc - centre
    variance = jnp.mean(away * away, axis=-1, keepdims=True)
    v = away * lax.rsqrt(variance + EPS) * vecs[1:2, lanes] + vecs[2:3, lanes]
    return (v / (1.0 + jnp.exp(-v))).astype(BF16)


def conv_body(
    _, value, gate, kernel, vecs, pick, logits, prob, weight_in,
    rest, front, taps, spread, picked, weight,
    ext, cols, sem,
):
    large = pltpu.make_async_copy(weight_in, weight, sem.at[0])
    large.start()
    n_taps, width = kernel.shape
    length = value.shape[0]
    blocks = width // LANE
    for b in range(blocks):
        lanes = slice(b * LANE, (b + 1) * LANE)
        taps[b, 0:n_taps, :] = kernel[:, lanes].astype(F32)
        glued = value[:, lanes].astype(F32) * jax.nn.sigmoid(gate[:, lanes].astype(F32))
        ext[b, HALO : HALO + length, :] = glued.astype(BF16).astype(F32)
        front[b, :, :] = ext[b, HALO : 2 * HALO, :]

    def block(b, carry):
        lanes = pl.ds(pl.multiple_of(b * LANE, LANE), LANE)
        for r in range(HALO, length, HALO):
            rest[r : r + HALO, lanes] = taps_and_norm(ext, taps, vecs, b, r, HALO, n_taps)
        return carry

    lax.fori_loop(0, blocks, block, 0)
    route(pick, logits, prob, cols, spread)
    select(cols, picked)
    large.wait()


def head_body(cores, me, rest, front, taps, vecs, halo, mine, theirs, ext, mixed):
    n_taps = 31
    blocks, _, _ = front.shape
    half = mine.shape[0]
    for b in range(blocks):
        lanes = slice(b * LANE, (b + 1) * LANE)
        ext[b, 0:HALO, :] = jnp.where(me[0] >= cores, halo[:, lanes].astype(F32), 0.0)
        ext[b, HALO : 2 * HALO, :] = front[b, :, :]
    for b in range(blocks):
        lanes = slice(b * LANE, (b + 1) * LANE)
        mixed[:, lanes] = taps_and_norm(ext, taps, vecs, b, 0, HALO, n_taps)

    core = lax.rem(me[0], cores)

    @pl.when(core == 0)
    def _():
        mine[0:HALO, :] = mixed[...]
        mine[HALO:half, :] = rest[HALO:half, :]
        theirs[...] = rest[half : 2 * half, :]

    @pl.when(core != 0)
    def _():
        theirs[0:HALO, :] = mixed[...]
        theirs[HALO:half, :] = rest[HALO:half, :]
        mine[...] = rest[half : 2 * half, :]


def own_body(cores, me, mine, weight, residual, partial):
    half = mine.shape[1]
    step = partial.shape[1] // 4
    here = pl.ds(pl.multiple_of(lax.rem(me[0], cores) * half, half), half)
    for q in range(4):
        lanes = slice(q * step, (q + 1) * step)
        acc = jnp.dot(mine[...], weight[here, lanes], preferred_element_type=F32)
        partial[:, lanes] = acc + residual[:, lanes].astype(F32)


def project_body(cores, me, other, weight, partial, gain, spread, hidden, out, stacked):
    tokens, half = other.shape
    width = partial.shape[1]
    step = width // 4
    there = pl.ds(pl.multiple_of((1 - lax.rem(me[0], cores)) * half, half), half)
    total = jnp.zeros((tokens, 1), F32)
    for q in range(4):
        lanes = slice(q * step, (q + 1) * step)
        acc = jnp.dot(other[...], weight[there, lanes], preferred_element_type=F32)
        full = (acc + partial[:, lanes]).astype(BF16)
        hidden[:, lanes] = full
        wide = full.astype(F32)
        total = total + jnp.sum(wide * wide, axis=-1, keepdims=True)
    scale = lax.rsqrt(total / width + EPS)
    step = width // PARTS
    for q in range(PARTS):
        lanes = slice(q * step, (q + 1) * step)
        stacked[q * tokens : (q + 1) * tokens, :] = (
            hidden[:, lanes].astype(F32) * scale * gain[:, lanes]
        ).astype(BF16)
    chunk = 2 * LANE
    for b in range(out.shape[0] // chunk):
        rows = slice(b * chunk, (b + 1) * chunk)
        out[rows, :] = jnp.dot(spread[rows, :], stacked[...], preferred_element_type=F32).astype(BF16)


def perm(back):
    i, j = iota((LANE, LANE), 0), iota((LANE, LANE), 1)
    if back:
        i, j = j, i
    rows = LANE // PARTS
    return onehot(j == (i % rows) // RANKS * (RANKS * PARTS) + i // rows * RANKS + i % RANKS)


def unpack(message, flat):
    p = perm(False)
    rows = LANE // PARTS
    step = message.shape[1]
    for b in range(message.shape[0] // LANE):
        y = jnp.dot(p, message[b * LANE : (b + 1) * LANE, :], preferred_element_type=F32).astype(BF16)
        for q in range(PARTS):
            flat[b * rows : (b + 1) * rows, q * step : (q + 1) * step] = y[q * rows : (q + 1) * rows]


def expert_body(message, gate, up, down, out, flat, answer):
    unpack(message, flat)
    x = flat[...]
    g = jnp.dot(x, gate[...], preferred_element_type=F32)
    u = jnp.dot(x, up[...], preferred_element_type=F32)
    active = (g / (1.0 + jnp.exp(-g)) * u).astype(BF16)
    answer[...] = jnp.dot(active, down[...], preferred_element_type=F32).astype(BF16)
    p = perm(True)
    rows = LANE // PARTS
    step = out.shape[1]
    for b in range(out.shape[0] // LANE):
        z = jnp.concatenate(
            [answer[b * rows : (b + 1) * rows, q * step : (q + 1) * step] for q in range(PARTS)], axis=0
        )
        out[b * LANE : (b + 1) * LANE, :] = jnp.dot(p, z, preferred_element_type=F32).astype(BF16)


def combine_body(message, picked, base, out_hbm, out, sems):
    tokens = out.shape[0]
    step = message.shape[1]
    pieces = 4
    size = step // pieces
    copies = []
    for p in range(pieces):
        got = jnp.dot(picked[...], message[:, p * size : (p + 1) * size], preferred_element_type=F32)
        for q in range(PARTS):
            lanes = slice(q * step + p * size, q * step + (p + 1) * size)
            out[:, lanes] = (base[:, lanes].astype(F32) + got[q * tokens : (q + 1) * tokens]).astype(BF16)
            copy = pltpu.make_async_copy(
                out.at[:, lanes], out_hbm.at[:, lanes], sems.at[p * PARTS + q]
            )
            copy.start()
            copies.append(copy)
    for copy in copies:
        copy.wait()


def local(
    glu_value,
    glu_gate,
    conv_kernel,
    conv_bias,
    group_gain,
    group_shift,
    out_weight,
    residual,
    ffn_gain,
    expert_pick,
    pair_logits,
    group_prob,
    gate_weight,
    up_weight,
    down_weight,
):
    shape = jax.ShapeDtypeStruct
    length, width = glu_value.shape
    tokens, model = residual.shape
    experts = lax.axis_size("sp") * lax.axis_size("tp")
    peers = lax.axis_size("sp")
    me = lax.axis_index(("sp", "tp")).astype(jnp.int32).reshape(1)

    n_taps = conv_kernel.shape[0]
    blocks = width // LANE
    cores = lax.axis_size("tp")
    step = model // PARTS
    rows = experts * RANKS * PARTS
    message = shape((rows, step), BF16)
    value, gate, tail, kernel, vecs, pick, logits, prob = call(
        load_body,
        (
            shape((length, width), BF16),
            shape((length, width), BF16),
            shape((HALO, width), BF16),
            shape((n_taps, width), BF16),
            shape((8, width), F32),
            shape((2, tokens), jnp.int32),
            shape((2, tokens), F32),
            shape((1, tokens), F32),
        ),
        scratch=(pltpu.SemaphoreType.DMA((11,)),),
        hbm=range(9),
        n_in=9,
        limit=4,
        flops=1_000_000,
        name="load",
    )(
        glu_value,
        glu_gate,
        conv_kernel,
        conv_bias.reshape(1, width),
        group_gain.reshape(1, width),
        group_shift.reshape(1, width),
        expert_pick.T,
        pair_logits.T,
        group_prob.reshape(1, tokens),
    )
    halo = lax.ppermute(tail, "sp", [(i, (i + 1) % peers) for i in range(peers)])
    rest, front, taps, spread, picked, weight = call(
        conv_body,
        (
            shape((length, width), BF16),
            shape((blocks, HALO, LANE), F32),
            shape((blocks, 32, LANE), F32),
            shape((rows, PARTS * tokens), BF16),
            shape((PARTS * tokens, rows), BF16),
            shape(out_weight.shape, BF16),
        ),
        scratch=(
            pltpu.VMEM((blocks, HALO + length, LANE), F32),
            pltpu.VMEM((tokens, LANE), F32),
            pltpu.SemaphoreType.DMA((1,)),
        ),
        smem=(0,),
        hbm=(8,),
        n_in=9,
        limit=8,
        flops=3_000_000_000,
        name="conv",
    )(me, value, gate, kernel, vecs, pick, logits, prob, out_weight)
    mine, theirs = call(
        functools.partial(head_body, cores),
        (shape((length // 2, width), BF16), shape((length // 2, width), BF16)),
        scratch=(pltpu.VMEM((blocks, 2 * HALO, LANE), F32), pltpu.VMEM((HALO, width), BF16)),
        smem=(0,),
        n_in=6,
        limit=4,
        flops=500_000_000,
        name="head",
    )(me, rest, front, taps, vecs, halo)
    other = lax.ppermute(theirs, "tp", [(0, 1), (1, 0)])
    (partial,) = call(
        functools.partial(own_body, cores),
        (shape((tokens, model), F32),),
        smem=(0,),
        n_in=4,
        limit=4,
        flops=500_000_000,
        name="own",
    )(me, mine, weight, residual)
    hidden, send = call(
        functools.partial(project_body, cores),
        (shape((tokens, model), BF16), message),
        scratch=(pltpu.VMEM((PARTS * tokens, step), BF16),),
        smem=(0,),
        n_in=6,
        limit=16,
        flops=1_000_000_000,
        name="project",
    )(me, other, weight, partial, ffn_gain.reshape(1, model), spread)
    flat = pltpu.VMEM((RANKS * experts, model), BF16)

    def exchange(x):
        x = x.reshape(experts, RANKS * PARTS, step)
        return lax.all_to_all(x, ("sp", "tp"), 0, 0, tiled=True).reshape(rows, step)

    got = exchange(send)
    (done,) = call(
        expert_body,
        (message,),
        scratch=(flat, flat),
        n_in=4,
        limit=24,
        flops=4_000_000_000,
        name="expert",
    )(got, gate_weight[0], up_weight[0], down_weight[0])
    back = exchange(done)
    (result,) = call(
        combine_body,
        (shape((tokens, model), BF16),),
        scratch=(pltpu.VMEM((tokens, model), BF16), pltpu.SemaphoreType.DMA((8,))),
        n_in=3,
        out_hbm=(0,),
        limit=12,
        flops=1_000_000_000,
        name="combine",
    )(back, picked, hidden)
    return result


def solution(mesh):
    in_specs = (
        P("sp", "tp"),
        P("sp", "tp"),
        P(None, "tp"),
        P("tp"),
        P("tp"),
        P("tp"),
        P(),
        P(("sp", "tp"), None),
        P(),
        P(("sp", "tp"), None),
        P(("sp", "tp"), None),
        P(("sp", "tp")),
        P(("sp", "tp"), None, None),
        P(("sp", "tp"), None, None),
        P(("sp", "tp"), None, None),
    )
    out_specs = P(("sp", "tp"), None)
    return jax.shard_map(local, mesh=mesh, in_specs=in_specs, out_specs=out_specs, check_vma=False)
```

```python
import functools
import jax
import jax.numpy as jnp
from jax import lax
from jax.experimental import pallas as pl
from jax.experimental.pallas import tpu as pltpu
from jax.sharding import PartitionSpec as P

EPS = 1e-06
F32 = jnp.float32
BF16 = jnp.bfloat16
HALO = 32
PARTS = 2
RANKS = 4
LANE = 128
MIB = 1024 * 1024


def iota(shape, axis):
    return lax.broadcasted_iota(jnp.int32, shape, axis)


def onehot(cond):
    return jnp.where(cond, 1.0, 0.0).astype(BF16)


def call(body, out_shape, scratch=(), limit=16, smem=(), hbm=(), n_in=0, out_hbm=(), flops=0, name=None):
    kind = {**dict.fromkeys(smem, pltpu.SMEM), **dict.fromkeys(hbm, pltpu.HBM)}
    n_out = len(out_shape)
    run = pl.pallas_call(
        body,
        out_shape=out_shape,
        in_specs=[pl.BlockSpec(memory_space=kind.get(i, pltpu.VMEM)) for i in range(n_in)],
        out_specs=[
            pl.BlockSpec(memory_space=pltpu.HBM if i in out_hbm else pltpu.VMEM) for i in range(n_out)
        ],
        scratch_shapes=list(scratch),
        compiler_params=pltpu.CompilerParams(vmem_limit_bytes=limit * MIB),
        cost_estimate=pl.CostEstimate(flops=flops, bytes_accessed=0, transcendentals=0),
        name=name,
    )
    return lambda *args: run(
        *(pltpu.with_memory_space_constraint(a, pltpu.HBM) if i in hbm else a for i, a in enumerate(args))
    )


def fetch(sources, targets, sems):
    copies = [
        pltpu.make_async_copy(source, target, sems.at[i])
        for i, (source, target) in enumerate(zip(sources, targets, strict=True))
    ]
    for copy in copies:
        copy.start()
    return copies


def route(pick, logits, prob, cols, spread):
    e_iota = iota((LANE, LANE), 0)
    n_iota = iota((LANE, LANE), 1)
    picks = [pick[k : k + 1, :] for k in range(2)]
    hits = [(e_iota == p).astype(F32) for p in picks]
    both = (hits[0] + hits[1]).astype(BF16)
    before = jnp.dot(both, onehot(e_iota < n_iota), preferred_element_type=F32)
    places = []
    for k in range(2):
        rank = jnp.sum(before * hits[k], axis=0, keepdims=True)
        places.append(RANKS * picks[k] + rank.astype(jnp.int32))
    first = prob[...] * jax.nn.sigmoid(logits[0:1, :] - logits[1:2, :])
    second = prob[...] * jax.nn.sigmoid(logits[1:2, :] - logits[0:1, :])
    rows = [places[0].astype(F32), places[1].astype(F32), first, second]
    table = jnp.zeros((LANE, LANE), F32)
    for i, row in enumerate(rows):
        table = jnp.where(e_iota == i, row, table)
    cols[...] = table.T
    part = e_iota // RANKS % PARTS
    for b in range(spread.shape[0] // LANE):
        row = e_iota + b * LANE
        code = row // (RANKS * PARTS) * RANKS + row % RANKS
        hit = jnp.logical_or(code == places[0], code == places[1])
        for q in range(PARTS):
            spread[b * LANE : (b + 1) * LANE, q * LANE : (q + 1) * LANE] = onehot(
                jnp.logical_and(hit, part == q)
            )


def select(cols, picked):
    tokens, rows = cols.shape[0], picked.shape[1]
    slot = iota((tokens, rows), 1)
    code = (slot // (RANKS * PARTS) * RANKS + slot % RANKS).astype(F32)
    share = jnp.where(cols[:, 0:1] == code, cols[:, 2:3], 0.0)
    share = jnp.where(cols[:, 1:2] == code, cols[:, 3:4], share)
    part = slot // RANKS % PARTS
    for q in range(PARTS):
        picked[q * tokens : (q + 1) * tokens, :] = jnp.where(part == q, share, 0.0).astype(BF16)


def load_body(
    value_in, gate_in, kernel_in, bias_in, gain_in, shift_in, pick_in, logits_in, prob_in,
    tail, kernel, vecs, pick, logits, prob,
    value, gate, sems,
):
    cut = value_in.shape[0] - HALO
    copies = fetch(
        (
            value_in.at[pl.ds(cut, HALO), :], gate_in.at[pl.ds(cut, HALO), :],
            kernel_in, bias_in, gain_in, shift_in, pick_in, logits_in, prob_in,
        ),
        (value, gate, kernel, vecs.at[0:1], vecs.at[1:2], vecs.at[2:3], pick, logits, prob),
        sems,
    )
    for copy in copies[:2]:
        copy.wait()
    glued = value[...].astype(F32) * jax.nn.sigmoid(gate[...].astype(F32))
    tail[...] = glued.astype(BF16)
    for copy in copies[2:]:
        copy.wait()


def taps_and_norm(ext, taps, vecs, b, start, rows, n_taps):
    lanes = pl.ds(pl.multiple_of(b * LANE, LANE), LANE)
    acc = jnp.broadcast_to(vecs[0:1, lanes], (rows, LANE))
    for j in range(n_taps):
        at = start + HALO - (n_taps - 1) + j
        acc = acc + taps[b, j : j + 1, :] * ext[b, at : at + rows, :]
    centre = jnp.mean(acc, axis=-1, keepdims=True)
    away = acc - centre
    variance = jnp.mean(away * away, axis=-1, keepdims=True)
    v = away * lax.rsqrt(variance + EPS) * vecs[1:2, lanes] + vecs[2:3, lanes]
    return (v / (1.0 + jnp.exp(-v))).astype(BF16)


def conv_body(
    _, value_in, gate_in, kernel, vecs, pick, logits, prob, weight_in,
    rest, front, taps, spread, picked, weight,
    value, gate, ext, cols, sems,
):
    *copies, large = fetch((value_in, gate_in, weight_in), (value, gate, weight), sems)
    route(pick, logits, prob, cols, spread)
    select(cols, picked)
    for copy in copies:
        copy.wait()
    n_taps, width = kernel.shape
    length = value.shape[0]
    blocks = width // LANE
    for b in range(blocks):
        lanes = slice(b * LANE, (b + 1) * LANE)
        taps[b, 0:n_taps, :] = kernel[:, lanes].astype(F32)
        glued = value[:, lanes].astype(F32) * jax.nn.sigmoid(gate[:, lanes].astype(F32))
        ext[b, HALO : HALO + length, :] = glued.astype(BF16).astype(F32)
        front[b, :, :] = ext[b, HALO : 2 * HALO, :]

    def block(b, carry):
        lanes = pl.ds(pl.multiple_of(b * LANE, LANE), LANE)
        for r in range(HALO, length, HALO):
            rest[r : r + HALO, lanes] = taps_and_norm(ext, taps, vecs, b, r, HALO, n_taps)
        return carry

    lax.fori_loop(0, blocks, block, 0)
    large.wait()


def head_body(cores, me, rest, front, taps, vecs, halo, mine, theirs, ext, mixed):
    n_taps = 31
    blocks, _, _ = front.shape
    half = mine.shape[0]
    for b in range(blocks):
        lanes = slice(b * LANE, (b + 1) * LANE)
        ext[b, 0:HALO, :] = jnp.where(me[0] >= cores, halo[:, lanes].astype(F32), 0.0)
        ext[b, HALO : 2 * HALO, :] = front[b, :, :]
    for b in range(blocks):
        lanes = slice(b * LANE, (b + 1) * LANE)
        mixed[:, lanes] = taps_and_norm(ext, taps, vecs, b, 0, HALO, n_taps)

    core = lax.rem(me[0], cores)

    @pl.when(core == 0)
    def _():
        mine[0:HALO, :] = mixed[...]
        mine[HALO:half, :] = rest[HALO:half, :]
        theirs[...] = rest[half : 2 * half, :]

    @pl.when(core != 0)
    def _():
        theirs[0:HALO, :] = mixed[...]
        theirs[HALO:half, :] = rest[HALO:half, :]
        mine[...] = rest[half : 2 * half, :]


def own_body(cores, me, mine, weight, residual, partial):
    half = mine.shape[1]
    step = partial.shape[1] // 4
    here = pl.ds(pl.multiple_of(lax.rem(me[0], cores) * half, half), half)
    for q in range(4):
        lanes = slice(q * step, (q + 1) * step)
        acc = jnp.dot(mine[...], weight[here, lanes], preferred_element_type=F32)
        partial[:, lanes] = acc + residual[:, lanes].astype(F32)


def project_body(cores, me, other, weight, partial, gain, spread, hidden, out, stacked):
    tokens, half = other.shape
    width = partial.shape[1]
    step = width // 4
    there = pl.ds(pl.multiple_of((1 - lax.rem(me[0], cores)) * half, half), half)
    total = jnp.zeros((tokens, 1), F32)
    for q in range(4):
        lanes = slice(q * step, (q + 1) * step)
        acc = jnp.dot(other[...], weight[there, lanes], preferred_element_type=F32)
        full = (acc + partial[:, lanes]).astype(BF16)
        hidden[:, lanes] = full
        wide = full.astype(F32)
        total = total + jnp.sum(wide * wide, axis=-1, keepdims=True)
    scale = lax.rsqrt(total / width + EPS)
    step = width // PARTS
    for q in range(PARTS):
        lanes = slice(q * step, (q + 1) * step)
        stacked[q * tokens : (q + 1) * tokens, :] = (
            hidden[:, lanes].astype(F32) * scale * gain[:, lanes]
        ).astype(BF16)
    chunk = 2 * LANE
    for b in range(out.shape[0] // chunk):
        rows = slice(b * chunk, (b + 1) * chunk)
        out[rows, :] = jnp.dot(spread[rows, :], stacked[...], preferred_element_type=F32).astype(BF16)


def trade(a, b):
    low = iota(a.shape, 1) < RANKS
    return jnp.where(low, a, pltpu.roll(b, RANKS, 1)), jnp.where(low, pltpu.roll(a, RANKS, 1), b)


def expert_body(message, gate, up, down, out, flat):
    rows, step = message.shape
    tile = RANKS * PARTS
    pairs = rows // (2 * tile)
    pieces = 4
    size = step // pieces
    for p in range(pieces):
        here = slice(p * size, (p + 1) * size)
        wide = message[:, here].astype(F32).reshape(pairs, 2, tile, size)
        for q, half in enumerate(trade(wide[:, 0], wide[:, 1])):
            flat[:, q * step + p * size : q * step + (p + 1) * size] = half.reshape(rows // 2, size).astype(BF16)
    x = flat[...]
    g = jnp.dot(x, gate[...], preferred_element_type=F32)
    u = jnp.dot(x, up[...], preferred_element_type=F32)
    active = (g / (1.0 + jnp.exp(-g)) * u).astype(BF16)
    for p in range(pieces):
        halves = [
            jnp.dot(
                active, down[:, q * step + p * size : q * step + (p + 1) * size], preferred_element_type=F32
            ).reshape(pairs, tile, size)
            for q in range(PARTS)
        ]
        both = jnp.stack(trade(*halves), axis=1)
        out[:, p * size : (p + 1) * size] = both.reshape(rows, size).astype(BF16)


def combine_body(message, picked, base, out_hbm, out, sems):
    tokens = out.shape[0]
    step = message.shape[1]
    pieces = 4
    size = step // pieces
    copies = []
    for p in range(pieces):
        got = jnp.dot(picked[...], message[:, p * size : (p + 1) * size], preferred_element_type=F32)
        for q in range(PARTS):
            lanes = slice(q * step + p * size, q * step + (p + 1) * size)
            out[:, lanes] = (base[:, lanes].astype(F32) + got[q * tokens : (q + 1) * tokens]).astype(BF16)
            copy = pltpu.make_async_copy(
                out.at[:, lanes], out_hbm.at[:, lanes], sems.at[p * PARTS + q]
            )
            copy.start()
            copies.append(copy)
    for copy in copies:
        copy.wait()


def local(
    glu_value,
    glu_gate,
    conv_kernel,
    conv_bias,
    group_gain,
    group_shift,
    out_weight,
    residual,
    ffn_gain,
    expert_pick,
    pair_logits,
    group_prob,
    gate_weight,
    up_weight,
    down_weight,
):
    shape = jax.ShapeDtypeStruct
    length, width = glu_value.shape
    tokens, model = residual.shape
    experts = lax.axis_size("sp") * lax.axis_size("tp")
    peers = lax.axis_size("sp")
    me = lax.axis_index(("sp", "tp")).astype(jnp.int32).reshape(1)

    n_taps = conv_kernel.shape[0]
    blocks = width // LANE
    cores = lax.axis_size("tp")
    step = model // PARTS
    rows = experts * RANKS * PARTS
    message = shape((rows, step), BF16)
    tail, kernel, vecs, pick, logits, prob = call(
        load_body,
        (
            shape((HALO, width), BF16),
            shape((n_taps, width), BF16),
            shape((8, width), F32),
            shape((2, tokens), jnp.int32),
            shape((2, tokens), F32),
            shape((1, tokens), F32),
        ),
        scratch=(
            pltpu.VMEM((HALO, width), BF16),
            pltpu.VMEM((HALO, width), BF16),
            pltpu.SemaphoreType.DMA((9,)),
        ),
        hbm=range(9),
        n_in=9,
        limit=4,
        flops=1_000_000,
        name="load",
    )(
        glu_value,
        glu_gate,
        conv_kernel,
        conv_bias.reshape(1, width),
        group_gain.reshape(1, width),
        group_shift.reshape(1, width),
        expert_pick.T,
        pair_logits.T,
        group_prob.reshape(1, tokens),
    )
    halo = lax.ppermute(tail, "sp", [(i, (i + 1) % peers) for i in range(peers)])
    rest, front, taps, spread, picked, weight = call(
        conv_body,
        (
            shape((length, width), BF16),
            shape((blocks, HALO, LANE), F32),
            shape((blocks, 32, LANE), F32),
            shape((rows, PARTS * tokens), BF16),
            shape((PARTS * tokens, rows), BF16),
            shape(out_weight.shape, BF16),
        ),
        scratch=(
            pltpu.VMEM((length, width), BF16),
            pltpu.VMEM((length, width), BF16),
            pltpu.VMEM((blocks, HALO + length, LANE), F32),
            pltpu.VMEM((tokens, LANE), F32),
            pltpu.SemaphoreType.DMA((3,)),
        ),
        smem=(0,),
        hbm=(1, 2, 8),
        n_in=9,
        limit=8,
        flops=3_000_000_000,
        name="conv",
    )(me, glu_value, glu_gate, kernel, vecs, pick, logits, prob, out_weight)
    mine, theirs = call(
        functools.partial(head_body, cores),
        (shape((length // 2, width), BF16), shape((length // 2, width), BF16)),
        scratch=(pltpu.VMEM((blocks, 2 * HALO, LANE), F32), pltpu.VMEM((HALO, width), BF16)),
        smem=(0,),
        n_in=6,
        limit=4,
        flops=500_000_000,
        name="head",
    )(me, rest, front, taps, vecs, halo)
    other = lax.ppermute(theirs, "tp", [(0, 1), (1, 0)])
    (partial,) = call(
        functools.partial(own_body, cores),
        (shape((tokens, model), F32),),
        smem=(0,),
        n_in=4,
        limit=4,
        flops=500_000_000,
        name="own",
    )(me, mine, weight, residual)
    hidden, send = call(
        functools.partial(project_body, cores),
        (shape((tokens, model), BF16), message),
        scratch=(pltpu.VMEM((PARTS * tokens, step), BF16),),
        smem=(0,),
        n_in=6,
        limit=16,
        flops=1_000_000_000,
        name="project",
    )(me, other, weight, partial, ffn_gain.reshape(1, model), spread)
    flat = pltpu.VMEM((RANKS * experts, model), BF16)

    def exchange(x):
        x = x.reshape(experts, RANKS * PARTS, step)
        return lax.all_to_all(x, ("sp", "tp"), 0, 0, tiled=True).reshape(rows, step)

    got = exchange(send)
    (done,) = call(
        expert_body,
        (message,),
        scratch=(flat,),
        n_in=4,
        limit=24,
        flops=4_000_000_000,
        name="expert",
    )(got, gate_weight[0], up_weight[0], down_weight[0])
    back = exchange(done)
    (result,) = call(
        combine_body,
        (shape((tokens, model), BF16),),
        scratch=(pltpu.VMEM((tokens, model), BF16), pltpu.SemaphoreType.DMA((8,))),
        n_in=3,
        out_hbm=(0,),
        limit=12,
        flops=1_000_000_000,
        name="combine",
    )(back, picked, hidden)
    return result


def solution(mesh):
    in_specs = (
        P("sp", "tp"),
        P("sp", "tp"),
        P(None, "tp"),
        P("tp"),
        P("tp"),
        P("tp"),
        P(),
        P(("sp", "tp"), None),
        P(),
        P(("sp", "tp"), None),
        P(("sp", "tp"), None),
        P(("sp", "tp")),
        P(("sp", "tp"), None, None),
        P(("sp", "tp"), None, None),
        P(("sp", "tp"), None, None),
    )
    out_specs = P(("sp", "tp"), None)
    return jax.shard_map(local, mesh=mesh, in_specs=in_specs, out_specs=out_specs, check_vma=False)
```

```python
import functools
import jax
import jax.numpy as jnp
from jax import lax
from jax.experimental import pallas as pl
from jax.experimental.pallas import tpu as pltpu
from jax.sharding import PartitionSpec as P


EPS = 1e-06
F32 = jnp.float32
BF16 = jnp.bfloat16
HALO = 32
PARTS = 2
RANKS = 4
LANE = 128
MIB = 1024 * 1024


def iota(shape, axis):
    return lax.broadcasted_iota(jnp.int32, shape, axis)


def onehot(cond):
    return jnp.where(cond, 1.0, 0.0).astype(BF16)


def call(body, out_shape, scratch=(), limit=16, smem=(), hbm=(), n_in=0, out_hbm=(), flops=0):
    kind = {**dict.fromkeys(smem, pltpu.SMEM), **dict.fromkeys(hbm, pltpu.HBM)}
    n_out = len(out_shape)
    run = pl.pallas_call(
        body,
        out_shape=out_shape,
        in_specs=[pl.BlockSpec(memory_space=kind.get(i, pltpu.VMEM)) for i in range(n_in)],
        out_specs=[
            pl.BlockSpec(memory_space=pltpu.HBM if i in out_hbm else pltpu.VMEM) for i in range(n_out)
        ],
        scratch_shapes=list(scratch),
        compiler_params=pltpu.CompilerParams(vmem_limit_bytes=limit * MIB),
        cost_estimate=pl.CostEstimate(flops=flops, bytes_accessed=0, transcendentals=0),
    )
    return lambda *args: run(
        *(pltpu.with_memory_space_constraint(a, pltpu.HBM) if i in hbm else a for i, a in enumerate(args))
    )


def fetch(sources, targets, sems):
    copies = [
        pltpu.make_async_copy(source, target, sems.at[i])
        for i, (source, target) in enumerate(zip(sources, targets, strict=True))
    ]
    for copy in copies:
        copy.start()
    return copies


def route(pick, logits, prob, cols, spread):
    e_iota = iota((LANE, LANE), 0)
    n_iota = iota((LANE, LANE), 1)
    picks = [pick[k : k + 1, :] for k in range(2)]
    hits = [(e_iota == p).astype(F32) for p in picks]
    both = (hits[0] + hits[1]).astype(BF16)
    before = jnp.dot(both, onehot(e_iota < n_iota), preferred_element_type=F32)
    places = []
    for k in range(2):
        rank = jnp.sum(before * hits[k], axis=0, keepdims=True)
        places.append(RANKS * picks[k] + rank.astype(jnp.int32))
    first = prob[...] * jax.nn.sigmoid(logits[0:1, :] - logits[1:2, :])
    second = prob[...] * jax.nn.sigmoid(logits[1:2, :] - logits[0:1, :])
    rows = [places[0].astype(F32), places[1].astype(F32), first, second]
    table = jnp.zeros((LANE, LANE), F32)
    for i, row in enumerate(rows):
        table = jnp.where(e_iota == i, row, table)
    cols[...] = table.T
    part = e_iota // RANKS % PARTS
    for b in range(spread.shape[0] // LANE):
        row = e_iota + b * LANE
        code = row // (RANKS * PARTS) * RANKS + row % RANKS
        hit = jnp.logical_or(code == places[0], code == places[1])
        for q in range(PARTS):
            spread[b * LANE : (b + 1) * LANE, q * LANE : (q + 1) * LANE] = onehot(
                jnp.logical_and(hit, part == q)
            )


def select(cols, picked):
    tokens, rows = cols.shape[0], picked.shape[1]
    slot = iota((tokens, rows), 1)
    code = (slot // (RANKS * PARTS) * RANKS + slot % RANKS).astype(F32)
    share = jnp.where(cols[:, 0:1] == code, cols[:, 2:3], 0.0)
    share = jnp.where(cols[:, 1:2] == code, cols[:, 3:4], share)
    part = slot // RANKS % PARTS
    for q in range(PARTS):
        picked[q * tokens : (q + 1) * tokens, :] = jnp.where(part == q, share, 0.0).astype(BF16)


def load_body(
    value_in, gate_in, kernel_in, bias_in, gain_in, shift_in, pick_in, logits_in, prob_in,
    tail, kernel, vecs, pick, logits, prob,
    value, gate, sems,
):
    cut = value_in.shape[0] - HALO
    copies = fetch(
        (
            value_in.at[pl.ds(cut, HALO), :], gate_in.at[pl.ds(cut, HALO), :],
            kernel_in, bias_in, gain_in, shift_in, pick_in, logits_in, prob_in,
        ),
        (value, gate, kernel, vecs.at[0:1], vecs.at[1:2], vecs.at[2:3], pick, logits, prob),
        sems,
    )
    for copy in copies[:2]:
        copy.wait()
    glued = value[...].astype(F32) * jax.nn.sigmoid(gate[...].astype(F32))
    tail[...] = glued.astype(BF16)
    for copy in copies[2:]:
        copy.wait()


def taps_and_norm(ext, taps, vecs, b, start, rows, n_taps):
    lanes = pl.ds(pl.multiple_of(b * LANE, LANE), LANE)
    acc = jnp.broadcast_to(vecs[0:1, lanes], (rows, LANE))
    for j in range(n_taps):
        at = start + HALO - (n_taps - 1) + j
        acc = acc + taps[b, j : j + 1, :] * ext[b, at : at + rows, :]
    centre = jnp.mean(acc, axis=-1, keepdims=True)
    away = acc - centre
    variance = jnp.mean(away * away, axis=-1, keepdims=True)
    v = away * lax.rsqrt(variance + EPS) * vecs[1:2, lanes] + vecs[2:3, lanes]
    return (v / (1.0 + jnp.exp(-v))).astype(BF16)


def conv_body(
    cores, me, value_in, gate_in, kernel, vecs, pick, logits, prob, weight_in,
    mine, packet, front, taps, spread, picked, weight,
    value, gate, ext, mixed, cols, sems,
):
    *copies, large = fetch((value_in, gate_in, weight_in), (value, gate, weight), sems)
    route(pick, logits, prob, cols, spread)
    select(cols, picked)
    for copy in copies:
        copy.wait()
    n_taps, width = kernel.shape
    length = value.shape[0]
    half = length // 2
    blocks = width // LANE
    for b in range(blocks):
        lanes = slice(b * LANE, (b + 1) * LANE)
        taps[b, 0:n_taps, :] = kernel[:, lanes].astype(F32)
        glued = (value[:, lanes].astype(F32) * jax.nn.sigmoid(gate[:, lanes].astype(F32))).astype(BF16)
        ext[b, HALO : HALO + length, :] = glued.astype(F32)
        front[b, :, :] = ext[b, HALO : 2 * HALO, :]
        packet[half : half + HALO, lanes] = glued[0:HALO]
    packet[half + HALO : half + HALO + n_taps, :] = kernel[...]
    piece = iota((16, width), 0)
    pieces = jnp.zeros((16, width), F32)
    for i in range(3):
        left = vecs[i : i + 1, :]
        for j in range(3):
            top = left.astype(BF16).astype(F32)
            pieces = jnp.where(piece == 3 * i + j, top, pieces)
            left = left - top
    packet[half + 2 * HALO : half + 2 * HALO + 16, :] = pieces.astype(BF16)
    mixed[0:HALO, :] = jnp.zeros((HALO, width), BF16)

    def block(b, carry):
        lanes = pl.ds(pl.multiple_of(b * LANE, LANE), LANE)
        for r in range(HALO, length, HALO):
            mixed[r : r + HALO, lanes] = taps_and_norm(ext, taps, vecs, b, r, HALO, n_taps)
        return carry

    lax.fori_loop(0, blocks, block, 0)
    core = lax.rem(me[0], cores)
    mine[...] = mixed[pl.ds(pl.multiple_of(core * half, half), half), :]
    packet[0:half, :] = mixed[pl.ds(pl.multiple_of((1 - core) * half, half), half), :]
    large.wait()


def head(me, cores, halo, front, taps, vecs, ext, out, n_taps):
    for b in range(front.shape[0]):
        lanes = slice(b * LANE, (b + 1) * LANE)
        ext[b, 0:HALO, :] = jnp.where(me[0] >= cores, halo[:, lanes].astype(F32), 0.0)
        ext[b, HALO : 2 * HALO, :] = front[b, :, :]
    for b in range(front.shape[0]):
        lanes = slice(b * LANE, (b + 1) * LANE)
        out[0:HALO, lanes] = taps_and_norm(ext, taps, vecs, b, 0, HALO, n_taps)


def own_body(cores, n_taps, me, mine, halo, front, taps, vecs, weight, residual, partial, ext, full):
    half = mine.shape[1]
    step = partial.shape[1] // 4
    core = lax.rem(me[0], cores)
    full[...] = mine[...]

    @pl.when(core == 0)
    def _():
        head(me, cores, halo, front, taps, vecs, ext, full, n_taps)

    here = pl.ds(pl.multiple_of(core * half, half), half)
    for q in range(4):
        lanes = slice(q * step, (q + 1) * step)
        acc = jnp.dot(full[...], weight[here, lanes], preferred_element_type=F32)
        partial[:, lanes] = acc + residual[:, lanes].astype(F32)


def project_body(
    cores, n_taps, me, packet, halo, weight, partial, gain, spread,
    hidden, out,
    stacked, ext, front, taps, vecs, full,
):
    tokens, width = partial.shape
    half = packet.shape[1]
    core = lax.rem(me[0], cores)
    full[...] = packet[0:tokens, :]

    @pl.when(core == 0)
    def _():
        pieces = packet[tokens + 2 * HALO : tokens + 2 * HALO + 16, :].astype(F32)
        for i in range(3):
            vecs[i : i + 1, :] = (pieces[3 * i : 3 * i + 1] + pieces[3 * i + 1 : 3 * i + 2]) + pieces[
                3 * i + 2 : 3 * i + 3
            ]
        for b in range(front.shape[0]):
            lanes = slice(b * LANE, (b + 1) * LANE)
            front[b, :, :] = packet[tokens : tokens + HALO, lanes].astype(F32)
            taps[b, 0:n_taps, :] = packet[tokens + HALO : tokens + HALO + n_taps, lanes].astype(F32)
        head(me, cores, halo, front, taps, vecs, ext, full, n_taps)

    step = width // 4
    there = pl.ds(pl.multiple_of((1 - core) * half, half), half)
    total = jnp.zeros((tokens, 1), F32)
    for q in range(4):
        lanes = slice(q * step, (q + 1) * step)
        acc = jnp.dot(full[...], weight[there, lanes], preferred_element_type=F32)
        rounded = (acc + partial[:, lanes]).astype(BF16)
        hidden[:, lanes] = rounded
        wide = rounded.astype(F32)
        total = total + jnp.sum(wide * wide, axis=-1, keepdims=True)
    scale = lax.rsqrt(total / width + EPS)
    step = width // PARTS
    for q in range(PARTS):
        lanes = slice(q * step, (q + 1) * step)
        stacked[q * tokens : (q + 1) * tokens, :] = (
            hidden[:, lanes].astype(F32) * scale * gain[:, lanes]
        ).astype(BF16)
    chunk = 2 * LANE
    for b in range(out.shape[0] // chunk):
        rows = slice(b * chunk, (b + 1) * chunk)
        out[rows, :] = jnp.dot(spread[rows, :], stacked[...], preferred_element_type=F32).astype(BF16)


def trade(a, b):
    low = iota(a.shape, 1) < RANKS
    return jnp.where(low, a, pltpu.roll(b, RANKS, 1)), jnp.where(low, pltpu.roll(a, RANKS, 1), b)


def expert_body(message, gate, up, down, out, flat):
    rows, step = message.shape
    tile = RANKS * PARTS
    pairs = rows // (2 * tile)
    pieces = 4
    size = step // pieces
    for p in range(pieces):
        here = slice(p * size, (p + 1) * size)
        wide = message[:, here].astype(F32).reshape(pairs, 2, tile, size)
        for q, half in enumerate(trade(wide[:, 0], wide[:, 1])):
            flat[:, q * step + p * size : q * step + (p + 1) * size] = half.reshape(rows // 2, size).astype(BF16)
    x = flat[...]
    g = jnp.dot(x, gate[...], preferred_element_type=F32)
    u = jnp.dot(x, up[...], preferred_element_type=F32)
    active = (g / (1.0 + jnp.exp(-g)) * u).astype(BF16)
    for p in range(pieces):
        halves = [
            jnp.dot(
                active, down[:, q * step + p * size : q * step + (p + 1) * size], preferred_element_type=F32
            ).reshape(pairs, tile, size)
            for q in range(PARTS)
        ]
        both = jnp.stack(trade(*halves), axis=1)
        out[:, p * size : (p + 1) * size] = both.reshape(rows, size).astype(BF16)


def combine_body(message, picked, base, out_hbm, out, sems):
    tokens = out.shape[0]
    step = message.shape[1]
    pieces = 4
    size = step // pieces
    copies = []
    for p in range(pieces):
        got = jnp.dot(picked[...], message[:, p * size : (p + 1) * size], preferred_element_type=F32)
        for q in range(PARTS):
            lanes = slice(q * step + p * size, q * step + (p + 1) * size)
            out[:, lanes] = (base[:, lanes].astype(F32) + got[q * tokens : (q + 1) * tokens]).astype(BF16)
            copy = pltpu.make_async_copy(
                out.at[:, lanes], out_hbm.at[:, lanes], sems.at[p * PARTS + q]
            )
            copy.start()
            copies.append(copy)
    for copy in copies:
        copy.wait()


def local(
    glu_value,
    glu_gate,
    conv_kernel,
    conv_bias,
    group_gain,
    group_shift,
    out_weight,
    residual,
    ffn_gain,
    expert_pick,
    pair_logits,
    group_prob,
    gate_weight,
    up_weight,
    down_weight,
):
    shape = jax.ShapeDtypeStruct
    length, width = glu_value.shape
    tokens, model = residual.shape
    experts = lax.axis_size("sp") * lax.axis_size("tp")
    peers = lax.axis_size("sp")
    me = lax.axis_index(("sp", "tp")).astype(jnp.int32).reshape(1)

    n_taps = conv_kernel.shape[0]
    blocks = width // LANE
    cores = lax.axis_size("tp")
    step = model // PARTS
    rows = experts * RANKS * PARTS
    message = shape((rows, step), BF16)
    tail, kernel, vecs, pick, logits, prob = call(
        load_body,
        (
            shape((HALO, width), BF16),
            shape((n_taps, width), BF16),
            shape((8, width), F32),
            shape((2, tokens), jnp.int32),
            shape((2, tokens), F32),
            shape((1, tokens), F32),
        ),
        scratch=(
            pltpu.VMEM((HALO, width), BF16),
            pltpu.VMEM((HALO, width), BF16),
            pltpu.SemaphoreType.DMA((9,)),
        ),
        hbm=range(9),
        n_in=9,
        limit=4,
        flops=1_000_000,
    )(
        glu_value,
        glu_gate,
        conv_kernel,
        conv_bias.reshape(1, width),
        group_gain.reshape(1, width),
        group_shift.reshape(1, width),
        expert_pick.T,
        pair_logits.T,
        group_prob.reshape(1, tokens),
    )
    behind = lax.ppermute(tail, "sp", [(i, (i + 1) % peers) for i in range(peers)])
    crossed = lax.ppermute(
        tail,
        ("sp", "tp"),
        [
            (i * cores + c, (i + 1) % peers * cores + (c + 1) % cores)
            for i in range(peers)
            for c in range(cores)
        ],
    )
    half = length // 2
    front_shape = (blocks, HALO, LANE)
    ext_shape = (blocks, 2 * HALO, LANE)
    mine, packet, front, taps, spread, picked, weight = call(
        functools.partial(conv_body, cores),
        (
            shape((half, width), BF16),
            shape((half + 2 * HALO + 16, width), BF16),
            shape(front_shape, F32),
            shape((blocks, 32, LANE), F32),
            shape((rows, PARTS * tokens), BF16),
            shape((PARTS * tokens, rows), BF16),
            shape(out_weight.shape, BF16),
        ),
        scratch=(
            pltpu.VMEM((length, width), BF16),
            pltpu.VMEM((length, width), BF16),
            pltpu.VMEM((blocks, HALO + length, LANE), F32),
            pltpu.VMEM((length, width), BF16),
            pltpu.VMEM((tokens, LANE), F32),
            pltpu.SemaphoreType.DMA((3,)),
        ),
        smem=(0,),
        hbm=(1, 2, 8),
        n_in=9,
        limit=8,
        flops=3_000_000_000,
    )(me, glu_value, glu_gate, kernel, vecs, pick, logits, prob, out_weight)
    other = lax.ppermute(packet, "tp", [(0, 1), (1, 0)])
    (partial,) = call(
        functools.partial(own_body, cores, n_taps),
        (shape((tokens, model), F32),),
        scratch=(pltpu.VMEM(ext_shape, F32), pltpu.VMEM((half, width), BF16)),
        smem=(0,),
        n_in=8,
        limit=4,
        flops=500_000_000,
    )(me, mine, behind, front, taps, vecs, weight, residual)
    hidden, send = call(
        functools.partial(project_body, cores, n_taps),
        (shape((tokens, model), BF16), message),
        scratch=(
            pltpu.VMEM((PARTS * tokens, step), BF16),
            pltpu.VMEM(ext_shape, F32),
            pltpu.VMEM(front_shape, F32),
            pltpu.VMEM((blocks, 32, LANE), F32),
            pltpu.VMEM((8, width), F32),
            pltpu.VMEM((half, width), BF16),
        ),
        smem=(0,),
        n_in=7,
        limit=16,
        flops=1_000_000_000,
    )(me, other, crossed, weight, partial, ffn_gain.reshape(1, model), spread)
    flat = pltpu.VMEM((RANKS * experts, model), BF16)

    def exchange(x):
        x = x.reshape(experts, RANKS * PARTS, step)
        return lax.all_to_all(x, ("sp", "tp"), 0, 0, tiled=True).reshape(rows, step)

    got = exchange(send)
    (done,) = call(
        expert_body, (message,), scratch=(flat,), n_in=4, limit=24, flops=4_000_000_000
    )(got, gate_weight[0], up_weight[0], down_weight[0])
    back = exchange(done)
    (result,) = call(
        combine_body,
        (shape((tokens, model), BF16),),
        scratch=(pltpu.VMEM((tokens, model), BF16), pltpu.SemaphoreType.DMA((8,))),
        n_in=3,
        out_hbm=(0,),
        limit=12,
        flops=1_000_000_000,
    )(back, picked, hidden)
    return result


def solution(mesh):
    in_specs = (
        P("sp", "tp"),
        P("sp", "tp"),
        P(None, "tp"),
        P("tp"),
        P("tp"),
        P("tp"),
        P(),
        P(("sp", "tp"), None),
        P(),
        P(("sp", "tp"), None),
        P(("sp", "tp"), None),
        P(("sp", "tp")),
        P(("sp", "tp"), None, None),
        P(("sp", "tp"), None, None),
        P(("sp", "tp"), None, None),
    )
    out_specs = P(("sp", "tp"), None)

    return jax.shard_map(local, mesh=mesh, in_specs=in_specs, out_specs=out_specs, check_vma=False)
```

```python
import functools
import jax
import jax.numpy as jnp
from jax import lax
from jax.experimental import pallas as pl
from jax.experimental.pallas import tpu as pltpu
from jax.sharding import PartitionSpec as P


EPS = 1e-06
F32 = jnp.float32
BF16 = jnp.bfloat16
HALO = 32
PARTS = 2
RANKS = 4
LANE = 128
MIB = 1024 * 1024


def iota(shape, axis):
    return lax.broadcasted_iota(jnp.int32, shape, axis)


def onehot(cond):
    return jnp.where(cond, 1.0, 0.0).astype(BF16)


def call(body, out_shape, scratch=(), limit=16, smem=(), hbm=(), n_in=0, out_hbm=(), flops=0):
    kind = {**dict.fromkeys(smem, pltpu.SMEM), **dict.fromkeys(hbm, pltpu.HBM)}
    n_out = len(out_shape)
    run = pl.pallas_call(
        body,
        out_shape=out_shape,
        in_specs=[pl.BlockSpec(memory_space=kind.get(i, pltpu.VMEM)) for i in range(n_in)],
        out_specs=[
            pl.BlockSpec(memory_space=pltpu.HBM if i in out_hbm else pltpu.VMEM) for i in range(n_out)
        ],
        scratch_shapes=list(scratch),
        compiler_params=pltpu.CompilerParams(vmem_limit_bytes=limit * MIB),
        cost_estimate=pl.CostEstimate(flops=flops, bytes_accessed=0, transcendentals=0),
    )
    return lambda *args: run(
        *(pltpu.with_memory_space_constraint(a, pltpu.HBM) if i in hbm else a for i, a in enumerate(args))
    )


def fetch(sources, targets, sems):
    copies = [
        pltpu.make_async_copy(source, target, sems.at[i])
        for i, (source, target) in enumerate(zip(sources, targets, strict=True))
    ]
    for copy in copies:
        copy.start()
    return copies


def route(pick, logits, prob, cols, spread):
    e_iota = iota((LANE, LANE), 0)
    n_iota = iota((LANE, LANE), 1)
    picks = [pick[k : k + 1, :] for k in range(2)]
    hits = [(e_iota == p).astype(F32) for p in picks]
    both = (hits[0] + hits[1]).astype(BF16)
    before = jnp.dot(both, onehot(e_iota < n_iota), preferred_element_type=F32)
    places = []
    for k in range(2):
        rank = jnp.sum(before * hits[k], axis=0, keepdims=True)
        places.append(RANKS * picks[k] + rank.astype(jnp.int32))
    first = prob[...] * jax.nn.sigmoid(logits[0:1, :] - logits[1:2, :])
    second = prob[...] * jax.nn.sigmoid(logits[1:2, :] - logits[0:1, :])
    rows = [places[0].astype(F32), places[1].astype(F32), first, second]
    table = jnp.zeros((LANE, LANE), F32)
    for i, row in enumerate(rows):
        table = jnp.where(e_iota == i, row, table)
    cols[...] = table.T
    part = e_iota // RANKS % PARTS
    for b in range(spread.shape[0] // LANE):
        row = e_iota + b * LANE
        code = row // (RANKS * PARTS) * RANKS + row % RANKS
        hit = jnp.logical_or(code == places[0], code == places[1])
        for q in range(PARTS):
            spread[b * LANE : (b + 1) * LANE, q * LANE : (q + 1) * LANE] = onehot(
                jnp.logical_and(hit, part == q)
            )


def select(cols, picked):
    tokens, rows = cols.shape[0], picked.shape[1]
    slot = iota((tokens, rows), 1)
    code = (slot // (RANKS * PARTS) * RANKS + slot % RANKS).astype(F32)
    share = jnp.where(cols[:, 0:1] == code, cols[:, 2:3], 0.0)
    share = jnp.where(cols[:, 1:2] == code, cols[:, 3:4], share)
    part = slot // RANKS % PARTS
    for q in range(PARTS):
        picked[q * tokens : (q + 1) * tokens, :] = jnp.where(part == q, share, 0.0).astype(BF16)


def load_body(
    value_in, gate_in, kernel_in, bias_in, gain_in, shift_in, pick_in, logits_in, prob_in,
    tail, kernel, vecs, pick, logits, prob,
    value, gate, sems,
):
    cut = value_in.shape[0] - HALO
    copies = fetch(
        (
            value_in.at[pl.ds(cut, HALO), :], gate_in.at[pl.ds(cut, HALO), :],
            kernel_in, bias_in, gain_in, shift_in, pick_in, logits_in, prob_in,
        ),
        (value, gate, kernel, vecs.at[0:1], vecs.at[1:2], vecs.at[2:3], pick, logits, prob),
        sems,
    )
    for copy in copies[:2]:
        copy.wait()
    glued = value[...].astype(F32) * jax.nn.sigmoid(gate[...].astype(F32))
    tail[...] = glued.astype(BF16)
    for copy in copies[2:]:
        copy.wait()


def taps_and_norm(ext, taps, vecs, b, start, rows, n_taps):
    lanes = pl.ds(pl.multiple_of(b * LANE, LANE), LANE)
    acc = jnp.broadcast_to(vecs[0:1, lanes], (rows, LANE))
    for j in range(n_taps):
        at = start + HALO - (n_taps - 1) + j
        acc = acc + taps[b, j : j + 1, :] * ext[b, at : at + rows, :]
    centre = jnp.mean(acc, axis=-1, keepdims=True)
    away = acc - centre
    variance = jnp.mean(away * away, axis=-1, keepdims=True)
    v = away * lax.rsqrt(variance + EPS) * vecs[1:2, lanes] + vecs[2:3, lanes]
    return (v / (1.0 + jnp.exp(-v))).astype(BF16)


def conv_body(
    cores, me, value_in, gate_in, kernel, vecs, pick, logits, prob, weight_in,
    mine, packet, front, taps, spread, picked, weight,
    value, gate, ext, mixed, cols, sems,
):
    *copies, large = fetch((value_in, gate_in, weight_in), (value, gate, weight), sems)
    route(pick, logits, prob, cols, spread)
    select(cols, picked)
    for copy in copies:
        copy.wait()
    n_taps, width = kernel.shape
    length = value.shape[0]
    half = length // 2
    blocks = width // LANE
    for b in range(blocks):
        lanes = slice(b * LANE, (b + 1) * LANE)
        taps[b, 0:n_taps, :] = kernel[:, lanes].astype(F32)
        glued = (value[:, lanes].astype(F32) * jax.nn.sigmoid(gate[:, lanes].astype(F32))).astype(BF16)
        ext[b, HALO : HALO + length, :] = glued.astype(F32)
        front[b, :, :] = ext[b, HALO : 2 * HALO, :]
        packet[half : half + HALO, lanes] = glued[0:HALO]
    packet[half + HALO : half + HALO + n_taps, :] = kernel[...]
    piece = iota((16, width), 0)
    pieces = jnp.zeros((16, width), F32)
    for i in range(3):
        left = vecs[i : i + 1, :]
        for j in range(3):
            top = left.astype(BF16).astype(F32)
            pieces = jnp.where(piece == 3 * i + j, top, pieces)
            left = left - top
    packet[half + 2 * HALO : half + 2 * HALO + 16, :] = pieces.astype(BF16)
    mixed[0:HALO, :] = jnp.zeros((HALO, width), BF16)

    def block(b, carry):
        lanes = pl.ds(pl.multiple_of(b * LANE, LANE), LANE)
        for r in range(HALO, length, HALO):
            mixed[r : r + HALO, lanes] = taps_and_norm(ext, taps, vecs, b, r, HALO, n_taps)
        return carry

    lax.fori_loop(0, blocks, block, 0)
    core = lax.rem(me[0], cores)
    mine[...] = mixed[pl.ds(pl.multiple_of(core * half, half), half), :]
    packet[0:half, :] = mixed[pl.ds(pl.multiple_of((1 - core) * half, half), half), :]
    large.wait()


def head(me, cores, halo, front, taps, vecs, ext, out, n_taps):
    for b in range(front.shape[0]):
        lanes = slice(b * LANE, (b + 1) * LANE)
        ext[b, 0:HALO, :] = jnp.where(me[0] >= cores, halo[:, lanes].astype(F32), 0.0)
        ext[b, HALO : 2 * HALO, :] = front[b, :, :]
    for b in range(front.shape[0]):
        lanes = slice(b * LANE, (b + 1) * LANE)
        out[0:HALO, lanes] = taps_and_norm(ext, taps, vecs, b, 0, HALO, n_taps)


def own_body(cores, n_taps, me, mine, halo, front, taps, vecs, weight, residual, partial, ext, full):
    half = mine.shape[1]
    step = partial.shape[1] // 4
    core = lax.rem(me[0], cores)
    full[...] = mine[...]

    @pl.when(core == 0)
    def _():
        head(me, cores, halo, front, taps, vecs, ext, full, n_taps)

    here = pl.ds(pl.multiple_of(core * half, half), half)
    for q in range(4):
        lanes = slice(q * step, (q + 1) * step)
        acc = jnp.dot(full[...], weight[here, lanes], preferred_element_type=F32)
        partial[:, lanes] = acc + residual[:, lanes].astype(F32)


def project_body(
    cores, n_taps, me, packet, halo, weight, partial, gain, spread,
    hidden, out,
    stacked, ext, front, taps, vecs, full,
):
    tokens, width = partial.shape
    half = packet.shape[1]
    core = lax.rem(me[0], cores)
    full[...] = packet[0:tokens, :]

    @pl.when(core == 0)
    def _():
        pieces = packet[tokens + 2 * HALO : tokens + 2 * HALO + 16, :].astype(F32)
        for i in range(3):
            vecs[i : i + 1, :] = (pieces[3 * i : 3 * i + 1] + pieces[3 * i + 1 : 3 * i + 2]) + pieces[
                3 * i + 2 : 3 * i + 3
            ]
        for b in range(front.shape[0]):
            lanes = slice(b * LANE, (b + 1) * LANE)
            front[b, :, :] = packet[tokens : tokens + HALO, lanes].astype(F32)
            taps[b, 0:n_taps, :] = packet[tokens + HALO : tokens + HALO + n_taps, lanes].astype(F32)
        head(me, cores, halo, front, taps, vecs, ext, full, n_taps)

    step = width // 4
    there = pl.ds(pl.multiple_of((1 - core) * half, half), half)
    total = jnp.zeros((tokens, 1), F32)
    for q in range(4):
        lanes = slice(q * step, (q + 1) * step)
        acc = jnp.dot(full[...], weight[there, lanes], preferred_element_type=F32)
        rounded = (acc + partial[:, lanes]).astype(BF16)
        hidden[:, lanes] = rounded
        wide = rounded.astype(F32)
        total = total + jnp.sum(wide * wide, axis=-1, keepdims=True)
    scale = lax.rsqrt(total / width + EPS)
    step = width // PARTS
    for q in range(PARTS):
        lanes = slice(q * step, (q + 1) * step)
        stacked[q * tokens : (q + 1) * tokens, :] = (
            hidden[:, lanes].astype(F32) * scale * gain[:, lanes]
        ).astype(BF16)
    chunk = 2 * LANE
    for b in range(out.shape[0] // chunk):
        rows = slice(b * chunk, (b + 1) * chunk)
        out[rows, :] = jnp.dot(spread[rows, :], stacked[...], preferred_element_type=F32).astype(BF16)


def trade(a, b):
    low = iota(a.shape, 1) < RANKS
    return jnp.where(low, a, pltpu.roll(b, RANKS, 1)), jnp.where(low, pltpu.roll(a, RANKS, 1), b)


def expert_body(message, gate, up, down, out, flat):
    rows, step = message.shape
    tile = RANKS * PARTS
    pairs = rows // (2 * tile)
    pieces = 4
    size = step // pieces
    for p in range(pieces):
        here = slice(p * size, (p + 1) * size)
        wide = message[:, here].astype(F32).reshape(pairs, 2, tile, size)
        for q, half in enumerate(trade(wide[:, 0], wide[:, 1])):
            flat[:, q * step + p * size : q * step + (p + 1) * size] = half.reshape(rows // 2, size).astype(BF16)
    x = flat[...]
    g = jnp.dot(x, gate[...], preferred_element_type=F32)
    u = jnp.dot(x, up[...], preferred_element_type=F32)
    active = (g / (1.0 + jnp.exp(-g)) * u).astype(BF16)
    for p in range(pieces):
        halves = [
            jnp.dot(
                active, down[:, q * step + p * size : q * step + (p + 1) * size], preferred_element_type=F32
            ).reshape(pairs, tile, size)
            for q in range(PARTS)
        ]
        both = jnp.stack(trade(*halves), axis=1)
        out[:, p * size : (p + 1) * size] = both.reshape(rows, size).astype(BF16)


def combine_body(message, picked, base, out_hbm, out, sems):
    tokens = out.shape[0]
    step = message.shape[1]
    pieces = 4
    size = step // pieces
    copies = []
    for p in range(pieces):
        got = jnp.dot(picked[...], message[:, p * size : (p + 1) * size], preferred_element_type=F32)
        for q in range(PARTS):
            lanes = slice(q * step + p * size, q * step + (p + 1) * size)
            out[:, lanes] = (base[:, lanes].astype(F32) + got[q * tokens : (q + 1) * tokens]).astype(BF16)
            copy = pltpu.make_async_copy(
                out.at[:, lanes], out_hbm.at[:, lanes], sems.at[p * PARTS + q]
            )
            copy.start()
            copies.append(copy)
    for copy in copies:
        copy.wait()


def local(
    glu_value,
    glu_gate,
    conv_kernel,
    conv_bias,
    group_gain,
    group_shift,
    out_weight,
    residual,
    ffn_gain,
    expert_pick,
    pair_logits,
    group_prob,
    gate_weight,
    up_weight,
    down_weight,
):
    shape = jax.ShapeDtypeStruct
    length, width = glu_value.shape
    tokens, model = residual.shape
    experts = lax.axis_size("sp") * lax.axis_size("tp")
    peers = lax.axis_size("sp")
    me = lax.axis_index(("sp", "tp")).astype(jnp.int32).reshape(1)

    n_taps = conv_kernel.shape[0]
    blocks = width // LANE
    cores = lax.axis_size("tp")
    step = model // PARTS
    rows = experts * RANKS * PARTS
    message = shape((rows, step), BF16)
    tail, kernel, vecs, pick, logits, prob = call(
        load_body,
        (
            shape((HALO, width), BF16),
            shape((n_taps, width), BF16),
            shape((8, width), F32),
            shape((2, tokens), jnp.int32),
            shape((2, tokens), F32),
            shape((1, tokens), F32),
        ),
        scratch=(
            pltpu.VMEM((HALO, width), BF16),
            pltpu.VMEM((HALO, width), BF16),
            pltpu.SemaphoreType.DMA((9,)),
        ),
        hbm=range(9),
        n_in=9,
        limit=4,
        flops=1_000_000,
    )(
        glu_value,
        glu_gate,
        conv_kernel,
        conv_bias.reshape(1, width),
        group_gain.reshape(1, width),
        group_shift.reshape(1, width),
        expert_pick.T,
        pair_logits.T,
        group_prob.reshape(1, tokens),
    )
    ahead = [(i + 1) % peers * cores for i in range(peers)]
    crossed = lax.ppermute(
        tail,
        ("sp", "tp"),
        [(i * cores + 1, ahead[i]) for i in range(peers)] + [(i * cores, i * cores + 1) for i in range(peers)],
    )
    behind = lax.ppermute(
        tail,
        ("sp", "tp"),
        [(i * cores, ahead[i]) for i in range(peers)] + [(i * cores + 1, i * cores + 1) for i in range(peers)],
    )
    half = length // 2
    front_shape = (blocks, HALO, LANE)
    ext_shape = (blocks, 2 * HALO, LANE)
    mine, packet, front, taps, spread, picked, weight = call(
        functools.partial(conv_body, cores),
        (
            shape((half, width), BF16),
            shape((half + 2 * HALO + 16, width), BF16),
            shape(front_shape, F32),
            shape((blocks, 32, LANE), F32),
            shape((rows, PARTS * tokens), BF16),
            shape((PARTS * tokens, rows), BF16),
            shape(out_weight.shape, BF16),
        ),
        scratch=(
            pltpu.VMEM((length, width), BF16),
            pltpu.VMEM((length, width), BF16),
            pltpu.VMEM((blocks, HALO + length, LANE), F32),
            pltpu.VMEM((length, width), BF16),
            pltpu.VMEM((tokens, LANE), F32),
            pltpu.SemaphoreType.DMA((3,)),
        ),
        smem=(0,),
        hbm=(1, 2, 8),
        n_in=9,
        limit=8,
        flops=3_000_000_000,
    )(me, glu_value, glu_gate, kernel, vecs, pick, logits, prob, out_weight)
    other = lax.ppermute(packet, "tp", [(0, 1), (1, 0)])
    (partial,) = call(
        functools.partial(own_body, cores, n_taps),
        (shape((tokens, model), F32),),
        scratch=(pltpu.VMEM(ext_shape, F32), pltpu.VMEM((half, width), BF16)),
        smem=(0,),
        n_in=8,
        limit=4,
        flops=500_000_000,
    )(me, mine, behind, front, taps, vecs, weight, residual)
    hidden, send = call(
        functools.partial(project_body, cores, n_taps),
        (shape((tokens, model), BF16), message),
        scratch=(
            pltpu.VMEM((PARTS * tokens, step), BF16),
            pltpu.VMEM(ext_shape, F32),
            pltpu.VMEM(front_shape, F32),
            pltpu.VMEM((blocks, 32, LANE), F32),
            pltpu.VMEM((8, width), F32),
            pltpu.VMEM((half, width), BF16),
        ),
        smem=(0,),
        n_in=7,
        limit=16,
        flops=1_000_000_000,
    )(me, other, crossed, weight, partial, ffn_gain.reshape(1, model), spread)
    flat = pltpu.VMEM((RANKS * experts, model), BF16)

    def exchange(x):
        x = x.reshape(experts, RANKS * PARTS, step)
        return lax.all_to_all(x, ("sp", "tp"), 0, 0, tiled=True).reshape(rows, step)

    got = exchange(send)
    (done,) = call(
        expert_body, (message,), scratch=(flat,), n_in=4, limit=24, flops=4_000_000_000
    )(got, gate_weight[0], up_weight[0], down_weight[0])
    back = exchange(done)
    (result,) = call(
        combine_body,
        (shape((tokens, model), BF16),),
        scratch=(pltpu.VMEM((tokens, model), BF16), pltpu.SemaphoreType.DMA((8,))),
        n_in=3,
        out_hbm=(0,),
        limit=12,
        flops=1_000_000_000,
    )(back, picked, hidden)
    return result


def solution(mesh):
    in_specs = (
        P("sp", "tp"),
        P("sp", "tp"),
        P(None, "tp"),
        P("tp"),
        P("tp"),
        P("tp"),
        P(),
        P(("sp", "tp"), None),
        P(),
        P(("sp", "tp"), None),
        P(("sp", "tp"), None),
        P(("sp", "tp")),
        P(("sp", "tp"), None, None),
        P(("sp", "tp"), None, None),
        P(("sp", "tp"), None, None),
    )
    out_specs = P(("sp", "tp"), None)

    return jax.shard_map(local, mesh=mesh, in_specs=in_specs, out_specs=out_specs, check_vma=False)
```

```python
import functools
import jax
import jax.numpy as jnp
from jax import lax
from jax.experimental import pallas as pl
from jax.experimental.pallas import tpu as pltpu
from jax.sharding import PartitionSpec as P


EPS = 1e-06
F32 = jnp.float32
BF16 = jnp.bfloat16
HALO = 32
PARTS = 2
RANKS = 4
LANE = 128
MIB = 1024 * 1024


def iota(shape, axis):
    return lax.broadcasted_iota(jnp.int32, shape, axis)


def onehot(cond):
    return jnp.where(cond, 1.0, 0.0).astype(BF16)


def call(body, out_shape, scratch=(), limit=16, smem=(), hbm=(), n_in=0, out_hbm=(), flops=0):
    kind = {**dict.fromkeys(smem, pltpu.SMEM), **dict.fromkeys(hbm, pltpu.HBM)}
    n_out = len(out_shape)
    run = pl.pallas_call(
        body,
        out_shape=out_shape,
        in_specs=[pl.BlockSpec(memory_space=kind.get(i, pltpu.VMEM)) for i in range(n_in)],
        out_specs=[
            pl.BlockSpec(memory_space=pltpu.HBM if i in out_hbm else pltpu.VMEM) for i in range(n_out)
        ],
        scratch_shapes=list(scratch),
        compiler_params=pltpu.CompilerParams(vmem_limit_bytes=limit * MIB),
        cost_estimate=pl.CostEstimate(flops=flops, bytes_accessed=0, transcendentals=0),
    )
    return lambda *args: run(
        *(pltpu.with_memory_space_constraint(a, pltpu.HBM) if i in hbm else a for i, a in enumerate(args))
    )


def fetch(sources, targets, sems):
    copies = [
        pltpu.make_async_copy(source, target, sems.at[i])
        for i, (source, target) in enumerate(zip(sources, targets, strict=True))
    ]
    for copy in copies:
        copy.start()
    return copies


def route(pick, logits, prob, cols, spread):
    e_iota = iota((LANE, LANE), 0)
    n_iota = iota((LANE, LANE), 1)
    picks = [pick[k : k + 1, :] for k in range(2)]
    hits = [(e_iota == p).astype(F32) for p in picks]
    both = (hits[0] + hits[1]).astype(BF16)
    before = jnp.dot(both, onehot(e_iota < n_iota), preferred_element_type=F32)
    places = []
    for k in range(2):
        rank = jnp.sum(before * hits[k], axis=0, keepdims=True)
        places.append(RANKS * picks[k] + rank.astype(jnp.int32))
    first = prob[...] * jax.nn.sigmoid(logits[0:1, :] - logits[1:2, :])
    second = prob[...] * jax.nn.sigmoid(logits[1:2, :] - logits[0:1, :])
    rows = [places[0].astype(F32), places[1].astype(F32), first, second]
    table = jnp.zeros((LANE, LANE), F32)
    for i, row in enumerate(rows):
        table = jnp.where(e_iota == i, row, table)
    cols[...] = table.T
    part = e_iota // RANKS % PARTS
    for b in range(spread.shape[0] // LANE):
        row = e_iota + b * LANE
        code = row // (RANKS * PARTS) * RANKS + row % RANKS
        hit = jnp.logical_or(code == places[0], code == places[1])
        for q in range(PARTS):
            spread[b * LANE : (b + 1) * LANE, q * LANE : (q + 1) * LANE] = onehot(
                jnp.logical_and(hit, part == q)
            )


def select(cols, picked):
    tokens, rows = cols.shape[0], picked.shape[1]
    slot = iota((tokens, rows), 1)
    code = (slot // (RANKS * PARTS) * RANKS + slot % RANKS).astype(F32)
    share = jnp.where(cols[:, 0:1] == code, cols[:, 2:3], 0.0)
    share = jnp.where(cols[:, 1:2] == code, cols[:, 3:4], share)
    part = slot // RANKS % PARTS
    for q in range(PARTS):
        picked[q * tokens : (q + 1) * tokens, :] = jnp.where(part == q, share, 0.0).astype(BF16)


def load_body(
    value_in, gate_in, kernel_in, bias_in, gain_in, shift_in, pick_in, logits_in, prob_in,
    tail, kernel, vecs, pick, logits, prob,
    value, gate, sems,
):
    cut = value_in.shape[0] - HALO
    copies = fetch(
        (
            value_in.at[pl.ds(cut, HALO), :], gate_in.at[pl.ds(cut, HALO), :],
            kernel_in, bias_in, gain_in, shift_in, pick_in, logits_in, prob_in,
        ),
        (value, gate, kernel, vecs.at[0:1], vecs.at[1:2], vecs.at[2:3], pick, logits, prob),
        sems,
    )
    for copy in copies[:2]:
        copy.wait()
    glued = value[...].astype(F32) * jax.nn.sigmoid(gate[...].astype(F32))
    tail[...] = glued.astype(BF16)
    for copy in copies[2:]:
        copy.wait()


def taps_and_norm(ext, taps, vecs, b, start, rows, n_taps):
    lanes = pl.ds(pl.multiple_of(b * LANE, LANE), LANE)
    acc = jnp.broadcast_to(vecs[0:1, lanes], (rows, LANE))
    for j in range(n_taps):
        at = start + HALO - (n_taps - 1) + j
        acc = acc + taps[b, j : j + 1, :] * ext[b, at : at + rows, :]
    centre = jnp.mean(acc, axis=-1, keepdims=True)
    away = acc - centre
    variance = jnp.mean(away * away, axis=-1, keepdims=True)
    v = away * lax.rsqrt(variance + EPS) * vecs[1:2, lanes] + vecs[2:3, lanes]
    return (v / (1.0 + jnp.exp(-v))).astype(BF16)


def gate_body(
    value, gate, kernel, vecs, pick, logits, prob,
    ext, taps, aside, spread, picked,
    cols,
):
    n_taps, width = kernel.shape
    for b in range(width // LANE):
        lanes = slice(b * LANE, (b + 1) * LANE)
        taps[b, 0:n_taps, :] = kernel[:, lanes].astype(F32)
        glued = (value[:, lanes].astype(F32) * jax.nn.sigmoid(gate[:, lanes].astype(F32))).astype(BF16)
        ext[b, :, :] = glued.astype(F32)
        aside[0:HALO, lanes] = glued[0:HALO]
    aside[HALO : HALO + n_taps, :] = kernel[...]
    piece = iota((16, width), 0)
    pieces = jnp.zeros((16, width), F32)
    for i in range(3):
        left = vecs[i : i + 1, :]
        for j in range(3):
            top = left.astype(BF16).astype(F32)
            pieces = jnp.where(piece == 3 * i + j, top, pieces)
            left = left - top
    aside[2 * HALO : 2 * HALO + 16, :] = pieces.astype(BF16)
    route(pick, logits, prob, cols, spread)
    select(cols, picked)


def conv_body(cores, n_taps, me, ext, taps, vecs, aside, mine, packet, mixed):
    blocks, length, _ = ext.shape
    half = length // 2
    width = mixed.shape[1]
    packet[half : half + aside.shape[0], :] = aside[...]
    mixed[0:HALO, :] = jnp.zeros((HALO, width), BF16)

    def block(b, carry):
        lanes = pl.ds(pl.multiple_of(b * LANE, LANE), LANE)
        for r in range(HALO, length, HALO):
            mixed[r : r + HALO, lanes] = taps_and_norm(ext, taps, vecs, b, r - HALO, HALO, n_taps)
        return carry

    lax.fori_loop(0, blocks, block, 0)
    core = lax.rem(me[0], cores)
    mine[...] = mixed[pl.ds(pl.multiple_of(core * half, half), half), :]
    packet[0:half, :] = mixed[pl.ds(pl.multiple_of((1 - core) * half, half), half), :]


def head(me, cores, halo, front, taps, vecs, ext, out, n_taps):
    for b in range(ext.shape[0]):
        lanes = slice(b * LANE, (b + 1) * LANE)
        ext[b, 0:HALO, :] = jnp.where(me[0] >= cores, halo[:, lanes].astype(F32), 0.0)
        ext[b, HALO : 2 * HALO, :] = front[b, 0:HALO, :]
    for b in range(ext.shape[0]):
        lanes = slice(b * LANE, (b + 1) * LANE)
        out[0:HALO, lanes] = taps_and_norm(ext, taps, vecs, b, 0, HALO, n_taps)


def own_body(cores, n_taps, me, mine, halo, front, taps, vecs, weight, residual, partial, ext, full):
    half = mine.shape[1]
    step = partial.shape[1] // 4
    core = lax.rem(me[0], cores)
    full[...] = mine[...]

    @pl.when(core == 0)
    def _():
        head(me, cores, halo, front, taps, vecs, ext, full, n_taps)

    here = pl.ds(pl.multiple_of(core * half, half), half)
    for q in range(4):
        lanes = slice(q * step, (q + 1) * step)
        acc = jnp.dot(full[...], weight[here, lanes], preferred_element_type=F32)
        partial[:, lanes] = acc + residual[:, lanes].astype(F32)


def project_body(
    cores, n_taps, me, packet, halo, weight, partial, gain, spread,
    hidden, out,
    stacked, ext, front, taps, vecs, full,
):
    tokens, width = partial.shape
    half = packet.shape[1]
    core = lax.rem(me[0], cores)
    full[...] = packet[0:tokens, :]

    @pl.when(core == 0)
    def _():
        pieces = packet[tokens + 2 * HALO : tokens + 2 * HALO + 16, :].astype(F32)
        for i in range(3):
            vecs[i : i + 1, :] = (pieces[3 * i : 3 * i + 1] + pieces[3 * i + 1 : 3 * i + 2]) + pieces[
                3 * i + 2 : 3 * i + 3
            ]
        for b in range(front.shape[0]):
            lanes = slice(b * LANE, (b + 1) * LANE)
            front[b, :, :] = packet[tokens : tokens + HALO, lanes].astype(F32)
            taps[b, 0:n_taps, :] = packet[tokens + HALO : tokens + HALO + n_taps, lanes].astype(F32)
        head(me, cores, halo, front, taps, vecs, ext, full, n_taps)

    step = width // 4
    there = pl.ds(pl.multiple_of((1 - core) * half, half), half)
    total = jnp.zeros((tokens, 1), F32)
    for q in range(4):
        lanes = slice(q * step, (q + 1) * step)
        acc = jnp.dot(full[...], weight[there, lanes], preferred_element_type=F32)
        rounded = (acc + partial[:, lanes]).astype(BF16)
        hidden[:, lanes] = rounded
        wide = rounded.astype(F32)
        total = total + jnp.sum(wide * wide, axis=-1, keepdims=True)
    scale = lax.rsqrt(total / width + EPS)
    step = width // PARTS
    for q in range(PARTS):
        lanes = slice(q * step, (q + 1) * step)
        stacked[q * tokens : (q + 1) * tokens, :] = (
            hidden[:, lanes].astype(F32) * scale * gain[:, lanes]
        ).astype(BF16)
    chunk = 2 * LANE
    for b in range(out.shape[0] // chunk):
        rows = slice(b * chunk, (b + 1) * chunk)
        out[rows, :] = jnp.dot(spread[rows, :], stacked[...], preferred_element_type=F32).astype(BF16)


def trade(a, b):
    low = iota(a.shape, 1) < RANKS
    return jnp.where(low, a, pltpu.roll(b, RANKS, 1)), jnp.where(low, pltpu.roll(a, RANKS, 1), b)


def expert_body(message, gate, up, down, out, flat):
    rows, step = message.shape
    tile = RANKS * PARTS
    pairs = rows // (2 * tile)
    pieces = 4
    size = step // pieces
    for p in range(pieces):
        here = slice(p * size, (p + 1) * size)
        wide = message[:, here].astype(F32).reshape(pairs, 2, tile, size)
        for q, half in enumerate(trade(wide[:, 0], wide[:, 1])):
            flat[:, q * step + p * size : q * step + (p + 1) * size] = half.reshape(rows // 2, size).astype(BF16)
    x = flat[...]
    g = jnp.dot(x, gate[...], preferred_element_type=F32)
    u = jnp.dot(x, up[...], preferred_element_type=F32)
    active = (g / (1.0 + jnp.exp(-g)) * u).astype(BF16)
    for p in range(pieces):
        halves = [
            jnp.dot(
                active, down[:, q * step + p * size : q * step + (p + 1) * size], preferred_element_type=F32
            ).reshape(pairs, tile, size)
            for q in range(PARTS)
        ]
        both = jnp.stack(trade(*halves), axis=1)
        out[:, p * size : (p + 1) * size] = both.reshape(rows, size).astype(BF16)


def combine_body(message, picked, base, out_hbm, out, sems):
    tokens = out.shape[0]
    step = message.shape[1]
    pieces = 4
    size = step // pieces
    copies = []
    for p in range(pieces):
        got = jnp.dot(picked[...], message[:, p * size : (p + 1) * size], preferred_element_type=F32)
        for q in range(PARTS):
            lanes = slice(q * step + p * size, q * step + (p + 1) * size)
            out[:, lanes] = (base[:, lanes].astype(F32) + got[q * tokens : (q + 1) * tokens]).astype(BF16)
            copy = pltpu.make_async_copy(
                out.at[:, lanes], out_hbm.at[:, lanes], sems.at[p * PARTS + q]
            )
            copy.start()
            copies.append(copy)
    for copy in copies:
        copy.wait()


def local(
    glu_value,
    glu_gate,
    conv_kernel,
    conv_bias,
    group_gain,
    group_shift,
    out_weight,
    residual,
    ffn_gain,
    expert_pick,
    pair_logits,
    group_prob,
    gate_weight,
    up_weight,
    down_weight,
):
    shape = jax.ShapeDtypeStruct
    length, width = glu_value.shape
    tokens, model = residual.shape
    experts = lax.axis_size("sp") * lax.axis_size("tp")
    peers = lax.axis_size("sp")
    me = lax.axis_index(("sp", "tp")).astype(jnp.int32).reshape(1)

    n_taps = conv_kernel.shape[0]
    blocks = width // LANE
    cores = lax.axis_size("tp")
    step = model // PARTS
    rows = experts * RANKS * PARTS
    message = shape((rows, step), BF16)
    tail, kernel, vecs, pick, logits, prob = call(
        load_body,
        (
            shape((HALO, width), BF16),
            shape((n_taps, width), BF16),
            shape((8, width), F32),
            shape((2, tokens), jnp.int32),
            shape((2, tokens), F32),
            shape((1, tokens), F32),
        ),
        scratch=(
            pltpu.VMEM((HALO, width), BF16),
            pltpu.VMEM((HALO, width), BF16),
            pltpu.SemaphoreType.DMA((9,)),
        ),
        hbm=range(9),
        n_in=9,
        limit=4,
        flops=5_000_000_000,
    )(
        glu_value,
        glu_gate,
        conv_kernel,
        conv_bias.reshape(1, width),
        group_gain.reshape(1, width),
        group_shift.reshape(1, width),
        expert_pick.T,
        pair_logits.T,
        group_prob.reshape(1, tokens),
    )
    behind = lax.ppermute(tail, "sp", [(i, (i + 1) % peers) for i in range(peers)])
    crossed = lax.ppermute(
        tail,
        ("sp", "tp"),
        [
            (i * cores + c, (i + 1) % peers * cores + (c + 1) % cores)
            for i in range(peers)
            for c in range(cores)
        ],
    )
    half = length // 2
    front_shape = (blocks, HALO, LANE)
    ext_shape = (blocks, 2 * HALO, LANE)
    ext, taps, aside, spread, picked = call(
        gate_body,
        (
            shape((blocks, length, LANE), F32),
            shape((blocks, 32, LANE), F32),
            shape((2 * HALO + 16, width), BF16),
            shape((rows, PARTS * tokens), BF16),
            shape((PARTS * tokens, rows), BF16),
        ),
        scratch=(pltpu.VMEM((tokens, LANE), F32),),
        n_in=7,
        limit=4,
        flops=3_000_000_000,
    )(glu_value, glu_gate, kernel, vecs, pick, logits, prob)
    mine, packet = call(
        functools.partial(conv_body, cores, n_taps),
        (shape((half, width), BF16), shape((half + 2 * HALO + 16, width), BF16)),
        scratch=(pltpu.VMEM((length, width), BF16),),
        smem=(0,),
        n_in=5,
        limit=4,
        flops=3_000_000_000,
    )(me, ext, taps, vecs, aside)
    other = lax.ppermute(packet, "tp", [(0, 1), (1, 0)])
    (partial,) = call(
        functools.partial(own_body, cores, n_taps),
        (shape((tokens, model), F32),),
        scratch=(pltpu.VMEM(ext_shape, F32), pltpu.VMEM((half, width), BF16)),
        smem=(0,),
        n_in=8,
        limit=4,
        flops=500_000_000,
    )(me, mine, behind, ext, taps, vecs, out_weight, residual)
    hidden, send = call(
        functools.partial(project_body, cores, n_taps),
        (shape((tokens, model), BF16), message),
        scratch=(
            pltpu.VMEM((PARTS * tokens, step), BF16),
            pltpu.VMEM(ext_shape, F32),
            pltpu.VMEM(front_shape, F32),
            pltpu.VMEM((blocks, 32, LANE), F32),
            pltpu.VMEM((8, width), F32),
            pltpu.VMEM((half, width), BF16),
        ),
        smem=(0,),
        n_in=7,
        limit=16,
        flops=1_000_000_000,
    )(me, other, crossed, out_weight, partial, ffn_gain.reshape(1, model), spread)
    flat = pltpu.VMEM((RANKS * experts, model), BF16)

    def exchange(x):
        x = x.reshape(experts, RANKS * PARTS, step)
        return lax.all_to_all(x, ("sp", "tp"), 0, 0, tiled=True).reshape(rows, step)

    got = exchange(send)
    (done,) = call(
        expert_body, (message,), scratch=(flat,), n_in=4, limit=24, flops=4_000_000_000
    )(got, gate_weight[0], up_weight[0], down_weight[0])
    back = exchange(done)
    (result,) = call(
        combine_body,
        (shape((tokens, model), BF16),),
        scratch=(pltpu.VMEM((tokens, model), BF16), pltpu.SemaphoreType.DMA((8,))),
        n_in=3,
        out_hbm=(0,),
        limit=12,
        flops=1_000_000_000,
    )(back, picked, hidden)
    return result


def solution(mesh):
    in_specs = (
        P("sp", "tp"),
        P("sp", "tp"),
        P(None, "tp"),
        P("tp"),
        P("tp"),
        P("tp"),
        P(),
        P(("sp", "tp"), None),
        P(),
        P(("sp", "tp"), None),
        P(("sp", "tp"), None),
        P(("sp", "tp")),
        P(("sp", "tp"), None, None),
        P(("sp", "tp"), None, None),
        P(("sp", "tp"), None, None),
    )
    out_specs = P(("sp", "tp"), None)

    return jax.shard_map(local, mesh=mesh, in_specs=in_specs, out_specs=out_specs, check_vma=False)
```

```python
import functools
import jax
import jax.numpy as jnp
from jax import lax
from jax.experimental import pallas as pl
from jax.experimental.pallas import tpu as pltpu
from jax.sharding import PartitionSpec as P


EPS = 1e-06
F32 = jnp.float32
BF16 = jnp.bfloat16
HALO = 32
PARTS = 2
RANKS = 4
LANE = 128
MIB = 1024 * 1024


def iota(shape, axis):
    return lax.broadcasted_iota(jnp.int32, shape, axis)


def onehot(cond):
    return jnp.where(cond, 1.0, 0.0).astype(BF16)


def call(body, out_shape, scratch=(), limit=16, smem=(), hbm=(), n_in=0, out_hbm=(), flops=0):
    kind = {**dict.fromkeys(smem, pltpu.SMEM), **dict.fromkeys(hbm, pltpu.HBM)}
    n_out = len(out_shape)
    run = pl.pallas_call(
        body,
        out_shape=out_shape,
        in_specs=[pl.BlockSpec(memory_space=kind.get(i, pltpu.VMEM)) for i in range(n_in)],
        out_specs=[
            pl.BlockSpec(memory_space=pltpu.HBM if i in out_hbm else pltpu.VMEM) for i in range(n_out)
        ],
        scratch_shapes=list(scratch),
        compiler_params=pltpu.CompilerParams(vmem_limit_bytes=limit * MIB),
        cost_estimate=pl.CostEstimate(flops=flops, bytes_accessed=0, transcendentals=0),
    )
    return lambda *args: run(
        *(pltpu.with_memory_space_constraint(a, pltpu.HBM) if i in hbm else a for i, a in enumerate(args))
    )


def fetch(sources, targets, sems):
    copies = [
        pltpu.make_async_copy(source, target, sems.at[i])
        for i, (source, target) in enumerate(zip(sources, targets, strict=True))
    ]
    for copy in copies:
        copy.start()
    return copies


def route(pick, logits, prob, cols, spread):
    e_iota = iota((LANE, LANE), 0)
    n_iota = iota((LANE, LANE), 1)
    picks = [pick[k : k + 1, :] for k in range(2)]
    hits = [(e_iota == p).astype(F32) for p in picks]
    both = (hits[0] + hits[1]).astype(BF16)
    before = jnp.dot(both, onehot(e_iota < n_iota), preferred_element_type=F32)
    places = []
    for k in range(2):
        rank = jnp.sum(before * hits[k], axis=0, keepdims=True)
        places.append(RANKS * picks[k] + rank.astype(jnp.int32))
    first = prob[...] * jax.nn.sigmoid(logits[0:1, :] - logits[1:2, :])
    second = prob[...] * jax.nn.sigmoid(logits[1:2, :] - logits[0:1, :])
    rows = [places[0].astype(F32), places[1].astype(F32), first, second]
    table = jnp.zeros((LANE, LANE), F32)
    for i, row in enumerate(rows):
        table = jnp.where(e_iota == i, row, table)
    cols[...] = table.T
    part = e_iota // RANKS % PARTS
    for b in range(spread.shape[0] // LANE):
        row = e_iota + b * LANE
        code = row // (RANKS * PARTS) * RANKS + row % RANKS
        hit = jnp.logical_or(code == places[0], code == places[1])
        for q in range(PARTS):
            spread[b * LANE : (b + 1) * LANE, q * LANE : (q + 1) * LANE] = onehot(
                jnp.logical_and(hit, part == q)
            )


def select(cols, picked):
    tokens, rows = cols.shape[0], picked.shape[1]
    slot = iota((tokens, rows), 1)
    code = (slot // (RANKS * PARTS) * RANKS + slot % RANKS).astype(F32)
    share = jnp.where(cols[:, 0:1] == code, cols[:, 2:3], 0.0)
    share = jnp.where(cols[:, 1:2] == code, cols[:, 3:4], share)
    part = slot // RANKS % PARTS
    for q in range(PARTS):
        picked[q * tokens : (q + 1) * tokens, :] = jnp.where(part == q, share, 0.0).astype(BF16)


def load_body(
    value_in, gate_in, kernel_in, bias_in, gain_in, shift_in, pick_in, logits_in, prob_in,
    tail, kernel, vecs, pick, logits, prob,
    value, gate, sems,
):
    cut = value_in.shape[0] - HALO
    copies = fetch(
        (
            value_in.at[pl.ds(cut, HALO), :], gate_in.at[pl.ds(cut, HALO), :],
            kernel_in, bias_in, gain_in, shift_in, pick_in, logits_in, prob_in,
        ),
        (value, gate, kernel, vecs.at[0:1], vecs.at[1:2], vecs.at[2:3], pick, logits, prob),
        sems,
    )
    for copy in copies[:2]:
        copy.wait()
    glued = value[...].astype(F32) * jax.nn.sigmoid(gate[...].astype(F32))
    tail[...] = glued.astype(BF16)
    for copy in copies[2:]:
        copy.wait()


def taps_and_norm(ext, taps, vecs, b, start, rows, n_taps):
    lanes = pl.ds(pl.multiple_of(b * LANE, LANE), LANE)
    acc = jnp.broadcast_to(vecs[0:1, lanes], (rows, LANE))
    for j in range(n_taps):
        at = start + HALO - (n_taps - 1) + j
        acc = acc + taps[b, j : j + 1, :] * ext[b, at : at + rows, :]
    centre = jnp.mean(acc, axis=-1, keepdims=True)
    away = acc - centre
    variance = jnp.mean(away * away, axis=-1, keepdims=True)
    v = away * lax.rsqrt(variance + EPS) * vecs[1:2, lanes] + vecs[2:3, lanes]
    return (v / (1.0 + jnp.exp(-v))).astype(BF16)


def conv_body(
    value, gate, kernel, vecs, pick, logits, prob,
    mixed, ext, taps, spread, picked,
    cols,
):
    n_taps, width = kernel.shape
    blocks, length, _ = ext.shape
    for b in range(blocks):
        lanes = slice(b * LANE, (b + 1) * LANE)
        taps[b, 0:n_taps, :] = kernel[:, lanes].astype(F32)
        glued = value[:, lanes].astype(F32) * jax.nn.sigmoid(gate[:, lanes].astype(F32))
        ext[b, :, :] = glued.astype(BF16).astype(F32)
    mixed[0:HALO, :] = jnp.zeros((HALO, width), BF16)
    route(pick, logits, prob, cols, spread)
    select(cols, picked)

    def block(b, carry):
        lanes = pl.ds(pl.multiple_of(b * LANE, LANE), LANE)
        for r in range(HALO, length, HALO):
            mixed[r : r + HALO, lanes] = taps_and_norm(ext, taps, vecs, b, r - HALO, HALO, n_taps)
        return carry

    lax.fori_loop(0, blocks, block, 0)


def head(me, cores, halo, front, taps, vecs, ext, out, n_taps):
    for b in range(ext.shape[0]):
        lanes = slice(b * LANE, (b + 1) * LANE)
        ext[b, 0:HALO, :] = jnp.where(me[0] >= cores, halo[:, lanes].astype(F32), 0.0)
        ext[b, HALO : 2 * HALO, :] = front[b, 0:HALO, :]
    for b in range(ext.shape[0]):
        lanes = slice(b * LANE, (b + 1) * LANE)
        out[0:HALO, lanes] = taps_and_norm(ext, taps, vecs, b, 0, HALO, n_taps)


def give_body(cores, n_taps, me, mixed, halo, front, taps, vecs, theirs, ext):
    half = theirs.shape[0]
    core = lax.rem(me[0], cores)

    @pl.when(core == 0)
    def _():
        theirs[...] = mixed[half : 2 * half, :]

    @pl.when(core != 0)
    def _():
        theirs[...] = mixed[0:half, :]
        head(me, cores, halo, front, taps, vecs, ext, theirs, n_taps)


def own_body(cores, n_taps, me, mixed, halo, front, taps, vecs, weight, residual, partial, ext, mine):
    half, width = mine.shape
    step = partial.shape[1] // 4
    core = lax.rem(me[0], cores)

    @pl.when(core == 0)
    def _():
        mine[...] = mixed[0:half, :]
        head(me, cores, halo, front, taps, vecs, ext, mine, n_taps)

    @pl.when(core != 0)
    def _():
        mine[...] = mixed[half : 2 * half, :]

    here = pl.ds(pl.multiple_of(core * width, width), width)
    for q in range(4):
        lanes = slice(q * step, (q + 1) * step)
        acc = jnp.dot(mine[...], weight[here, lanes], preferred_element_type=F32)
        partial[:, lanes] = acc + residual[:, lanes].astype(F32)


def project_body(cores, me, other, weight, partial, gain, spread, hidden, out, stacked):
    tokens, half = other.shape
    width = partial.shape[1]
    step = width // 4
    there = pl.ds(pl.multiple_of((1 - lax.rem(me[0], cores)) * half, half), half)
    total = jnp.zeros((tokens, 1), F32)
    for q in range(4):
        lanes = slice(q * step, (q + 1) * step)
        acc = jnp.dot(other[...], weight[there, lanes], preferred_element_type=F32)
        rounded = (acc + partial[:, lanes]).astype(BF16)
        hidden[:, lanes] = rounded
        wide = rounded.astype(F32)
        total = total + jnp.sum(wide * wide, axis=-1, keepdims=True)
    scale = lax.rsqrt(total / width + EPS)
    step = width // PARTS
    for q in range(PARTS):
        lanes = slice(q * step, (q + 1) * step)
        stacked[q * tokens : (q + 1) * tokens, :] = (
            hidden[:, lanes].astype(F32) * scale * gain[:, lanes]
        ).astype(BF16)
    chunk = 2 * LANE
    for b in range(out.shape[0] // chunk):
        rows = slice(b * chunk, (b + 1) * chunk)
        out[rows, :] = jnp.dot(spread[rows, :], stacked[...], preferred_element_type=F32).astype(BF16)


def trade(a, b):
    low = iota(a.shape, 1) < RANKS
    return jnp.where(low, a, pltpu.roll(b, RANKS, 1)), jnp.where(low, pltpu.roll(a, RANKS, 1), b)


def expert_body(message, gate, up, down, out, flat):
    rows, step = message.shape
    tile = RANKS * PARTS
    pairs = rows // (2 * tile)
    pieces = 4
    size = step // pieces
    for p in range(pieces):
        here = slice(p * size, (p + 1) * size)
        wide = message[:, here].astype(F32).reshape(pairs, 2, tile, size)
        for q, half in enumerate(trade(wide[:, 0], wide[:, 1])):
            flat[:, q * step + p * size : q * step + (p + 1) * size] = half.reshape(rows // 2, size).astype(BF16)
    x = flat[...]
    g = jnp.dot(x, gate[...], preferred_element_type=F32)
    u = jnp.dot(x, up[...], preferred_element_type=F32)
    active = (g / (1.0 + jnp.exp(-g)) * u).astype(BF16)
    for p in range(pieces):
        halves = [
            jnp.dot(
                active, down[:, q * step + p * size : q * step + (p + 1) * size], preferred_element_type=F32
            ).reshape(pairs, tile, size)
            for q in range(PARTS)
        ]
        both = jnp.stack(trade(*halves), axis=1)
        out[:, p * size : (p + 1) * size] = both.reshape(rows, size).astype(BF16)


def combine_body(message, picked, base, out_hbm, out, sems):
    tokens = out.shape[0]
    step = message.shape[1]
    pieces = 4
    size = step // pieces
    copies = []
    for p in range(pieces):
        got = jnp.dot(picked[...], message[:, p * size : (p + 1) * size], preferred_element_type=F32)
        for q in range(PARTS):
            lanes = slice(q * step + p * size, q * step + (p + 1) * size)
            out[:, lanes] = (base[:, lanes].astype(F32) + got[q * tokens : (q + 1) * tokens]).astype(BF16)
            copy = pltpu.make_async_copy(
                out.at[:, lanes], out_hbm.at[:, lanes], sems.at[p * PARTS + q]
            )
            copy.start()
            copies.append(copy)
    for copy in copies:
        copy.wait()


def local(
    glu_value,
    glu_gate,
    conv_kernel,
    conv_bias,
    group_gain,
    group_shift,
    out_weight,
    residual,
    ffn_gain,
    expert_pick,
    pair_logits,
    group_prob,
    gate_weight,
    up_weight,
    down_weight,
):
    shape = jax.ShapeDtypeStruct
    length, width = glu_value.shape
    tokens, model = residual.shape
    experts = lax.axis_size("sp") * lax.axis_size("tp")
    peers = lax.axis_size("sp")
    me = lax.axis_index(("sp", "tp")).astype(jnp.int32).reshape(1)

    n_taps = conv_kernel.shape[0]
    blocks = width // LANE
    cores = lax.axis_size("tp")
    step = model // PARTS
    rows = experts * RANKS * PARTS
    message = shape((rows, step), BF16)
    tail, kernel, vecs, pick, logits, prob = call(
        load_body,
        (
            shape((HALO, width), BF16),
            shape((n_taps, width), BF16),
            shape((8, width), F32),
            shape((2, tokens), jnp.int32),
            shape((2, tokens), F32),
            shape((1, tokens), F32),
        ),
        scratch=(
            pltpu.VMEM((HALO, width), BF16),
            pltpu.VMEM((HALO, width), BF16),
            pltpu.SemaphoreType.DMA((9,)),
        ),
        hbm=range(9),
        n_in=9,
        limit=4,
        flops=5_000_000_000,
    )(
        glu_value,
        glu_gate,
        conv_kernel,
        conv_bias.reshape(1, width),
        group_gain.reshape(1, width),
        group_shift.reshape(1, width),
        expert_pick.T,
        pair_logits.T,
        group_prob.reshape(1, tokens),
    )
    halo = lax.ppermute(tail, "sp", [(i, (i + 1) % peers) for i in range(peers)])
    half = length // 2
    ext_shape = (blocks, 2 * HALO, LANE)
    mixed, ext, taps, spread, picked = call(
        conv_body,
        (
            shape((length, width), BF16),
            shape((blocks, length, LANE), F32),
            shape((blocks, 32, LANE), F32),
            shape((rows, PARTS * tokens), BF16),
            shape((PARTS * tokens, rows), BF16),
        ),
        scratch=(pltpu.VMEM((tokens, LANE), F32),),
        n_in=7,
        limit=4,
        flops=6_000_000_000,
    )(glu_value, glu_gate, kernel, vecs, pick, logits, prob)
    (theirs,) = call(
        functools.partial(give_body, cores, n_taps),
        (shape((half, width), BF16),),
        scratch=(pltpu.VMEM(ext_shape, F32),),
        smem=(0,),
        n_in=6,
        limit=4,
        flops=500_000_000,
    )(me, mixed, halo, ext, taps, vecs)
    other = lax.ppermute(theirs, "tp", [(0, 1), (1, 0)])
    (partial,) = call(
        functools.partial(own_body, cores, n_taps),
        (shape((tokens, model), F32),),
        scratch=(pltpu.VMEM(ext_shape, F32), pltpu.VMEM((half, width), BF16)),
        smem=(0,),
        n_in=8,
        limit=4,
        flops=500_000_000,
    )(me, mixed, halo, ext, taps, vecs, out_weight, residual)
    hidden, send = call(
        functools.partial(project_body, cores),
        (shape((tokens, model), BF16), message),
        scratch=(pltpu.VMEM((PARTS * tokens, step), BF16),),
        smem=(0,),
        n_in=6,
        limit=16,
        flops=1_000_000_000,
    )(me, other, out_weight, partial, ffn_gain.reshape(1, model), spread)
    flat = pltpu.VMEM((RANKS * experts, model), BF16)

    def exchange(x):
        x = x.reshape(experts, RANKS * PARTS, step)
        return lax.all_to_all(x, ("sp", "tp"), 0, 0, tiled=True).reshape(rows, step)

    got = exchange(send)
    (done,) = call(
        expert_body, (message,), scratch=(flat,), n_in=4, limit=24, flops=4_000_000_000
    )(got, gate_weight[0], up_weight[0], down_weight[0])
    back = exchange(done)
    (result,) = call(
        combine_body,
        (shape((tokens, model), BF16),),
        scratch=(pltpu.VMEM((tokens, model), BF16), pltpu.SemaphoreType.DMA((8,))),
        n_in=3,
        out_hbm=(0,),
        limit=12,
        flops=1_000_000_000,
    )(back, picked, hidden)
    return result


def solution(mesh):
    in_specs = (
        P("sp", "tp"),
        P("sp", "tp"),
        P(None, "tp"),
        P("tp"),
        P("tp"),
        P("tp"),
        P(),
        P(("sp", "tp"), None),
        P(),
        P(("sp", "tp"), None),
        P(("sp", "tp"), None),
        P(("sp", "tp")),
        P(("sp", "tp"), None, None),
        P(("sp", "tp"), None, None),
        P(("sp", "tp"), None, None),
    )
    out_specs = P(("sp", "tp"), None)

    return jax.shard_map(local, mesh=mesh, in_specs=in_specs, out_specs=out_specs, check_vma=False)
```

```python
import functools
import jax
import jax.numpy as jnp
from jax import lax
from jax.experimental import pallas as pl
from jax.experimental.pallas import tpu as pltpu
from jax.sharding import PartitionSpec as P


EPS = 1e-06
F32 = jnp.float32
BF16 = jnp.bfloat16
HALO = 32
PARTS = 2
RANKS = 4
LANE = 128
MIB = 1024 * 1024


def iota(shape, axis):
    return lax.broadcasted_iota(jnp.int32, shape, axis)


def onehot(cond):
    return jnp.where(cond, 1.0, 0.0).astype(BF16)


def call(body, out_shape, scratch=(), limit=16, smem=(), hbm=(), n_in=0, out_hbm=(), flops=0):
    kind = {**dict.fromkeys(smem, pltpu.SMEM), **dict.fromkeys(hbm, pltpu.HBM)}
    n_out = len(out_shape)
    run = pl.pallas_call(
        body,
        out_shape=out_shape,
        in_specs=[pl.BlockSpec(memory_space=kind.get(i, pltpu.VMEM)) for i in range(n_in)],
        out_specs=[
            pl.BlockSpec(memory_space=pltpu.HBM if i in out_hbm else pltpu.VMEM) for i in range(n_out)
        ],
        scratch_shapes=list(scratch),
        compiler_params=pltpu.CompilerParams(vmem_limit_bytes=limit * MIB),
        cost_estimate=pl.CostEstimate(flops=flops, bytes_accessed=0, transcendentals=0),
    )
    return lambda *args: run(
        *(pltpu.with_memory_space_constraint(a, pltpu.HBM) if i in hbm else a for i, a in enumerate(args))
    )


def fetch(sources, targets, sems):
    copies = [
        pltpu.make_async_copy(source, target, sems.at[i])
        for i, (source, target) in enumerate(zip(sources, targets, strict=True))
    ]
    for copy in copies:
        copy.start()
    return copies


def route(pick, logits, prob, cols, spread):
    e_iota = iota((LANE, LANE), 0)
    n_iota = iota((LANE, LANE), 1)
    picks = [pick[k : k + 1, :] for k in range(2)]
    hits = [(e_iota == p).astype(F32) for p in picks]
    both = (hits[0] + hits[1]).astype(BF16)
    before = jnp.dot(both, onehot(e_iota < n_iota), preferred_element_type=F32)
    places = []
    for k in range(2):
        rank = jnp.sum(before * hits[k], axis=0, keepdims=True)
        places.append(RANKS * picks[k] + rank.astype(jnp.int32))
    first = prob[...] * jax.nn.sigmoid(logits[0:1, :] - logits[1:2, :])
    second = prob[...] * jax.nn.sigmoid(logits[1:2, :] - logits[0:1, :])
    rows = [places[0].astype(F32), places[1].astype(F32), first, second]
    table = jnp.zeros((LANE, LANE), F32)
    for i, row in enumerate(rows):
        table = jnp.where(e_iota == i, row, table)
    cols[...] = table.T
    part = e_iota // RANKS % PARTS
    for b in range(spread.shape[0] // LANE):
        row = e_iota + b * LANE
        code = row // (RANKS * PARTS) * RANKS + row % RANKS
        hit = jnp.logical_or(code == places[0], code == places[1])
        for q in range(PARTS):
            spread[b * LANE : (b + 1) * LANE, q * LANE : (q + 1) * LANE] = onehot(
                jnp.logical_and(hit, part == q)
            )


def select(cols, picked):
    tokens, rows = cols.shape[0], picked.shape[1]
    slot = iota((tokens, rows), 1)
    code = (slot // (RANKS * PARTS) * RANKS + slot % RANKS).astype(F32)
    share = jnp.where(cols[:, 0:1] == code, cols[:, 2:3], 0.0)
    share = jnp.where(cols[:, 1:2] == code, cols[:, 3:4], share)
    part = slot // RANKS % PARTS
    for q in range(PARTS):
        picked[q * tokens : (q + 1) * tokens, :] = jnp.where(part == q, share, 0.0).astype(BF16)


def tail_body(value_in, gate_in, tail, value, gate, sems):
    last = pl.ds(value_in.shape[0] - HALO, HALO)
    for copy in fetch((value_in.at[last, :], gate_in.at[last, :]), (value, gate), sems):
        copy.wait()
    glued = value[...].astype(F32) * jax.nn.sigmoid(gate[...].astype(F32))
    tail[...] = glued.astype(BF16)


def taps_and_norm(ext, taps, vecs, b, start, rows, n_taps):
    lanes = pl.ds(pl.multiple_of(b * LANE, LANE), LANE)
    acc = jnp.broadcast_to(vecs[0:1, lanes], (rows, LANE))
    for j in range(n_taps):
        at = start + HALO - (n_taps - 1) + j
        acc = acc + taps[b, j : j + 1, :] * ext[b, at : at + rows, :]
    centre = jnp.mean(acc, axis=-1, keepdims=True)
    away = acc - centre
    variance = jnp.mean(away * away, axis=-1, keepdims=True)
    v = away * lax.rsqrt(variance + EPS) * vecs[1:2, lanes] + vecs[2:3, lanes]
    return (v / (1.0 + jnp.exp(-v))).astype(BF16)


def conv_body(
    value, gate, kernel, bias, gain, shift, pick, logits, prob,
    mixed, ext, taps, vecs, spread, picked,
    cols,
):
    for i, row in enumerate((bias, gain, shift)):
        vecs[i : i + 1, :] = row[...]
    n_taps, width = kernel.shape
    blocks, length, _ = ext.shape
    for b in range(blocks):
        lanes = slice(b * LANE, (b + 1) * LANE)
        taps[b, 0:n_taps, :] = kernel[:, lanes].astype(F32)
        glued = value[:, lanes].astype(F32) * jax.nn.sigmoid(gate[:, lanes].astype(F32))
        ext[b, :, :] = glued.astype(BF16).astype(F32)
    mixed[0:HALO, :] = jnp.zeros((HALO, width), BF16)
    route(pick, logits, prob, cols, spread)
    select(cols, picked)

    def block(b, carry):
        lanes = pl.ds(pl.multiple_of(b * LANE, LANE), LANE)
        for r in range(HALO, length, HALO):
            mixed[r : r + HALO, lanes] = taps_and_norm(ext, taps, vecs, b, r - HALO, HALO, n_taps)
        return carry

    lax.fori_loop(0, blocks, block, 0)


def head(me, cores, halo, front, taps, vecs, ext, out, n_taps):
    for b in range(ext.shape[0]):
        lanes = slice(b * LANE, (b + 1) * LANE)
        ext[b, 0:HALO, :] = jnp.where(me[0] >= cores, halo[:, lanes].astype(F32), 0.0)
        ext[b, HALO : 2 * HALO, :] = front[b, 0:HALO, :]
    for b in range(ext.shape[0]):
        lanes = slice(b * LANE, (b + 1) * LANE)
        out[0:HALO, lanes] = taps_and_norm(ext, taps, vecs, b, 0, HALO, n_taps)


def give_body(cores, n_taps, me, mixed, halo, front, taps, vecs, theirs, ext):
    half = theirs.shape[0]
    core = lax.rem(me[0], cores)

    @pl.when(core == 0)
    def _():
        theirs[...] = mixed[half : 2 * half, :]

    @pl.when(core != 0)
    def _():
        theirs[...] = mixed[0:half, :]
        head(me, cores, halo, front, taps, vecs, ext, theirs, n_taps)


def own_body(cores, n_taps, me, mixed, halo, front, taps, vecs, weight, residual, partial, ext, mine):
    half, width = mine.shape
    step = partial.shape[1] // 4
    core = lax.rem(me[0], cores)

    @pl.when(core == 0)
    def _():
        mine[...] = mixed[0:half, :]
        head(me, cores, halo, front, taps, vecs, ext, mine, n_taps)

    @pl.when(core != 0)
    def _():
        mine[...] = mixed[half : 2 * half, :]

    here = pl.ds(pl.multiple_of(core * width, width), width)
    for q in range(4):
        lanes = slice(q * step, (q + 1) * step)
        acc = jnp.dot(mine[...], weight[here, lanes], preferred_element_type=F32)
        partial[:, lanes] = acc + residual[:, lanes].astype(F32)


def project_body(cores, me, other, weight, partial, gain, spread, hidden, out, stacked):
    tokens, half = other.shape
    width = partial.shape[1]
    step = width // 4
    there = pl.ds(pl.multiple_of((1 - lax.rem(me[0], cores)) * half, half), half)
    total = jnp.zeros((tokens, 1), F32)
    for q in range(4):
        lanes = slice(q * step, (q + 1) * step)
        acc = jnp.dot(other[...], weight[there, lanes], preferred_element_type=F32)
        rounded = (acc + partial[:, lanes]).astype(BF16)
        hidden[:, lanes] = rounded
        wide = rounded.astype(F32)
        total = total + jnp.sum(wide * wide, axis=-1, keepdims=True)
    scale = lax.rsqrt(total / width + EPS)
    step = width // PARTS
    for q in range(PARTS):
        lanes = slice(q * step, (q + 1) * step)
        stacked[q * tokens : (q + 1) * tokens, :] = (
            hidden[:, lanes].astype(F32) * scale * gain[:, lanes]
        ).astype(BF16)
    chunk = 2 * LANE
    for b in range(out.shape[0] // chunk):
        rows = slice(b * chunk, (b + 1) * chunk)
        out[rows, :] = jnp.dot(spread[rows, :], stacked[...], preferred_element_type=F32).astype(BF16)


def trade(a, b):
    low = iota(a.shape, 1) < RANKS
    return jnp.where(low, a, pltpu.roll(b, RANKS, 1)), jnp.where(low, pltpu.roll(a, RANKS, 1), b)


def expert_body(message, gate, up, down, out, flat):
    rows, step = message.shape
    tile = RANKS * PARTS
    pairs = rows // (2 * tile)
    pieces = 4
    size = step // pieces
    for p in range(pieces):
        here = slice(p * size, (p + 1) * size)
        wide = message[:, here].astype(F32).reshape(pairs, 2, tile, size)
        for q, half in enumerate(trade(wide[:, 0], wide[:, 1])):
            flat[:, q * step + p * size : q * step + (p + 1) * size] = half.reshape(rows // 2, size).astype(BF16)
    x = flat[...]
    g = jnp.dot(x, gate[...], preferred_element_type=F32)
    u = jnp.dot(x, up[...], preferred_element_type=F32)
    active = (g / (1.0 + jnp.exp(-g)) * u).astype(BF16)
    for p in range(pieces):
        halves = [
            jnp.dot(
                active, down[:, q * step + p * size : q * step + (p + 1) * size], preferred_element_type=F32
            ).reshape(pairs, tile, size)
            for q in range(PARTS)
        ]
        both = jnp.stack(trade(*halves), axis=1)
        out[:, p * size : (p + 1) * size] = both.reshape(rows, size).astype(BF16)


def combine_body(message, picked, base, out_hbm, out, sems):
    tokens = out.shape[0]
    step = message.shape[1]
    pieces = 4
    size = step // pieces
    copies = []
    for p in range(pieces):
        got = jnp.dot(picked[...], message[:, p * size : (p + 1) * size], preferred_element_type=F32)
        for q in range(PARTS):
            lanes = slice(q * step + p * size, q * step + (p + 1) * size)
            out[:, lanes] = (base[:, lanes].astype(F32) + got[q * tokens : (q + 1) * tokens]).astype(BF16)
            copy = pltpu.make_async_copy(
                out.at[:, lanes], out_hbm.at[:, lanes], sems.at[p * PARTS + q]
            )
            copy.start()
            copies.append(copy)
    for copy in copies:
        copy.wait()


def local(
    glu_value,
    glu_gate,
    conv_kernel,
    conv_bias,
    group_gain,
    group_shift,
    out_weight,
    residual,
    ffn_gain,
    expert_pick,
    pair_logits,
    group_prob,
    gate_weight,
    up_weight,
    down_weight,
):
    shape = jax.ShapeDtypeStruct
    length, width = glu_value.shape
    tokens, model = residual.shape
    experts = lax.axis_size("sp") * lax.axis_size("tp")
    peers = lax.axis_size("sp")
    me = lax.axis_index(("sp", "tp")).astype(jnp.int32).reshape(1)

    n_taps = conv_kernel.shape[0]
    blocks = width // LANE
    cores = lax.axis_size("tp")
    step = model // PARTS
    rows = experts * RANKS * PARTS
    message = shape((rows, step), BF16)
    (tail,) = call(
        tail_body,
        (shape((HALO, width), BF16),),
        scratch=(
            pltpu.VMEM((HALO, width), BF16),
            pltpu.VMEM((HALO, width), BF16),
            pltpu.SemaphoreType.DMA((2,)),
        ),
        hbm=range(2),
        n_in=2,
        limit=4,
        flops=5_000_000_000,
    )(glu_value, glu_gate)
    halo = lax.ppermute(tail, "sp", [(i, (i + 1) % peers) for i in range(peers)])
    half = length // 2
    ext_shape = (blocks, 2 * HALO, LANE)
    mixed, ext, taps, vecs, spread, picked = call(
        conv_body,
        (
            shape((length, width), BF16),
            shape((blocks, length, LANE), F32),
            shape((blocks, 32, LANE), F32),
            shape((8, width), F32),
            shape((rows, PARTS * tokens), BF16),
            shape((PARTS * tokens, rows), BF16),
        ),
        scratch=(pltpu.VMEM((tokens, LANE), F32),),
        n_in=9,
        limit=4,
        flops=6_000_000_000,
    )(
        glu_value,
        glu_gate,
        conv_kernel,
        conv_bias.reshape(1, width),
        group_gain.reshape(1, width),
        group_shift.reshape(1, width),
        expert_pick.T,
        pair_logits.T,
        group_prob.reshape(1, tokens),
    )
    (theirs,) = call(
        functools.partial(give_body, cores, n_taps),
        (shape((half, width), BF16),),
        scratch=(pltpu.VMEM(ext_shape, F32),),
        smem=(0,),
        n_in=6,
        limit=4,
        flops=500_000_000,
    )(me, mixed, halo, ext, taps, vecs)
    other = lax.ppermute(theirs, "tp", [(0, 1), (1, 0)])
    (partial,) = call(
        functools.partial(own_body, cores, n_taps),
        (shape((tokens, model), F32),),
        scratch=(pltpu.VMEM(ext_shape, F32), pltpu.VMEM((half, width), BF16)),
        smem=(0,),
        n_in=8,
        limit=4,
        flops=500_000_000,
    )(me, mixed, halo, ext, taps, vecs, out_weight, residual)
    hidden, send = call(
        functools.partial(project_body, cores),
        (shape((tokens, model), BF16), message),
        scratch=(pltpu.VMEM((PARTS * tokens, step), BF16),),
        smem=(0,),
        n_in=6,
        limit=16,
        flops=1_000_000_000,
    )(me, other, out_weight, partial, ffn_gain.reshape(1, model), spread)
    flat = pltpu.VMEM((RANKS * experts, model), BF16)

    def exchange(x):
        x = x.reshape(experts, RANKS * PARTS, step)
        return lax.all_to_all(x, ("sp", "tp"), 0, 0, tiled=True).reshape(rows, step)

    got = exchange(send)
    (done,) = call(
        expert_body, (message,), scratch=(flat,), n_in=4, limit=24, flops=4_000_000_000
    )(got, gate_weight[0], up_weight[0], down_weight[0])
    back = exchange(done)
    (result,) = call(
        combine_body,
        (shape((tokens, model), BF16),),
        scratch=(pltpu.VMEM((tokens, model), BF16), pltpu.SemaphoreType.DMA((8,))),
        n_in=3,
        out_hbm=(0,),
        limit=12,
        flops=1_000_000_000,
    )(back, picked, hidden)
    return result


def solution(mesh):
    in_specs = (
        P("sp", "tp"),
        P("sp", "tp"),
        P(None, "tp"),
        P("tp"),
        P("tp"),
        P("tp"),
        P(),
        P(("sp", "tp"), None),
        P(),
        P(("sp", "tp"), None),
        P(("sp", "tp"), None),
        P(("sp", "tp")),
        P(("sp", "tp"), None, None),
        P(("sp", "tp"), None, None),
        P(("sp", "tp"), None, None),
    )
    out_specs = P(("sp", "tp"), None)

    return jax.shard_map(local, mesh=mesh, in_specs=in_specs, out_specs=out_specs, check_vma=False)
```

```python
import functools
import jax
import jax.numpy as jnp
from jax import lax
from jax.experimental import pallas as pl
from jax.experimental.pallas import tpu as pltpu
from jax.sharding import PartitionSpec as P


EPS = 1e-06
F32 = jnp.float32
BF16 = jnp.bfloat16
HALO = 32
PARTS = 2
RANKS = 4
LANE = 128
MIB = 1024 * 1024


def iota(shape, axis):
    return lax.broadcasted_iota(jnp.int32, shape, axis)


def onehot(cond):
    return jnp.where(cond, 1.0, 0.0).astype(BF16)


def call(body, out_shape, scratch=(), limit=16, smem=(), hbm=(), n_in=0, out_hbm=(), flops=0):
    kind = {**dict.fromkeys(smem, pltpu.SMEM), **dict.fromkeys(hbm, pltpu.HBM)}
    n_out = len(out_shape)
    run = pl.pallas_call(
        body,
        out_shape=out_shape,
        in_specs=[pl.BlockSpec(memory_space=kind.get(i, pltpu.VMEM)) for i in range(n_in)],
        out_specs=[
            pl.BlockSpec(memory_space=pltpu.HBM if i in out_hbm else pltpu.VMEM) for i in range(n_out)
        ],
        scratch_shapes=list(scratch),
        compiler_params=pltpu.CompilerParams(vmem_limit_bytes=limit * MIB),
        cost_estimate=pl.CostEstimate(flops=flops, bytes_accessed=0, transcendentals=0),
    )
    return lambda *args: run(
        *(pltpu.with_memory_space_constraint(a, pltpu.HBM) if i in hbm else a for i, a in enumerate(args))
    )


def fetch(sources, targets, sems):
    copies = [
        pltpu.make_async_copy(source, target, sems.at[i])
        for i, (source, target) in enumerate(zip(sources, targets, strict=True))
    ]
    for copy in copies:
        copy.start()
    return copies


def route(pick, logits, prob, cols, spread):
    e_iota = iota((LANE, LANE), 0)
    n_iota = iota((LANE, LANE), 1)
    picks = [pick[k : k + 1, :] for k in range(2)]
    hits = [(e_iota == p).astype(F32) for p in picks]
    both = (hits[0] + hits[1]).astype(BF16)
    before = jnp.dot(both, onehot(e_iota < n_iota), preferred_element_type=F32)
    places = []
    for k in range(2):
        rank = jnp.sum(before * hits[k], axis=0, keepdims=True)
        places.append(RANKS * picks[k] + rank.astype(jnp.int32))
    first = prob[...] * jax.nn.sigmoid(logits[0:1, :] - logits[1:2, :])
    second = prob[...] * jax.nn.sigmoid(logits[1:2, :] - logits[0:1, :])
    rows = [places[0].astype(F32), places[1].astype(F32), first, second]
    table = jnp.zeros((LANE, LANE), F32)
    for i, row in enumerate(rows):
        table = jnp.where(e_iota == i, row, table)
    cols[...] = table.T
    part = e_iota // RANKS % PARTS
    for b in range(spread.shape[0] // LANE):
        row = e_iota + b * LANE
        code = row // (RANKS * PARTS) * RANKS + row % RANKS
        hit = jnp.logical_or(code == places[0], code == places[1])
        for q in range(PARTS):
            spread[b * LANE : (b + 1) * LANE, q * LANE : (q + 1) * LANE] = onehot(
                jnp.logical_and(hit, part == q)
            )


def select(cols, picked):
    tokens, rows = cols.shape[0], picked.shape[1]
    slot = iota((tokens, rows), 1)
    code = (slot // (RANKS * PARTS) * RANKS + slot % RANKS).astype(F32)
    share = jnp.where(cols[:, 0:1] == code, cols[:, 2:3], 0.0)
    share = jnp.where(cols[:, 1:2] == code, cols[:, 3:4], share)
    part = slot // RANKS % PARTS
    for q in range(PARTS):
        picked[q * tokens : (q + 1) * tokens, :] = jnp.where(part == q, share, 0.0).astype(BF16)


def tail_body(value_in, gate_in, tail, value, gate, sems):
    last = pl.ds(value_in.shape[0] - HALO, HALO)
    for copy in fetch((value_in.at[last, :], gate_in.at[last, :]), (value, gate), sems):
        copy.wait()
    glued = value[...].astype(F32) * jax.nn.sigmoid(gate[...].astype(F32))
    tail[...] = glued.astype(BF16)


def taps_and_norm(ext, taps, vecs, b, start, rows, n_taps):
    lanes = pl.ds(pl.multiple_of(b * LANE, LANE), LANE)
    acc = jnp.broadcast_to(vecs[0:1, lanes], (rows, LANE))
    for j in range(n_taps):
        at = start + HALO - (n_taps - 1) + j
        acc = acc + taps[b, j : j + 1, :] * ext[b, at : at + rows, :]
    centre = jnp.mean(acc, axis=-1, keepdims=True)
    away = acc - centre
    variance = jnp.mean(away * away, axis=-1, keepdims=True)
    v = away * lax.rsqrt(variance + EPS) * vecs[1:2, lanes] + vecs[2:3, lanes]
    return (v / (1.0 + jnp.exp(-v))).astype(BF16)


def conv_body(
    value, gate, kernel, bias, gain, shift, pick, logits, prob,
    mixed, ext, taps, vecs, spread, picked,
    cols,
):
    for i, row in enumerate((bias, gain, shift)):
        vecs[i : i + 1, :] = row[...]
    n_taps, width = kernel.shape
    blocks, length, _ = ext.shape
    for b in range(blocks):
        lanes = slice(b * LANE, (b + 1) * LANE)
        taps[b, 0:n_taps, :] = kernel[:, lanes].astype(F32)
        glued = value[:, lanes].astype(F32) * jax.nn.sigmoid(gate[:, lanes].astype(F32))
        ext[b, :, :] = glued.astype(BF16).astype(F32)
    mixed[0:HALO, :] = jnp.zeros((HALO, width), BF16)
    route(pick, logits, prob, cols, spread)
    select(cols, picked)

    def block(b, carry):
        lanes = pl.ds(pl.multiple_of(b * LANE, LANE), LANE)
        for r in range(HALO, length, HALO):
            mixed[r : r + HALO, lanes] = taps_and_norm(ext, taps, vecs, b, r - HALO, HALO, n_taps)
        return carry

    lax.fori_loop(0, blocks, block, 0)


def head(halo, front, taps, vecs, ext, out, n_taps):
    for b in range(ext.shape[0]):
        lanes = slice(b * LANE, (b + 1) * LANE)
        ext[b, 0:HALO, :] = jnp.where(lax.axis_index("sp") > 0, halo[:, lanes].astype(F32), 0.0)
        ext[b, HALO : 2 * HALO, :] = front[b, 0:HALO, :]
    for b in range(ext.shape[0]):
        lanes = slice(b * LANE, (b + 1) * LANE)
        out[0:HALO, lanes] = taps_and_norm(ext, taps, vecs, b, 0, HALO, n_taps)


def give_body(n_taps, mixed, halo, front, taps, vecs, theirs, ext):
    half = theirs.shape[0]
    core = lax.axis_index("tp")

    @pl.when(core == 0)
    def _():
        theirs[...] = mixed[half : 2 * half, :]

    @pl.when(core != 0)
    def _():
        theirs[...] = mixed[0:half, :]
        head(halo, front, taps, vecs, ext, theirs, n_taps)


def own_body(n_taps, mixed, halo, front, taps, vecs, weight, residual, partial, ext, mine):
    half, width = mine.shape
    step = partial.shape[1] // 4
    core = lax.axis_index("tp")

    @pl.when(core == 0)
    def _():
        mine[...] = mixed[0:half, :]
        head(halo, front, taps, vecs, ext, mine, n_taps)

    @pl.when(core != 0)
    def _():
        mine[...] = mixed[half : 2 * half, :]

    here = pl.ds(pl.multiple_of(core * width, width), width)
    for q in range(4):
        lanes = slice(q * step, (q + 1) * step)
        acc = jnp.dot(mine[...], weight[here, lanes], preferred_element_type=F32)
        partial[:, lanes] = acc + residual[:, lanes].astype(F32)


def project_body(other, weight, partial, gain, spread, hidden, out, stacked):
    tokens, half = other.shape
    width = partial.shape[1]
    step = width // 4
    there = pl.ds(pl.multiple_of((1 - lax.axis_index("tp")) * half, half), half)
    total = jnp.zeros((tokens, 1), F32)
    for q in range(4):
        lanes = slice(q * step, (q + 1) * step)
        acc = jnp.dot(other[...], weight[there, lanes], preferred_element_type=F32)
        rounded = (acc + partial[:, lanes]).astype(BF16)
        hidden[:, lanes] = rounded
        wide = rounded.astype(F32)
        total = total + jnp.sum(wide * wide, axis=-1, keepdims=True)
    scale = lax.rsqrt(total / width + EPS)
    step = width // PARTS
    for q in range(PARTS):
        lanes = slice(q * step, (q + 1) * step)
        stacked[q * tokens : (q + 1) * tokens, :] = (
            hidden[:, lanes].astype(F32) * scale * gain[:, lanes]
        ).astype(BF16)
    chunk = 2 * LANE
    for b in range(out.shape[0] // chunk):
        rows = slice(b * chunk, (b + 1) * chunk)
        out[rows, :] = jnp.dot(spread[rows, :], stacked[...], preferred_element_type=F32).astype(BF16)


def trade(a, b):
    low = iota(a.shape, 1) < RANKS
    return jnp.where(low, a, pltpu.roll(b, RANKS, 1)), jnp.where(low, pltpu.roll(a, RANKS, 1), b)


def expert_body(message, gate, up, down, out, flat):
    rows, step = message.shape
    tile = RANKS * PARTS
    pairs = rows // (2 * tile)
    pieces = 4
    size = step // pieces
    for p in range(pieces):
        here = slice(p * size, (p + 1) * size)
        wide = message[:, here].astype(F32).reshape(pairs, 2, tile, size)
        for q, half in enumerate(trade(wide[:, 0], wide[:, 1])):
            flat[:, q * step + p * size : q * step + (p + 1) * size] = half.reshape(rows // 2, size).astype(BF16)
    x = flat[...]
    g = jnp.dot(x, gate[...], preferred_element_type=F32)
    u = jnp.dot(x, up[...], preferred_element_type=F32)
    active = (g / (1.0 + jnp.exp(-g)) * u).astype(BF16)
    for p in range(pieces):
        halves = [
            jnp.dot(
                active, down[:, q * step + p * size : q * step + (p + 1) * size], preferred_element_type=F32
            ).reshape(pairs, tile, size)
            for q in range(PARTS)
        ]
        both = jnp.stack(trade(*halves), axis=1)
        out[:, p * size : (p + 1) * size] = both.reshape(rows, size).astype(BF16)


def combine_body(message, picked, base, out_hbm, out, sems):
    tokens = out.shape[0]
    step = message.shape[1]
    pieces = 4
    size = step // pieces
    copies = []
    for p in range(pieces):
        got = jnp.dot(picked[...], message[:, p * size : (p + 1) * size], preferred_element_type=F32)
        for q in range(PARTS):
            lanes = slice(q * step + p * size, q * step + (p + 1) * size)
            out[:, lanes] = (base[:, lanes].astype(F32) + got[q * tokens : (q + 1) * tokens]).astype(BF16)
            copy = pltpu.make_async_copy(
                out.at[:, lanes], out_hbm.at[:, lanes], sems.at[p * PARTS + q]
            )
            copy.start()
            copies.append(copy)
    for copy in copies:
        copy.wait()


def local(
    glu_value,
    glu_gate,
    conv_kernel,
    conv_bias,
    group_gain,
    group_shift,
    out_weight,
    residual,
    ffn_gain,
    expert_pick,
    pair_logits,
    group_prob,
    gate_weight,
    up_weight,
    down_weight,
):
    shape = jax.ShapeDtypeStruct
    length, width = glu_value.shape
    tokens, model = residual.shape
    experts = lax.axis_size("sp") * lax.axis_size("tp")
    peers = lax.axis_size("sp")

    n_taps = conv_kernel.shape[0]
    blocks = width // LANE
    step = model // PARTS
    rows = experts * RANKS * PARTS
    message = shape((rows, step), BF16)
    (tail,) = call(
        tail_body,
        (shape((HALO, width), BF16),),
        scratch=(
            pltpu.VMEM((HALO, width), BF16),
            pltpu.VMEM((HALO, width), BF16),
            pltpu.SemaphoreType.DMA((2,)),
        ),
        hbm=range(2),
        n_in=2,
        limit=4,
        flops=5_000_000_000,
    )(glu_value, glu_gate)
    halo = lax.ppermute(tail, "sp", [(i, (i + 1) % peers) for i in range(peers)])
    half = length // 2
    ext_shape = (blocks, 2 * HALO, LANE)
    mixed, ext, taps, vecs, spread, picked = call(
        conv_body,
        (
            shape((length, width), BF16),
            shape((blocks, length, LANE), F32),
            shape((blocks, 32, LANE), F32),
            shape((8, width), F32),
            shape((rows, PARTS * tokens), BF16),
            shape((PARTS * tokens, rows), BF16),
        ),
        scratch=(pltpu.VMEM((tokens, LANE), F32),),
        n_in=9,
        limit=4,
        flops=6_000_000_000,
    )(
        glu_value,
        glu_gate,
        conv_kernel,
        conv_bias.reshape(1, width),
        group_gain.reshape(1, width),
        group_shift.reshape(1, width),
        expert_pick.T,
        pair_logits.T,
        group_prob.reshape(1, tokens),
    )
    (theirs,) = call(
        functools.partial(give_body, n_taps),
        (shape((half, width), BF16),),
        scratch=(pltpu.VMEM(ext_shape, F32),),
        n_in=5,
        limit=4,
        flops=500_000_000,
    )(mixed, halo, ext, taps, vecs)
    other = lax.ppermute(theirs, "tp", [(0, 1), (1, 0)])
    (partial,) = call(
        functools.partial(own_body, n_taps),
        (shape((tokens, model), F32),),
        scratch=(pltpu.VMEM(ext_shape, F32), pltpu.VMEM((half, width), BF16)),
        n_in=7,
        limit=4,
        flops=500_000_000,
    )(mixed, halo, ext, taps, vecs, out_weight, residual)
    hidden, send = call(
        project_body,
        (shape((tokens, model), BF16), message),
        scratch=(pltpu.VMEM((PARTS * tokens, step), BF16),),
        n_in=5,
        limit=16,
        flops=1_000_000_000,
    )(other, out_weight, partial, ffn_gain.reshape(1, model), spread)
    flat = pltpu.VMEM((RANKS * experts, model), BF16)

    def exchange(x):
        x = x.reshape(experts, RANKS * PARTS, step)
        return lax.all_to_all(x, ("sp", "tp"), 0, 0, tiled=True).reshape(rows, step)

    got = exchange(send)
    (done,) = call(
        expert_body, (message,), scratch=(flat,), n_in=4, limit=24, flops=4_000_000_000
    )(got, gate_weight[0], up_weight[0], down_weight[0])
    back = exchange(done)
    (result,) = call(
        combine_body,
        (shape((tokens, model), BF16),),
        scratch=(pltpu.VMEM((tokens, model), BF16), pltpu.SemaphoreType.DMA((8,))),
        n_in=3,
        out_hbm=(0,),
        limit=12,
        flops=1_000_000_000,
    )(back, picked, hidden)
    return result


def solution(mesh):
    in_specs = (
        P("sp", "tp"),
        P("sp", "tp"),
        P(None, "tp"),
        P("tp"),
        P("tp"),
        P("tp"),
        P(),
        P(("sp", "tp"), None),
        P(),
        P(("sp", "tp"), None),
        P(("sp", "tp"), None),
        P(("sp", "tp")),
        P(("sp", "tp"), None, None),
        P(("sp", "tp"), None, None),
        P(("sp", "tp"), None, None),
    )
    out_specs = P(("sp", "tp"), None)

    return jax.shard_map(local, mesh=mesh, in_specs=in_specs, out_specs=out_specs, check_vma=False)
```

```python
import functools
import jax
import jax.numpy as jnp
from jax import lax
from jax.experimental import pallas as pl
from jax.experimental.pallas import tpu as pltpu
from jax.sharding import PartitionSpec as P


EPS = 1e-06
F32 = jnp.float32
BF16 = jnp.bfloat16
HALO = 32
PARTS = 2
RANKS = 4
LANE = 128
MIB = 1024 * 1024


def iota(shape, axis):
    return lax.broadcasted_iota(jnp.int32, shape, axis)


def onehot(cond):
    return jnp.where(cond, 1.0, 0.0).astype(BF16)


def call(body, out_shape, scratch=(), limit=16, smem=(), hbm=(), n_in=0, out_hbm=(), flops=0):
    kind = {**dict.fromkeys(smem, pltpu.SMEM), **dict.fromkeys(hbm, pltpu.HBM)}
    n_out = len(out_shape)
    run = pl.pallas_call(
        body,
        out_shape=out_shape,
        in_specs=[pl.BlockSpec(memory_space=kind.get(i, pltpu.VMEM)) for i in range(n_in)],
        out_specs=[
            pl.BlockSpec(memory_space=pltpu.HBM if i in out_hbm else pltpu.VMEM) for i in range(n_out)
        ],
        scratch_shapes=list(scratch),
        compiler_params=pltpu.CompilerParams(vmem_limit_bytes=limit * MIB),
        cost_estimate=pl.CostEstimate(flops=flops, bytes_accessed=0, transcendentals=0),
    )
    return lambda *args: run(
        *(pltpu.with_memory_space_constraint(a, pltpu.HBM) if i in hbm else a for i, a in enumerate(args))
    )


def fetch(sources, targets, sems):
    copies = [
        pltpu.make_async_copy(source, target, sems.at[i])
        for i, (source, target) in enumerate(zip(sources, targets, strict=True))
    ]
    for copy in copies:
        copy.start()
    return copies


def route(pick, logits, prob, cols, spread):
    e_iota = iota((LANE, LANE), 0)
    n_iota = iota((LANE, LANE), 1)
    picks = [pick[k : k + 1, :] for k in range(2)]
    hits = [(e_iota == p).astype(F32) for p in picks]
    both = (hits[0] + hits[1]).astype(BF16)
    before = jnp.dot(both, onehot(e_iota < n_iota), preferred_element_type=F32)
    places = []
    for k in range(2):
        rank = jnp.sum(before * hits[k], axis=0, keepdims=True)
        places.append(RANKS * picks[k] + rank.astype(jnp.int32))
    first = prob[...] * jax.nn.sigmoid(logits[0:1, :] - logits[1:2, :])
    second = prob[...] * jax.nn.sigmoid(logits[1:2, :] - logits[0:1, :])
    rows = [places[0].astype(F32), places[1].astype(F32), first, second]
    table = jnp.zeros((LANE, LANE), F32)
    for i, row in enumerate(rows):
        table = jnp.where(e_iota == i, row, table)
    cols[...] = table.T
    part = e_iota // RANKS % PARTS
    for b in range(spread.shape[0] // LANE):
        row = e_iota + b * LANE
        code = row // (RANKS * PARTS) * RANKS + row % RANKS
        hit = jnp.logical_or(code == places[0], code == places[1])
        for q in range(PARTS):
            spread[b * LANE : (b + 1) * LANE, q * LANE : (q + 1) * LANE] = onehot(
                jnp.logical_and(hit, part == q)
            )


def select(cols, picked):
    tokens, rows = cols.shape[0], picked.shape[1]
    slot = iota((tokens, rows), 1)
    code = (slot // (RANKS * PARTS) * RANKS + slot % RANKS).astype(F32)
    share = jnp.where(cols[:, 0:1] == code, cols[:, 2:3], 0.0)
    share = jnp.where(cols[:, 1:2] == code, cols[:, 3:4], share)
    part = slot // RANKS % PARTS
    for q in range(PARTS):
        picked[q * tokens : (q + 1) * tokens, :] = jnp.where(part == q, share, 0.0).astype(BF16)


def tail_body(value_in, gate_in, tail, value, gate, sems):
    last = pl.ds(value_in.shape[0] - HALO, HALO)
    for copy in fetch((value_in.at[last, :], gate_in.at[last, :]), (value, gate), sems):
        copy.wait()
    glued = value[...].astype(F32) * jax.nn.sigmoid(gate[...].astype(F32))
    tail[...] = glued.astype(BF16)


def taps_and_norm(ext, taps, vecs, b, start, rows, n_taps):
    lanes = pl.ds(pl.multiple_of(b * LANE, LANE), LANE)
    acc = jnp.broadcast_to(vecs[0:1, lanes], (rows, LANE))
    for j in range(n_taps):
        at = start + HALO - (n_taps - 1) + j
        acc = acc + taps[b, j : j + 1, :] * ext[b, at : at + rows, :]
    centre = jnp.mean(acc, axis=-1, keepdims=True)
    away = acc - centre
    variance = jnp.mean(away * away, axis=-1, keepdims=True)
    v = away * lax.rsqrt(variance + EPS) * vecs[1:2, lanes] + vecs[2:3, lanes]
    return (v / (1.0 + jnp.exp(-v))).astype(BF16)


def conv_body(
    value, gate, kernel, bias, gain, shift, pick, logits, prob,
    mixed, ext, taps, vecs, spread, picked,
    cols,
):
    for i, row in enumerate((bias, gain, shift)):
        vecs[i : i + 1, :] = row[...]
    n_taps, width = kernel.shape
    blocks, length, _ = ext.shape
    for b in range(blocks):
        lanes = slice(b * LANE, (b + 1) * LANE)
        taps[b, 0:n_taps, :] = kernel[:, lanes].astype(F32)
        glued = value[:, lanes].astype(F32) * jax.nn.sigmoid(gate[:, lanes].astype(F32))
        ext[b, :, :] = glued.astype(BF16).astype(F32)
    mixed[0:HALO, :] = jnp.zeros((HALO, width), BF16)
    route(pick, logits, prob, cols, spread)
    select(cols, picked)

    def block(b, carry):
        lanes = pl.ds(pl.multiple_of(b * LANE, LANE), LANE)
        for r in range(HALO, length, HALO):
            mixed[r : r + HALO, lanes] = taps_and_norm(ext, taps, vecs, b, r - HALO, HALO, n_taps)
        return carry

    lax.fori_loop(0, blocks, block, 0)


def head(halo, front, taps, vecs, ext, out, n_taps):
    for b in range(ext.shape[0]):
        lanes = slice(b * LANE, (b + 1) * LANE)
        ext[b, 0:HALO, :] = jnp.where(lax.axis_index("sp") > 0, halo[:, lanes].astype(F32), 0.0)
        ext[b, HALO : 2 * HALO, :] = front[b, 0:HALO, :]
    for b in range(ext.shape[0]):
        lanes = slice(b * LANE, (b + 1) * LANE)
        out[0:HALO, lanes] = taps_and_norm(ext, taps, vecs, b, 0, HALO, n_taps)


def give_body(n_taps, mixed, halo, front, taps, vecs, theirs, ext):
    half = theirs.shape[0]
    core = lax.axis_index("tp")

    @pl.when(core == 0)
    def _():
        theirs[...] = mixed[half : 2 * half, :]

    @pl.when(core != 0)
    def _():
        theirs[...] = mixed[0:half, :]
        head(halo, front, taps, vecs, ext, theirs, n_taps)


def own_body(n_taps, mixed, halo, front, taps, vecs, weight, residual, partial, ext, mine):
    half, width = mine.shape
    step = partial.shape[1] // 4
    core = lax.axis_index("tp")

    @pl.when(core == 0)
    def _():
        mine[...] = mixed[0:half, :]
        head(halo, front, taps, vecs, ext, mine, n_taps)

    @pl.when(core != 0)
    def _():
        mine[...] = mixed[half : 2 * half, :]

    here = pl.ds(pl.multiple_of(core * width, width), width)
    for q in range(4):
        lanes = slice(q * step, (q + 1) * step)
        acc = jnp.dot(mine[...], weight[here, lanes], preferred_element_type=F32)
        partial[:, lanes] = acc + residual[:, lanes].astype(F32)


def project_body(other, weight, partial, gain, spread, hidden, out, stacked):
    tokens, half = other.shape
    width = partial.shape[1]
    step = width // 4
    there = pl.ds(pl.multiple_of((1 - lax.axis_index("tp")) * half, half), half)
    total = jnp.zeros((tokens, 1), F32)
    for q in range(4):
        lanes = slice(q * step, (q + 1) * step)
        acc = jnp.dot(other[...], weight[there, lanes], preferred_element_type=F32)
        rounded = (acc + partial[:, lanes]).astype(BF16)
        hidden[:, lanes] = rounded
        wide = rounded.astype(F32)
        total = total + jnp.sum(wide * wide, axis=-1, keepdims=True)
    scale = lax.rsqrt(total / width + EPS)
    step = width // PARTS
    for q in range(PARTS):
        lanes = slice(q * step, (q + 1) * step)
        stacked[q * tokens : (q + 1) * tokens, :] = (
            hidden[:, lanes].astype(F32) * scale * gain[:, lanes]
        ).astype(BF16)
    chunk = 2 * LANE
    for b in range(out.shape[0] // chunk):
        rows = slice(b * chunk, (b + 1) * chunk)
        out[rows, :] = jnp.dot(spread[rows, :], stacked[...], preferred_element_type=F32).astype(BF16)


def trade(a, b):
    low = iota(a.shape, 1) < RANKS
    return jnp.where(low, a, pltpu.roll(b, RANKS, 1)), jnp.where(low, pltpu.roll(a, RANKS, 1), b)


def expert_body(message, gate, up, down, out, flat, active):
    rows, step = message.shape
    tile = RANKS * PARTS
    pairs = rows // (2 * tile)
    pieces = 4
    size = step // pieces
    for p in range(pieces):
        here = slice(p * size, (p + 1) * size)
        wide = message[:, here].astype(F32).reshape(pairs, 2, tile, size)
        for q, half in enumerate(trade(wide[:, 0], wide[:, 1])):
            flat[:, q * step + p * size : q * step + (p + 1) * size] = half.reshape(rows // 2, size).astype(BF16)
    hidden = gate.shape[1]
    for n in range(2):
        units = slice(n * hidden // 2, (n + 1) * hidden // 2)
        g = jnp.dot(flat[...], gate[:, units], preferred_element_type=F32)
        u = jnp.dot(flat[...], up[:, units], preferred_element_type=F32)
        active[:, units] = (g / (1.0 + jnp.exp(-g)) * u).astype(BF16)
    for p in range(pieces):
        halves = [
            jnp.dot(
                active[...], down[:, q * step + p * size : q * step + (p + 1) * size], preferred_element_type=F32
            ).reshape(pairs, tile, size)
            for q in range(PARTS)
        ]
        both = jnp.stack(trade(*halves), axis=1)
        out[:, p * size : (p + 1) * size] = both.reshape(rows, size).astype(BF16)


def combine_body(message, picked, base, out_hbm, out, sems):
    tokens = out.shape[0]
    step = message.shape[1]
    pieces = 4
    size = step // pieces
    copies = []
    for p in range(pieces):
        got = jnp.dot(picked[...], message[:, p * size : (p + 1) * size], preferred_element_type=F32)
        for q in range(PARTS):
            lanes = slice(q * step + p * size, q * step + (p + 1) * size)
            out[:, lanes] = (base[:, lanes].astype(F32) + got[q * tokens : (q + 1) * tokens]).astype(BF16)
            copy = pltpu.make_async_copy(
                out.at[:, lanes], out_hbm.at[:, lanes], sems.at[p * PARTS + q]
            )
            copy.start()
            copies.append(copy)
    for copy in copies:
        copy.wait()


def local(
    glu_value,
    glu_gate,
    conv_kernel,
    conv_bias,
    group_gain,
    group_shift,
    out_weight,
    residual,
    ffn_gain,
    expert_pick,
    pair_logits,
    group_prob,
    gate_weight,
    up_weight,
    down_weight,
):
    shape = jax.ShapeDtypeStruct
    length, width = glu_value.shape
    tokens, model = residual.shape
    experts = lax.axis_size("sp") * lax.axis_size("tp")
    peers = lax.axis_size("sp")

    n_taps = conv_kernel.shape[0]
    blocks = width // LANE
    step = model // PARTS
    rows = experts * RANKS * PARTS
    message = shape((rows, step), BF16)
    (tail,) = call(
        tail_body,
        (shape((HALO, width), BF16),),
        scratch=(
            pltpu.VMEM((HALO, width), BF16),
            pltpu.VMEM((HALO, width), BF16),
            pltpu.SemaphoreType.DMA((2,)),
        ),
        hbm=range(2),
        n_in=2,
        limit=4,
        flops=5_000_000_000,
    )(glu_value, glu_gate)
    halo = lax.ppermute(tail, "sp", [(i, (i + 1) % peers) for i in range(peers)])
    half = length // 2
    ext_shape = (blocks, 2 * HALO, LANE)
    mixed, ext, taps, vecs, spread, picked = call(
        conv_body,
        (
            shape((length, width), BF16),
            shape((blocks, length, LANE), F32),
            shape((blocks, 32, LANE), F32),
            shape((8, width), F32),
            shape((rows, PARTS * tokens), BF16),
            shape((PARTS * tokens, rows), BF16),
        ),
        scratch=(pltpu.VMEM((tokens, LANE), F32),),
        n_in=9,
        limit=4,
        flops=6_000_000_000,
    )(
        glu_value,
        glu_gate,
        conv_kernel,
        conv_bias.reshape(1, width),
        group_gain.reshape(1, width),
        group_shift.reshape(1, width),
        expert_pick.T,
        pair_logits.T,
        group_prob.reshape(1, tokens),
    )
    (theirs,) = call(
        functools.partial(give_body, n_taps),
        (shape((half, width), BF16),),
        scratch=(pltpu.VMEM(ext_shape, F32),),
        n_in=5,
        limit=4,
        flops=500_000_000,
    )(mixed, halo, ext, taps, vecs)
    other = lax.ppermute(theirs, "tp", [(0, 1), (1, 0)])
    (partial,) = call(
        functools.partial(own_body, n_taps),
        (shape((tokens, model), F32),),
        scratch=(pltpu.VMEM(ext_shape, F32), pltpu.VMEM((half, width), BF16)),
        n_in=7,
        limit=4,
        flops=500_000_000,
    )(mixed, halo, ext, taps, vecs, out_weight, residual)
    hidden, send = call(
        project_body,
        (shape((tokens, model), BF16), message),
        scratch=(pltpu.VMEM((PARTS * tokens, step), BF16),),
        n_in=5,
        limit=16,
        flops=1_000_000_000,
    )(other, out_weight, partial, ffn_gain.reshape(1, model), spread)
    flat = pltpu.VMEM((RANKS * experts, model), BF16)

    def exchange(x):
        x = x.reshape(experts, RANKS * PARTS, step)
        return lax.all_to_all(x, ("sp", "tp"), 0, 0, tiled=True).reshape(rows, step)

    got = exchange(send)
    (done,) = call(
        expert_body,
        (message,),
        scratch=(flat, pltpu.VMEM((RANKS * experts, gate_weight.shape[2]), BF16)),
        n_in=4,
        limit=24,
        flops=4_000_000_000,
    )(got, gate_weight[0], up_weight[0], down_weight[0])
    back = exchange(done)
    (result,) = call(
        combine_body,
        (shape((tokens, model), BF16),),
        scratch=(pltpu.VMEM((tokens, model), BF16), pltpu.SemaphoreType.DMA((8,))),
        n_in=3,
        out_hbm=(0,),
        limit=12,
        flops=1_000_000_000,
    )(back, picked, hidden)
    return result


def solution(mesh):
    in_specs = (
        P("sp", "tp"),
        P("sp", "tp"),
        P(None, "tp"),
        P("tp"),
        P("tp"),
        P("tp"),
        P(),
        P(("sp", "tp"), None),
        P(),
        P(("sp", "tp"), None),
        P(("sp", "tp"), None),
        P(("sp", "tp")),
        P(("sp", "tp"), None, None),
        P(("sp", "tp"), None, None),
        P(("sp", "tp"), None, None),
    )
    out_specs = P(("sp", "tp"), None)

    return jax.shard_map(local, mesh=mesh, in_specs=in_specs, out_specs=out_specs, check_vma=False)
```

```python
import functools
import jax
import jax.numpy as jnp
from jax import lax
from jax.experimental import pallas as pl
from jax.experimental.pallas import tpu as pltpu
from jax.sharding import PartitionSpec as P


EPS = 1e-06
F32 = jnp.float32
BF16 = jnp.bfloat16
HALO = 32
PARTS = 2
RANKS = 4
LANE = 128
MIB = 1024 * 1024


def iota(shape, axis):
    return lax.broadcasted_iota(jnp.int32, shape, axis)


def onehot(cond):
    return jnp.where(cond, 1.0, 0.0).astype(BF16)


def call(body, out_shape, scratch=(), limit=16, smem=(), hbm=(), n_in=0, out_hbm=(), flops=0):
    kind = {**dict.fromkeys(smem, pltpu.SMEM), **dict.fromkeys(hbm, pltpu.HBM)}
    n_out = len(out_shape)
    run = pl.pallas_call(
        body,
        out_shape=out_shape,
        in_specs=[pl.BlockSpec(memory_space=kind.get(i, pltpu.VMEM)) for i in range(n_in)],
        out_specs=[
            pl.BlockSpec(memory_space=pltpu.HBM if i in out_hbm else pltpu.VMEM) for i in range(n_out)
        ],
        scratch_shapes=list(scratch),
        compiler_params=pltpu.CompilerParams(vmem_limit_bytes=limit * MIB),
        cost_estimate=pl.CostEstimate(flops=flops, bytes_accessed=0, transcendentals=0),
    )
    return lambda *args: run(
        *(pltpu.with_memory_space_constraint(a, pltpu.HBM) if i in hbm else a for i, a in enumerate(args))
    )


def fetch(sources, targets, sems):
    copies = [
        pltpu.make_async_copy(source, target, sems.at[i])
        for i, (source, target) in enumerate(zip(sources, targets, strict=True))
    ]
    for copy in copies:
        copy.start()
    return copies


def route(pick, logits, prob, cols, spread):
    e_iota = iota((LANE, LANE), 0)
    n_iota = iota((LANE, LANE), 1)
    picks = [pick[k : k + 1, :] for k in range(2)]
    hits = [(e_iota == p).astype(F32) for p in picks]
    both = (hits[0] + hits[1]).astype(BF16)
    before = jnp.dot(both, onehot(e_iota < n_iota), preferred_element_type=F32)
    places = []
    for k in range(2):
        rank = jnp.sum(before * hits[k], axis=0, keepdims=True)
        places.append(RANKS * picks[k] + rank.astype(jnp.int32))
    first = prob[...] * jax.nn.sigmoid(logits[0:1, :] - logits[1:2, :])
    second = prob[...] * jax.nn.sigmoid(logits[1:2, :] - logits[0:1, :])
    rows = [places[0].astype(F32), places[1].astype(F32), first, second]
    table = jnp.zeros((LANE, LANE), F32)
    for i, row in enumerate(rows):
        table = jnp.where(e_iota == i, row, table)
    cols[...] = table.T
    part = e_iota // RANKS % PARTS
    for b in range(spread.shape[0] // LANE):
        row = e_iota + b * LANE
        code = row // (RANKS * PARTS) * RANKS + row % RANKS
        hit = jnp.logical_or(code == places[0], code == places[1])
        for q in range(PARTS):
            spread[b * LANE : (b + 1) * LANE, q * LANE : (q + 1) * LANE] = onehot(
                jnp.logical_and(hit, part == q)
            )


def select(cols, picked):
    tokens, rows = cols.shape[0], picked.shape[1]
    slot = iota((tokens, rows), 1)
    code = (slot // (RANKS * PARTS) * RANKS + slot % RANKS).astype(F32)
    share = jnp.where(cols[:, 0:1] == code, cols[:, 2:3], 0.0)
    share = jnp.where(cols[:, 1:2] == code, cols[:, 3:4], share)
    part = slot // RANKS % PARTS
    for q in range(PARTS):
        picked[q * tokens : (q + 1) * tokens, :] = jnp.where(part == q, share, 0.0).astype(BF16)


def tail_body(value_in, gate_in, tail, value, gate, sems):
    last = pl.ds(value_in.shape[0] - HALO, HALO)
    for copy in fetch((value_in.at[last, :], gate_in.at[last, :]), (value, gate), sems):
        copy.wait()
    glued = value[...].astype(F32) * jax.nn.sigmoid(gate[...].astype(F32))
    tail[...] = glued.astype(BF16)


def taps_and_norm(ext, taps, vecs, b, start, rows, n_taps):
    lanes = pl.ds(pl.multiple_of(b * LANE, LANE), LANE)
    acc = jnp.broadcast_to(vecs[0:1, lanes], (rows, LANE))
    for j in range(n_taps):
        at = start + HALO - (n_taps - 1) + j
        acc = acc + taps[b, j : j + 1, :] * ext[b, at : at + rows, :]
    centre = jnp.mean(acc, axis=-1, keepdims=True)
    away = acc - centre
    variance = jnp.mean(away * away, axis=-1, keepdims=True)
    v = away * lax.rsqrt(variance + EPS) * vecs[1:2, lanes] + vecs[2:3, lanes]
    return (v / (1.0 + jnp.exp(-v))).astype(BF16)


def conv_body(
    value, gate, kernel, bias, gain, shift, pick, logits, prob,
    mixed, ext, taps, vecs, spread, picked,
    cols,
):
    for i, row in enumerate((bias, gain, shift)):
        vecs[i : i + 1, :] = row[...]
    n_taps, width = kernel.shape
    blocks, length, _ = ext.shape
    for b in range(blocks):
        lanes = slice(b * LANE, (b + 1) * LANE)
        taps[b, 0:n_taps, :] = kernel[:, lanes].astype(F32)
        glued = value[:, lanes].astype(F32) * jax.nn.sigmoid(gate[:, lanes].astype(F32))
        ext[b, :, :] = glued.astype(BF16).astype(F32)
    mixed[0:HALO, :] = jnp.zeros((HALO, width), BF16)
    route(pick, logits, prob, cols, spread)
    select(cols, picked)

    def block(b, carry):
        lanes = pl.ds(pl.multiple_of(b * LANE, LANE), LANE)
        for r in range(HALO, length, HALO):
            mixed[r : r + HALO, lanes] = taps_and_norm(ext, taps, vecs, b, r - HALO, HALO, n_taps)
        return carry

    lax.fori_loop(0, blocks, block, 0)


def head(halo, front, taps, vecs, ext, out, n_taps):
    for b in range(ext.shape[0]):
        lanes = slice(b * LANE, (b + 1) * LANE)
        ext[b, 0:HALO, :] = jnp.where(lax.axis_index("sp") > 0, halo[:, lanes].astype(F32), 0.0)
        ext[b, HALO : 2 * HALO, :] = front[b, 0:HALO, :]
    for b in range(ext.shape[0]):
        lanes = slice(b * LANE, (b + 1) * LANE)
        out[0:HALO, lanes] = taps_and_norm(ext, taps, vecs, b, 0, HALO, n_taps)


def give_body(n_taps, mixed, halo, front, taps, vecs, theirs, ext):
    half = theirs.shape[0]
    core = lax.axis_index("tp")

    @pl.when(core == 0)
    def _():
        theirs[...] = mixed[half : 2 * half, :]

    @pl.when(core != 0)
    def _():
        theirs[...] = mixed[0:half, :]
        head(halo, front, taps, vecs, ext, theirs, n_taps)


def own_body(n_taps, mixed, halo, front, taps, vecs, weight, residual, partial, ext, mine):
    half, width = mine.shape
    step = partial.shape[1] // 4
    core = lax.axis_index("tp")

    @pl.when(core == 0)
    def _():
        mine[...] = mixed[0:half, :]
        head(halo, front, taps, vecs, ext, mine, n_taps)

    @pl.when(core != 0)
    def _():
        mine[...] = mixed[half : 2 * half, :]

    here = pl.ds(pl.multiple_of(core * width, width), width)
    for q in range(4):
        lanes = slice(q * step, (q + 1) * step)
        acc = jnp.dot(mine[...], weight[here, lanes], preferred_element_type=F32)
        partial[:, lanes] = acc + residual[:, lanes].astype(F32)


def project_body(other, weight, partial, gain, spread, hidden, out, stacked):
    tokens, half = other.shape
    width = partial.shape[1]
    step = width // 4
    there = pl.ds(pl.multiple_of((1 - lax.axis_index("tp")) * half, half), half)
    total = jnp.zeros((tokens, 1), F32)
    for q in range(4):
        lanes = slice(q * step, (q + 1) * step)
        acc = jnp.dot(other[...], weight[there, lanes], preferred_element_type=F32)
        rounded = (acc + partial[:, lanes]).astype(BF16)
        hidden[:, lanes] = rounded
        wide = rounded.astype(F32)
        total = total + jnp.sum(wide * wide, axis=-1, keepdims=True)
    scale = lax.rsqrt(total / width + EPS)
    step = width // PARTS
    for q in range(PARTS):
        lanes = slice(q * step, (q + 1) * step)
        stacked[q * tokens : (q + 1) * tokens, :] = (
            hidden[:, lanes].astype(F32) * scale * gain[:, lanes]
        ).astype(BF16)
    chunk = 2 * LANE
    for b in range(out.shape[0] // chunk):
        rows = slice(b * chunk, (b + 1) * chunk)
        out[rows, :] = jnp.dot(spread[rows, :], stacked[...], preferred_element_type=F32).astype(BF16)


def trade(a, b):
    low = iota(a.shape, 1) < RANKS
    return jnp.where(low, a, pltpu.roll(b, RANKS, 1)), jnp.where(low, pltpu.roll(a, RANKS, 1), b)


def expert_body(message, gate, up, down, out, flat):
    rows, step = message.shape
    tile = RANKS * PARTS
    pairs = rows // (2 * tile)
    pieces = 4
    size = step // pieces
    for p in range(pieces):
        here = slice(p * size, (p + 1) * size)
        wide = message[:, here].astype(F32).reshape(pairs, 2, tile, size)
        for q, half in enumerate(trade(wide[:, 0], wide[:, 1])):
            flat[:, q * step + p * size : q * step + (p + 1) * size] = half.reshape(rows // 2, size).astype(BF16)
    x = flat[...]
    g = jnp.dot(x, gate[...], preferred_element_type=F32)
    u = jnp.dot(x, up[...], preferred_element_type=F32)
    active = (g / (1.0 + jnp.exp(-g)) * u).astype(BF16)
    for p in range(pieces):
        halves = [
            jnp.dot(
                active, down[:, q * step + p * size : q * step + (p + 1) * size], preferred_element_type=F32
            ).reshape(pairs, tile, size)
            for q in range(PARTS)
        ]
        both = jnp.stack(trade(*halves), axis=1)
        out[:, p * size : (p + 1) * size] = both.reshape(rows, size).astype(BF16)


def combine_body(message, picked, base, out_hbm, out, sems):
    tokens = out.shape[0]
    step = message.shape[1]
    cuts = (0, step // 2, step - LANE, step)
    copies = []
    for start, end in zip(cuts[:-1], cuts[1:], strict=True):
        got = jnp.dot(picked[...], message[:, start:end], preferred_element_type=F32)
        for q in range(PARTS):
            lanes = slice(q * step + start, q * step + end)
            out[:, lanes] = (base[:, lanes].astype(F32) + got[q * tokens : (q + 1) * tokens]).astype(BF16)
            copy = pltpu.make_async_copy(out.at[:, lanes], out_hbm.at[:, lanes], sems.at[len(copies)])
            copy.start()
            copies.append(copy)
    for copy in copies:
        copy.wait()


def local(
    glu_value,
    glu_gate,
    conv_kernel,
    conv_bias,
    group_gain,
    group_shift,
    out_weight,
    residual,
    ffn_gain,
    expert_pick,
    pair_logits,
    group_prob,
    gate_weight,
    up_weight,
    down_weight,
):
    shape = jax.ShapeDtypeStruct
    length, width = glu_value.shape
    tokens, model = residual.shape
    experts = lax.axis_size("sp") * lax.axis_size("tp")
    peers = lax.axis_size("sp")

    n_taps = conv_kernel.shape[0]
    blocks = width // LANE
    step = model // PARTS
    rows = experts * RANKS * PARTS
    message = shape((rows, step), BF16)
    (tail,) = call(
        tail_body,
        (shape((HALO, width), BF16),),
        scratch=(
            pltpu.VMEM((HALO, width), BF16),
            pltpu.VMEM((HALO, width), BF16),
            pltpu.SemaphoreType.DMA((2,)),
        ),
        hbm=range(2),
        n_in=2,
        limit=4,
        flops=5_000_000_000,
    )(glu_value, glu_gate)
    halo = lax.ppermute(tail, "sp", [(i, (i + 1) % peers) for i in range(peers)])
    half = length // 2
    ext_shape = (blocks, 2 * HALO, LANE)
    mixed, ext, taps, vecs, spread, picked = call(
        conv_body,
        (
            shape((length, width), BF16),
            shape((blocks, length, LANE), F32),
            shape((blocks, 32, LANE), F32),
            shape((8, width), F32),
            shape((rows, PARTS * tokens), BF16),
            shape((PARTS * tokens, rows), BF16),
        ),
        scratch=(pltpu.VMEM((tokens, LANE), F32),),
        n_in=9,
        limit=4,
        flops=6_000_000_000,
    )(
        glu_value,
        glu_gate,
        conv_kernel,
        conv_bias.reshape(1, width),
        group_gain.reshape(1, width),
        group_shift.reshape(1, width),
        expert_pick.T,
        pair_logits.T,
        group_prob.reshape(1, tokens),
    )
    (theirs,) = call(
        functools.partial(give_body, n_taps),
        (shape((half, width), BF16),),
        scratch=(pltpu.VMEM(ext_shape, F32),),
        n_in=5,
        limit=4,
        flops=500_000_000,
    )(mixed, halo, ext, taps, vecs)
    other = lax.ppermute(theirs, "tp", [(0, 1), (1, 0)])
    (partial,) = call(
        functools.partial(own_body, n_taps),
        (shape((tokens, model), F32),),
        scratch=(pltpu.VMEM(ext_shape, F32), pltpu.VMEM((half, width), BF16)),
        n_in=7,
        limit=4,
        flops=500_000_000,
    )(mixed, halo, ext, taps, vecs, out_weight, residual)
    hidden, send = call(
        project_body,
        (shape((tokens, model), BF16), message),
        scratch=(pltpu.VMEM((PARTS * tokens, step), BF16),),
        n_in=5,
        limit=16,
        flops=1_000_000_000,
    )(other, out_weight, partial, ffn_gain.reshape(1, model), spread)
    flat = pltpu.VMEM((RANKS * experts, model), BF16)

    def exchange(x):
        x = x.reshape(experts, RANKS * PARTS, step)
        return lax.all_to_all(x, ("sp", "tp"), 0, 0, tiled=True).reshape(rows, step)

    got = exchange(send)
    (done,) = call(
        expert_body, (message,), scratch=(flat,), n_in=4, limit=24, flops=4_000_000_000
    )(got, gate_weight[0], up_weight[0], down_weight[0])
    back = exchange(done)
    (result,) = call(
        combine_body,
        (shape((tokens, model), BF16),),
        scratch=(pltpu.VMEM((tokens, model), BF16), pltpu.SemaphoreType.DMA((8,))),
        n_in=3,
        out_hbm=(0,),
        limit=12,
        flops=1_000_000_000,
    )(back, picked, hidden)
    return result


def solution(mesh):
    in_specs = (
        P("sp", "tp"),
        P("sp", "tp"),
        P(None, "tp"),
        P("tp"),
        P("tp"),
        P("tp"),
        P(),
        P(("sp", "tp"), None),
        P(),
        P(("sp", "tp"), None),
        P(("sp", "tp"), None),
        P(("sp", "tp")),
        P(("sp", "tp"), None, None),
        P(("sp", "tp"), None, None),
        P(("sp", "tp"), None, None),
    )
    out_specs = P(("sp", "tp"), None)

    return jax.shard_map(local, mesh=mesh, in_specs=in_specs, out_specs=out_specs, check_vma=False)
```
